32 devices in a mesh: sp: 4 (over z), fs: 4 (over y, x), tp: 2 (over core).
Axes of the slice: x: 2, y: 2, z: 4, core: 2. Of those that a mesh axis runs over, the one named last changes fastest.
Arguments:
- activations: bfloat16 [2048, 4096], P(('fs', 'sp'), 'tp'), parts along dimension 0, may hold values from -6 to 6
- input_norm_gain: float32 [4096], replicated, may hold values from 0.1 to 1.9
- window_query_weight: bfloat16 [4096, 2048], P('sp', 'tp'), may hold values from -0.09375 to 0.09375
- window_key_weight: bfloat16 [4096, 512], P('sp', 'tp'), may hold values from -0.09375 to 0.09375
- window_value_weight: bfloat16 [4096, 512], P('sp', 'tp'), may hold values from -0.09375 to 0.09375
- linear_query_weight: bfloat16 [4096, 1024], P('sp', 'tp'), may hold values from -0.09375 to 0.09375
- linear_key_weight: bfloat16 [4096, 1024], P('sp', 'tp'), may hold values from -0.09375 to 0.09375
- linear_value_weight: bfloat16 [4096, 2048], P('sp', 'tp'), may hold values from -0.09375 to 0.09375
- decay_down_factor: bfloat16 [4096, 16], replicated, may hold values from -0.09375 to 0.09375
- decay_up_factor: bfloat16 [16, 1024], P(None, 'tp'), may hold values from -1.5 to 1.5
- decay_offset_bias: float32 [1024], P('tp'), may hold values from -0.5 to 9
- extra_fading_exponent: float32 [2048, 8], P(('fs', 'sp'), 'tp'), parts along dimension 0, may hold values from -1.5 to 0
- starting_state: float32 [8, 128, 256], P('tp'), may hold values from -12 to 12
- head_sink_logit: float32 [32], P('tp'), may hold values from 1 to 5
- linear_head_gain: float32 [256], replicated, may hold values from 0.1 to 1.9
- window_output_weight: bfloat16 [2048, 4096], P('tp', 'sp'), may hold values from -0.09375 to 0.09375
- linear_output_weight: bfloat16 [2048, 4096], P('tp', 'sp'), may hold values from -0.09375 to 0.09375
Outputs:
- mixer_output: bfloat16 [2048, 4096], P(('fs', 'sp', 'tp')), parts along dimension 0
The draws below stay inside these ranges and needn't reach their ends.
There are 4 independent parts, one for each index of `fs`. The reference program is written for one: setup_inputs(seed, part) draws one part's arguments, and reference() takes and returns one part's arrays. A program takes and returns all parts, laid end to end along the dimension named above; an argument that names none is the same for every part. Nothing has to cross between parts.
All inputs are finite; a program needn't handle non-finite values.
Results may differ from the reference program's by a relative error of at most 0.019.
Values may be sent and summed in bfloat16 or wider, within the bound.
No kernel may reach another device: no remote copies, remote signals or barrier semaphores. Data moves between devices by JAX's collectives and lax.ppermute only.
A program may use at most 128 MiB of HBM per device.

```python
import jax
import jax.numpy as jnp
from jax import lax

D = 4096
QH = 32
KVH = 8
HD = 64
WINDOW = 128
GATED_MIXERS = 8
LOOKUP_FEATURES = 128
DV = 256
RANK = 16
SPAN = 64
T_DEV = 128
TOKENS = 512
N_TP = 2


def draw_decay_offset_bias(key, part):
    key_flags, key_slow, key_quick = jax.random.split(key, 3)
    fast_share = 0.5
    is_quick = jax.random.uniform(key_flags, (GATED_MIXERS, 1)) < fast_share
    slow_values = jax.random.uniform(key_slow, (GATED_MIXERS, LOOKUP_FEATURES), minval=6.0, maxval=9.0)
    quick_values = jax.random.uniform(key_quick, (GATED_MIXERS, LOOKUP_FEATURES), minval=-0.5, maxval=1.0)
    return jnp.where(is_quick, quick_values, slow_values).reshape(GATED_MIXERS * LOOKUP_FEATURES).astype(jnp.float32)


def draw_extra_fading_exponent(key, part):
    key_rate, key_place, key_depth = jax.random.split(key, 3)
    block_count = TOKENS // T_DEV
    low_end = 0.25
    rates = jnp.exp(jax.random.uniform(key_rate, (block_count, GATED_MIXERS), minval=jnp.log(low_end), maxval=0.0))
    equilibrium_memory = jnp.repeat(-0.8 * rates / TOKENS, T_DEV, axis=0)
    element_indices = jax.random.randint(key_place, (2, GATED_MIXERS), 0, TOKENS)
    accrued_fading_totals = jnp.log(jax.random.uniform(key_depth, (2, GATED_MIXERS), minval=0.5, maxval=0.8))
    element_ordinals = jnp.arange(TOKENS, dtype=jnp.int32)[:, None, None]
    spike_contributions = jnp.sum(jnp.where(element_ordinals == element_indices[None], accrued_fading_totals[None], 0.0), axis=1)
    return (equilibrium_memory + spike_contributions).astype(jnp.float32)


def levels(rng, shape, shards, low, top_value):
    def one(axis_at, blocks):
        heights = jax.random.uniform(jax.random.fold_in(jax.random.fold_in(rng, 6), axis_at), (blocks,), jnp.float32, low / len(shards), top_value / len(shards))
        return jnp.repeat(jnp.exp(heights), shape[axis_at] // blocks).reshape((-1,) + (1,) * (len(shape) - axis_at - 1))

    factor_of = one(*shards[0])
    for cut in shards[1:]:
        factor_of = factor_of * one(*cut)
    return factor_of


def scatter_about(stream_key, dims, spread, bound, shards=(), kind=jnp.bfloat16):
    level = levels(stream_key, dims, shards, -0.22, 0.18) if shards else 1.0
    values = jax.random.normal(stream_key, dims, jnp.float32) * spread * level
    return jnp.minimum(jnp.maximum(values, -bound), bound).astype(kind)


def setup_inputs(seed: int = 0, part: int = 0) -> dict:
    seeds = jax.random.split(jax.random.key(seed), 18)
    part_splits = jax.random.split(jax.random.fold_in(seeds[17], part), 18)
    activations = scatter_about(part_splits[0], (TOKENS, D), 1.0, 6.0, ((0, 4), (1, 2)))
    input_norm_gain = jnp.clip(1.0 + 0.18 * jax.random.normal(seeds[1], (D,), jnp.float32), 0.1, 1.9)
    window_query_weight = scatter_about(seeds[2], (D, QH * HD), D ** -0.5, 0.09375, ((0, 4), (1, 2)))
    window_key_weight = scatter_about(seeds[3], (D, KVH * HD), D ** -0.5, 0.09375, ((0, 4), (1, 2)))
    window_value_weight = scatter_about(seeds[4], (D, KVH * HD), D ** -0.5, 0.09375, ((0, 4), (1, 2)))
    linear_query_weight = scatter_about(seeds[5], (D, GATED_MIXERS * LOOKUP_FEATURES), D ** -0.5, 0.09375, ((0, 4), (1, 2)))
    linear_key_weight = scatter_about(seeds[6], (D, GATED_MIXERS * LOOKUP_FEATURES), D ** -0.5, 0.09375, ((0, 4), (1, 2)))
    linear_value_weight = scatter_about(seeds[7], (D, GATED_MIXERS * DV), D ** -0.5, 0.09375, ((0, 4), (1, 2)))
    decay_down_factor = scatter_about(seeds[8], (D, RANK), D ** -0.5, 0.09375)
    decay_up_factor = scatter_about(seeds[9], (RANK, GATED_MIXERS * LOOKUP_FEATURES), RANK ** -0.5, 1.5, ((1, 2),))
    decay_offset_bias = draw_decay_offset_bias(jax.random.fold_in(seeds[17], 71), part)
    extra_fading_exponent = draw_extra_fading_exponent(jax.random.fold_in(jax.random.fold_in(seeds[17], part), 71), part)
    starting_state = scatter_about(seeds[12], (GATED_MIXERS, LOOKUP_FEATURES, DV), 2.0, 12.0, ((0, 2),), jnp.float32)
    head_sink_logit = jnp.clip(1.0 + 4.0 * jax.random.uniform(seeds[13], (QH,), jnp.float32) ** levels(seeds[13], (QH,), ((0, 2),), -0.2, 0.2), 1.0, 5.0)
    linear_head_gain = jnp.clip(1.0 + 0.18 * jax.random.normal(seeds[14], (DV,), jnp.float32), 0.1, 1.9)
    window_output_weight = scatter_about(seeds[15], (QH * HD, D), (QH * HD + GATED_MIXERS * DV) ** -0.5, 0.09375, ((0, 2), (1, 4)))
    linear_output_weight = scatter_about(seeds[16], (GATED_MIXERS * DV, D), (QH * HD + GATED_MIXERS * DV) ** -0.5, 0.09375, ((0, 2), (1, 4)))
    return {"activations": activations, "input_norm_gain": input_norm_gain, "window_query_weight": window_query_weight, "window_key_weight": window_key_weight, "window_value_weight": window_value_weight, "linear_query_weight": linear_query_weight, "linear_key_weight": linear_key_weight, "linear_value_weight": linear_value_weight, "decay_down_factor": decay_down_factor, "decay_up_factor": decay_up_factor, "decay_offset_bias": decay_offset_bias, "extra_fading_exponent": extra_fading_exponent, "starting_state": starting_state, "head_sink_logit": head_sink_logit, "linear_head_gain": linear_head_gain, "window_output_weight": window_output_weight, "linear_output_weight": linear_output_weight}


EPS = 1e-05
FADING_SOFTNESS = 16.0
HIGH_PRECISION = lax.Precision.HIGHEST

def window_reference(near_query, near_keys, near_values, head_sink_logit):
    stream_extent = near_query.shape[0]
    blocks = stream_extent // WINDOW
    groups = QH // KVH
    zeros_front = jnp.zeros((WINDOW, KVH * HD), jnp.float32)

    def banded(current):
        extended = jnp.concatenate([zeros_front, current.astype(jnp.float32)], axis=0)
        earlier = extended[:stream_extent].reshape(blocks, WINDOW, KVH, HD)
        present = extended[WINDOW:].reshape(blocks, WINDOW, KVH, HD)
        return jnp.concatenate([earlier, present], axis=1)
    key_band = banded(near_keys)
    value_band = banded(near_values)
    queries = near_query.astype(jnp.float32).reshape(blocks, WINDOW, KVH, groups, HD)
    scores = jnp.einsum('nqhgd,nkhd->hgnqk', queries, key_band, precision=HIGH_PRECISION) * HD ** (-0.5)
    head_ids = jnp.arange(QH, dtype=jnp.int32)
    slopes = jnp.exp2(-8.0 * (head_ids + 1).astype(jnp.float32) / QH).reshape(KVH, groups)
    query_pos = jnp.arange(WINDOW, dtype=jnp.int32)
    key_pos = jnp.arange(2 * WINDOW, dtype=jnp.int32)
    distance = query_pos[:, None] - key_pos[None, :] + WINDOW
    start_pos = (jnp.arange(blocks, dtype=jnp.int32) - 1) * WINDOW
    absolute = start_pos[:, None] + key_pos[None, :]
    allowed = ((distance >= 0) & (distance < WINDOW))[None] & (absolute >= 0)[:, None, :]
    biased = scores - slopes[:, :, None, None, None] * distance.astype(jnp.float32)
    weights = jnp.where(allowed, jnp.exp(biased), 0.0)
    denominator = lax.optimization_barrier(jnp.sum(weights, axis=-1, keepdims=True)) + jnp.exp(head_sink_logit.reshape(KVH, groups))[:, :, None, None, None]
    attention = (weights / denominator).astype(jnp.bfloat16)
    attended = jnp.einsum('hgnqk,nkhd->nqhgd', attention.astype(jnp.float32), value_band, precision=HIGH_PRECISION)
    return attended.reshape(stream_extent, QH * HD).astype(jnp.bfloat16)

def linear_reference(gated_query, gated_keys, gated_values, fading_exponent, linear_head_gain, starting_state):
    stream_extent = gated_query.shape[0]
    span_count = stream_extent // SPAN
    scaled_query = gated_query.astype(jnp.float32).reshape(span_count, SPAN, GATED_MIXERS, LOOKUP_FEATURES) * LOOKUP_FEATURES ** (-0.5)
    keys_wide = gated_keys.astype(jnp.float32).reshape(span_count, SPAN, GATED_MIXERS, LOOKUP_FEATURES)
    values_wide = gated_values.astype(jnp.float32).reshape(span_count, SPAN, GATED_MIXERS, DV)
    running = jnp.cumsum(fading_exponent.reshape(span_count, SPAN, GATED_MIXERS, LOOKUP_FEATURES), axis=1)
    span_end = running[:, -1]
    query_with_decay = scaled_query * jnp.exp(running)
    inverse_keys = keys_wide * jnp.exp(-running)
    ending_keys = keys_wide * jnp.exp(span_end[:, None] - running)
    inner = jnp.einsum('nchk,nshk->nhcs', query_with_decay, inverse_keys, precision=HIGH_PRECISION)
    lower = jnp.tril(jnp.ones((SPAN, SPAN), dtype=bool))
    inner = jnp.where(lower, inner, 0.0)
    within = jnp.einsum('nhcs,nshv->nchv', inner, values_wide, precision=HIGH_PRECISION)

    def advance(running_state, inputs):
        query_portion, key_portion, value_portion, scale_factor = inputs
        layer_output = jnp.einsum('fmy,mys->fms', query_portion, running_state, precision=HIGH_PRECISION)
        running_state = running_state * scale_factor[..., None] + jnp.einsum('gxp,gxz->xpz', key_portion, value_portion, precision=HIGH_PRECISION)
        return (running_state, layer_output)
    start_state = starting_state.astype(jnp.float32)
    final_state, carried = lax.scan(advance, start_state, (query_with_decay, ending_keys, values_wide, jnp.exp(span_end)))
    flat = (within + carried).reshape(stream_extent, GATED_MIXERS, DV)
    normal = flat * lax.rsqrt(lax.optimization_barrier(jnp.mean(flat * flat, axis=-1, keepdims=True)) + EPS) * linear_head_gain
    return normal.reshape(stream_extent, GATED_MIXERS * DV).astype(jnp.bfloat16)

def reference(activations, input_norm_gain, window_query_weight, window_key_weight, window_value_weight, linear_query_weight, linear_key_weight, linear_value_weight, decay_down_factor, decay_up_factor, decay_offset_bias, extra_fading_exponent, starting_state, head_sink_logit, linear_head_gain, window_output_weight, linear_output_weight):
    widened = activations.astype(jnp.float32)
    normed = (widened * lax.rsqrt(lax.optimization_barrier(jnp.mean(widened * widened, axis=1, keepdims=True)) + EPS) * input_norm_gain).astype(jnp.bfloat16)

    def project(matrix):
        return jnp.dot(normed, matrix, preferred_element_type=jnp.float32).astype(jnp.bfloat16)
    near_query = project(window_query_weight)
    near_keys = project(window_key_weight)
    near_values = project(window_value_weight)
    gated_query = project(linear_query_weight)
    gated_keys = project(linear_key_weight)
    gated_values = project(linear_value_weight)
    low_rank = project(decay_down_factor)
    attention_energies = jnp.dot(low_rank, decay_up_factor, preferred_element_type=jnp.float32) + decay_offset_bias
    stream_extent = normed.shape[0]
    fading_exponent = (jax.nn.log_sigmoid(attention_energies) / FADING_SOFTNESS).reshape(stream_extent, GATED_MIXERS, LOOKUP_FEATURES) + extra_fading_exponent[:, :, None]
    near_out = window_reference(near_query, near_keys, near_values, head_sink_logit)
    gated_out = linear_reference(gated_query, gated_keys, gated_values, fading_exponent, linear_head_gain, starting_state)
    window_cols = QH * HD // N_TP
    linear_cols = GATED_MIXERS * DV // N_TP
    accumulated = jnp.zeros((stream_extent, D), jnp.float32)
    for member in range(N_TP):
        first_w = member * window_cols
        first_l = member * linear_cols
        partial_value = jnp.dot(near_out[:, first_w:first_w + window_cols], window_output_weight[first_w:first_w + window_cols], preferred_element_type=jnp.float32)
        partial_value = partial_value + jnp.dot(gated_out[:, first_l:first_l + linear_cols], linear_output_weight[first_l:first_l + linear_cols], preferred_element_type=jnp.float32)
        rounded = lax.optimization_barrier(partial_value.astype(jnp.bfloat16))
        accumulated = accumulated + rounded.astype(jnp.float32)
    return accumulated.astype(jnp.bfloat16)
```

```python
import functools

import jax
import jax.numpy as jnp
from jax import lax
from jax.experimental import pallas as pl
from jax.experimental.pallas import tpu as pltpu
from jax.sharding import PartitionSpec as P

QH = 32
HD = 64
WINDOW = 128
LOOKUP_FEATURES = 128
DV = 256
SPAN = 64


EPS = 1e-05
FADING_SOFTNESS = 16.0
HIGH_PRECISION = lax.Precision.HIGHEST


def passed_along(value, axis, steps):
    count = lax.axis_size(axis)
    leading, last = (max(0, -steps), min(count, count - steps))
    return lax.ppermute(value, axis, [(source, source + steps) for source in range(leading, last)])


def prefix(x, axis, combine, identity):
    peers, place = (lax.axis_size(axis), lax.axis_index(axis))
    everything = jax.tree.map(
        lambda part, kind: lax.all_gather(part.astype(kind), axis), x, (jnp.bfloat16, jnp.bfloat16)
    )
    start = jax.tree.map(
        lambda part, zero: jnp.broadcast_to(jnp.asarray(zero, part.dtype), part.shape), x, identity
    )

    def hop(k, before):
        reached = k < place
        new = combine(
            before, jax.tree.map(lambda part, own: part[k].astype(own.dtype), everything, x)
        )
        return jax.tree.map(lambda a, b: jnp.where(reached, a, b), new, before)

    return lax.fori_loop(0, peers, hop, start)


def window_attention(near_query, near_keys, near_values, head_sink_logit):
    stream_extent = near_query.shape[0]
    key_heads = near_keys.shape[1] // HD
    heads_here = near_query.shape[1] // HD
    groups = heads_here // key_heads
    blocks = stream_extent // WINDOW
    tail_rows = jnp.stack([near_keys, near_values])
    before = passed_along(tail_rows, "sp", 1)

    def banded(previous, current):
        extended = jnp.concatenate([previous, current], axis=0)
        earlier = extended[:stream_extent].reshape(blocks, WINDOW, key_heads, HD)
        present = extended[WINDOW:].reshape(blocks, WINDOW, key_heads, HD)
        return jnp.concatenate([earlier, present], axis=1)

    key_band = banded(before[0], near_keys)
    value_band = banded(before[1], near_values)
    queries = near_query.reshape(blocks, WINDOW, key_heads, groups, HD)
    scores = jnp.einsum(
        "nqhgd,nkhd->hgnqk", queries, key_band, preferred_element_type=jnp.float32
    ) * HD ** (-0.5)
    head_ids = lax.axis_index("tp") * heads_here + jnp.arange(heads_here, dtype=jnp.int32)
    slopes = jnp.exp2(-8.0 * (head_ids + 1).astype(jnp.float32) / QH).reshape(key_heads, groups)
    query_pos = jnp.arange(WINDOW, dtype=jnp.int32)
    key_pos = jnp.arange(2 * WINDOW, dtype=jnp.int32)
    distance = query_pos[:, None] - key_pos[None, :] + WINDOW
    start_pos = (
        lax.axis_index("sp") * stream_extent + (jnp.arange(blocks, dtype=jnp.int32) - 1) * WINDOW
    )
    absolute = start_pos[:, None] + key_pos[None, :]
    allowed = ((distance >= 0) & (distance < WINDOW))[None] & (absolute >= 0)[:, None, :]
    biased = scores - slopes[:, :, None, None, None] * distance.astype(jnp.float32)
    weights = jnp.where(allowed, jnp.exp(biased), 0.0)
    denominator = (
        jnp.sum(weights, axis=-1, keepdims=True)
        + jnp.exp(head_sink_logit.reshape(key_heads, groups))[:, :, None, None, None]
    )
    attention = (weights / denominator).astype(jnp.bfloat16)
    attended = jnp.einsum(
        "hgnqk,nkhd->nqhgd", attention, value_band, preferred_element_type=jnp.float32
    )
    return attended.reshape(stream_extent, heads_here * HD).astype(jnp.bfloat16)


def linear_attention(
    gated_query, gated_keys, gated_values, fading_exponent, linear_head_gain, starting_state
):
    stream_extent = gated_query.shape[0]
    head_total = gated_query.shape[1] // LOOKUP_FEATURES
    span_count = stream_extent // SPAN
    scaled_query = gated_query.astype(jnp.float32).reshape(
        span_count, SPAN, head_total, LOOKUP_FEATURES
    ) * LOOKUP_FEATURES ** (-0.5)
    keys_wide = gated_keys.astype(jnp.float32).reshape(
        span_count, SPAN, head_total, LOOKUP_FEATURES
    )
    values_wide = gated_values.astype(jnp.float32).reshape(span_count, SPAN, head_total, DV)
    running = jnp.cumsum(
        fading_exponent.reshape(span_count, SPAN, head_total, LOOKUP_FEATURES), axis=1
    )
    span_end = running[:, -1]
    query_with_decay = scaled_query * jnp.exp(running)
    inverse_keys = keys_wide * jnp.exp(-running)
    ending_keys = keys_wide * jnp.exp(span_end[:, None] - running)
    inner = jnp.einsum("nchk,nshk->nhcs", query_with_decay, inverse_keys, precision=HIGH_PRECISION)
    lower = jnp.tril(jnp.ones((SPAN, SPAN), dtype=bool))
    inner = jnp.where(lower, inner, 0.0)
    within = jnp.einsum("nhcs,nshv->nchv", inner, values_wide, precision=HIGH_PRECISION)

    def advance(running_state, inputs):
        query_portion, key_portion, value_portion, scale_factor = inputs
        layer_output = jnp.einsum(
            "fmy,mys->fms", query_portion, running_state, precision=HIGH_PRECISION
        )
        running_state = running_state * scale_factor[..., None] + jnp.einsum(
            "gxp,gxz->xpz", key_portion, value_portion, precision=HIGH_PRECISION
        )
        return (running_state, layer_output)

    start_state = jnp.zeros((head_total, LOOKUP_FEATURES, DV), jnp.float32)
    state_end, carried = lax.scan(
        advance, start_state, (query_with_decay, ending_keys, values_wide, jnp.exp(span_end))
    )
    device_decay = jnp.exp(jnp.sum(span_end, axis=0))
    prefix_sums = jnp.cumsum(span_end, axis=0) - span_end

    def combine(earlier, later):
        return (earlier[0] * later[0], later[0][..., None] * earlier[1] + later[1])

    decay_before, state_before = prefix(
        (device_decay, state_end),
        "sp",
        combine,
        (jnp.ones_like(device_decay), jnp.zeros_like(state_end)),
    )
    incoming_rows = state_before + decay_before[..., None] * starting_state
    crossing = jnp.einsum(
        "qwso,soz->qwsz",
        query_with_decay * jnp.exp(prefix_sums)[:, None],
        incoming_rows,
        precision=HIGH_PRECISION,
    )
    flat = (within + carried + crossing).reshape(stream_extent, head_total, DV)
    normal = (
        flat * lax.rsqrt(jnp.mean(flat * flat, axis=-1, keepdims=True) + EPS) * linear_head_gain
    )
    return normal.reshape(stream_extent, head_total * DV).astype(jnp.bfloat16)


def local(
    activations,
    input_norm_gain,
    window_query_weight,
    window_key_weight,
    window_value_weight,
    linear_query_weight,
    linear_key_weight,
    linear_value_weight,
    decay_down_factor,
    decay_up_factor,
    decay_offset_bias,
    extra_fading_exponent,
    starting_state,
    head_sink_logit,
    linear_head_gain,
    window_output_weight,
    linear_output_weight,
):
    gathered = lax.all_gather(activations, "tp", axis=1, tiled=True)
    widened = gathered.astype(jnp.float32)
    normed = (
        widened
        * lax.rsqrt(jnp.mean(widened * widened, axis=1, keepdims=True) + EPS)
        * input_norm_gain
    ).astype(jnp.bfloat16)
    row_total = normed.shape[0]
    matrices = (
        window_query_weight,
        window_key_weight,
        window_value_weight,
        linear_query_weight,
        linear_key_weight,
        linear_value_weight,
    )
    segments = (
        lax.all_gather(matrices[0], "sp", axis=0, tiled=True),
        lax.all_gather(matrices[1], "sp", axis=0, tiled=True),
        lax.all_gather(matrices[2], "sp", axis=0, tiled=True),
        lax.all_gather(matrices[3], "sp", axis=0, tiled=True),
        lax.all_gather(matrices[4], "sp", axis=0, tiled=True),
        lax.all_gather(matrices[5], "sp", axis=0, tiled=True),
    )
    projected = tuple(
        (jnp.dot(normed, segment, preferred_element_type=jnp.float32) for segment in segments)
    )
    near_query, near_keys, near_values, gated_query, gated_keys, gated_values = [
        product.astype(jnp.bfloat16) for product in projected
    ]
    low_rank = jnp.dot(normed, decay_down_factor, preferred_element_type=jnp.float32).astype(
        jnp.bfloat16
    )
    attention_energies = (
        jnp.dot(low_rank, decay_up_factor, preferred_element_type=jnp.float32) + decay_offset_bias
    )
    head_total = extra_fading_exponent.shape[1]
    fading_exponent = (jax.nn.log_sigmoid(attention_energies) / FADING_SOFTNESS).reshape(
        row_total, head_total, LOOKUP_FEATURES
    ) + extra_fading_exponent[:, :, None]
    near_out = window_attention(near_query, near_keys, near_values, head_sink_logit)
    gated_out = linear_attention(
        gated_query, gated_keys, gated_values, fading_exponent, linear_head_gain, starting_state
    )
    window_full, linear_full = (
        lax.all_gather(window_output_weight, "sp", axis=1, tiled=True),
        lax.all_gather(linear_output_weight, "sp", axis=1, tiled=True),
    )
    return lax.psum_scatter(
        (
            jnp.dot(near_out, window_full, preferred_element_type=jnp.float32)
            + jnp.dot(gated_out, linear_full, preferred_element_type=jnp.float32)
        ).astype(jnp.bfloat16),
        "tp",
        scatter_dimension=0,
        tiled=True,
    )


def _pairs(peers, depths, core):
    out = []
    for d in depths:
        out.append((d * 2 + core, (d + 1) * 2 + core))
        out.append(((peers - 1 - d) * 2 + 1 - core, (peers - 2 - d) * 2 + 1 - core))
    return out


SWAP = [(0, 1), (1, 0)]
VMEM = pl.BlockSpec(memory_space=pltpu.VMEM)
SMEM = pl.BlockSpec(memory_space=pltpu.SMEM)
ANY = pl.BlockSpec(memory_space=pl.ANY)
BY_COLUMNS = (((1,), (1,)), ((), ()))
BY_ROWS = (((0,), (0,)), ((), ()))


def _call(kernel, name, out_shape, flops, moved, **kw):
    return pl.pallas_call(
        kernel,
        out_shape=out_shape,
        compiler_params=pltpu.CompilerParams(vmem_limit_bytes=48 * 1024 * 1024),
        cost_estimate=pl.CostEstimate(flops=flops, bytes_accessed=moved, transcendentals=0),
        name=name,
        **kw,
    )


def _prefetch(scalars, grid, in_specs, out_specs, scratch=()):
    return pltpu.PrefetchScalarGridSpec(
        num_scalar_prefetch=scalars, grid=grid, in_specs=in_specs, out_specs=out_specs, scratch_shapes=scratch
    )


def norm_kernel(place_ref, x_ref, fade_ref, mate_ref, gain_ref, down_ref, out_ref):
    me = place_ref[0]
    pieces, rows, wide = out_ref.shape
    half_model = x_ref.shape[1]
    cut = 2 * half_model // pieces
    fades = fade_ref.shape[1]
    own = x_ref[pl.ds(pl.multiple_of(me * rows, rows), rows), :].astype(jnp.float32)
    mate = mate_ref[:, :half_model].astype(jnp.float32)
    square = jnp.sum(own * own, axis=1, keepdims=True) + jnp.sum(mate * mate, axis=1, keepdims=True)
    scale = lax.rsqrt(square / (2 * half_model) + EPS)
    low_rank = None
    for side, value in ((me, own), (1 - me, mate)):
        start = pl.multiple_of(side * half_model, half_model)
        normed = (value * scale * gain_ref[:, pl.ds(start, half_model)]).astype(jnp.bfloat16)
        part = jnp.dot(normed, down_ref[pl.ds(start, half_model), :], preferred_element_type=jnp.float32)
        low_rank = part if low_rank is None else low_rank + part
        for k in range(pieces // 2):
            out_ref[side * (pieces // 2) + k, :, :cut] = normed[:, k * cut : (k + 1) * cut]
    mine = fade_ref[pl.ds(pl.multiple_of(me * rows, rows), rows), :]
    theirs = mate_ref[:, half_model : half_model + fades]
    tail = jnp.concatenate(
        [
            low_rank.astype(jnp.bfloat16).astype(jnp.float32),
            jnp.where(me == 0, mine, theirs).astype(jnp.float32),
            jnp.where(me == 0, theirs, mine).astype(jnp.float32),
            jnp.zeros((rows, wide - cut - low_rank.shape[1] - 2 * fades), jnp.float32),
        ],
        axis=1,
    ).astype(jnp.bfloat16)
    for k in range(pieces):
        out_ref[k, :, cut:] = tail


def pack_kernel(key_heads, side_ref, wq, wk, wv, lq, lk, lv, out_ref):
    step = pl.program_id(0)
    half = out_ref.shape[2] // 2
    keys_and_values = step == 0
    queries = (step > 0) & (step <= key_heads)
    head_items = (step > key_heads) & ((step - key_heads) % 2 == 1)
    head_values = (step > key_heads) & ((step - key_heads) % 2 == 0)

    @pl.when(keys_and_values)
    def _():
        out_ref[0, :, :half] = wk[...]
        out_ref[0, :, half:] = wv[...]

    @pl.when(queries)
    def _():
        out_ref[0] = wq[...]

    @pl.when(head_items)
    def _():
        out_ref[0, :, :half] = lq[...]
        out_ref[0, :, half:] = lk[...]

    @pl.when(head_values)
    def _():
        out_ref[0] = lv[...]


def pack_items(side, lin, key_heads, matrices):
    depth = matrices[0].shape[0]
    width = 2 * LOOKUP_FEATURES
    count = 1 + key_heads + 2 * lin
    fixed = pl.BlockSpec((depth, width // 2), lambda i, side: (0, side[0]))
    query = pl.BlockSpec(
        (depth, width), lambda i, side: (0, side[0] * key_heads + jnp.clip(i - 1, 0, key_heads - 1))
    )
    head = lambda i, side: (0, side[0] * lin + jnp.clip((i - 1 - key_heads) // 2, 0, lin - 1))
    narrow, full = pl.BlockSpec((depth, width // 2), head), pl.BlockSpec((depth, width), head)
    return _call(
        functools.partial(pack_kernel, key_heads),
        "pack_items",
        jax.ShapeDtypeStruct((count, depth, width), jnp.bfloat16),
        10**9,
        4 * count * depth * width,
        grid_spec=_prefetch(
            1,
            (count,),
            [query, fixed, fixed, narrow, narrow, full],
            pl.BlockSpec((1, depth, width), lambda i, side: (i, 0, 0)),
        ),
    )(side, *matrices)


def partial_kernel(index_ref, mine_ref, theirs_ref, own_ref, other_ref, *rest):
    out_ref = rest[-1]
    width = own_ref.shape[-1]
    rows = mine_ref.shape[0]
    for top, x_ref in enumerate((mine_ref, theirs_ref)):
        for half, weight in enumerate((own_ref, other_ref)):
            at = slice(top * rows, (top + 1) * rows)
            span = slice(half * width, (half + 1) * width)
            total = jnp.dot(x_ref[...], weight[0], preferred_element_type=jnp.float32)
            if len(rest) == 2:
                total = total + rest[0][at, span].astype(jnp.float32)
            out_ref[at, span] = total.astype(out_ref.dtype)


def partial_sum(index, mine, theirs, own, other, arrived):
    rows = mine.shape[0]
    _, depth, width = own.shape
    operands = [mine, theirs, own, other] + ([] if arrived is None else [arrived])
    whole = pl.BlockSpec((2 * rows, 2 * width), lambda i, index: (0, 0))
    tokens = pl.BlockSpec((rows, depth), lambda i, index: (0, 0))
    block = pl.BlockSpec((1, depth, width), lambda i, index: (index[0], 0, 0))
    return _call(
        partial_kernel,
        "partial_sum",
        jax.ShapeDtypeStruct((2 * rows, 2 * width), jnp.bfloat16),
        8 * rows * depth * width,
        4 * depth * (rows + width),
        grid_spec=_prefetch(
            1, (1,), [tokens, tokens, block, block] + ([] if arrived is None else [whole]), whole
        ),
    )(index, *operands)


def decay_kernel(lin, rank, place_ref, mine_ref, theirs_ref, own_ref, other_ref, out_ref):
    me, side = place_ref[0], place_ref[1]
    rows = mine_ref.shape[0]
    features = LOOKUP_FEATURES
    all_heads = 4 * lin
    lower = (
        lax.broadcasted_iota(jnp.int32, (SPAN, SPAN), 0) >= lax.broadcasted_iota(jnp.int32, (SPAN, SPAN), 1)
    ).astype(jnp.bfloat16)
    for top, tail_ref in enumerate((mine_ref, theirs_ref)):
        tail = tail_ref[...]
        low_rank = tail[:, :rank]
        parts = [
            tail[:, rank + k * 2 * lin : rank + (k + 1) * 2 * lin].astype(jnp.float32) for k in range(6)
        ]
        by_core = [parts[0] + parts[1] + parts[2], parts[3] + parts[4] + parts[5]]
        fades = [jnp.where(me == 0, by_core[0], by_core[1]), jnp.where(me == 0, by_core[1], by_core[0])]
        for head in range(lin):
            for owner, small_ref in enumerate((own_ref, other_ref)):
                at = pl.ds(pl.multiple_of((side * lin + head) * features, features), features)
                up = small_ref[:rank, at].astype(jnp.bfloat16)
                energy = jnp.dot(low_rank, up, preferred_element_type=jnp.float32) + small_ref[rank : rank + 1, at]
                soft = jnp.minimum(energy, 0.0) - jnp.log1p(jnp.exp(-jnp.abs(energy)))
                both = fades[owner]
                fade = jnp.where(side == 0, both[:, head : head + 1], both[:, lin + head : lin + head + 1])
                step = soft * (1.0 / FADING_SOFTNESS) + fade
                high = step.astype(jnp.bfloat16)
                rest = step - high.astype(jnp.float32)
                middle = rest.astype(jnp.bfloat16)
                low = (rest - middle.astype(jnp.float32)).astype(jnp.bfloat16)
                column = (2 * head + owner) * features
                for span in range(rows // SPAN):
                    cut = slice(span * SPAN, (span + 1) * SPAN)
                    out_ref[top * rows + span * SPAN : top * rows + (span + 1) * SPAN, column : column + features] = (
                        jnp.dot(lower, high[cut], preferred_element_type=jnp.float32)
                        + jnp.dot(lower, middle[cut], preferred_element_type=jnp.float32)
                        + jnp.dot(lower, low[cut], preferred_element_type=jnp.float32)
                    )


def decay_sums(place, lin, rank, mine, theirs, own, other):
    rows, wide = mine.shape
    lanes = LOOKUP_FEATURES
    tail = pl.BlockSpec((rows, lanes), lambda i, place: (0, wide // lanes - 1))
    whole = lambda shape: pl.BlockSpec(shape, lambda i, place: (0, 0))
    out = (2 * rows, 2 * lin * LOOKUP_FEATURES)
    return _call(
        functools.partial(decay_kernel, lin, rank),
        "decay_sums",
        jax.ShapeDtypeStruct(out, jnp.float32),
        10**9,
        2**20,
        grid_spec=_prefetch(
            1, (1,), [tail, tail, whole(own.shape), whole(other.shape)], whole(out)
        ),
    )(place, mine, theirs, own, other)


def linear_kernel(lin, head, half, place_ref, query_key_ref, value_ref, running_ref, own_ref, other_ref, gain_ref, out_ref):
    me, side = place_ref[0], place_ref[1]
    rows, width = query_key_ref.shape
    features = LOOKUP_FEATURES
    values = width // 2
    lower = lax.broadcasted_iota(jnp.int32, (SPAN, SPAN), 0) >= lax.broadcasted_iota(
        jnp.int32, (SPAN, SPAN), 1
    )
    states = [state_ref[side * lin + head].T for state_ref in (own_ref, other_ref)]
    for span in range(rows // SPAN):
        per = half // SPAN
        device, inside = span // (2 * per), span % (2 * per)
        apart = jnp.where(me == inside // per, 0, rows // 2)
        at = pl.ds(pl.multiple_of(apart + device * half + (inside % per) * SPAN, SPAN), SPAN)
        for owner in range(2):
            base = owner * values
            running = running_ref[at, owner * features : (owner + 1) * features]
            query = query_key_ref[at, base : base + features].astype(jnp.float32)
            key = query_key_ref[at, base + features : base + 2 * features].astype(jnp.float32)
            value = value_ref[at, base : base + values]
            end = running[SPAN - 1 : SPAN]
            scaled = (query * features ** (-0.5) * jnp.exp(running)).astype(jnp.bfloat16)
            inverse = (key * jnp.exp(-running)).astype(jnp.bfloat16)
            ending = (key * jnp.exp(end - running)).astype(jnp.bfloat16)
            inner = lax.dot_general(scaled, inverse, BY_COLUMNS, preferred_element_type=jnp.float32)
            inner = jnp.where(lower, inner, 0.0).astype(jnp.bfloat16)
            state = states[owner]
            raw = jnp.dot(inner, value, preferred_element_type=jnp.float32) + lax.dot_general(
                scaled, state.astype(jnp.bfloat16), BY_COLUMNS, preferred_element_type=jnp.float32
            )
            states[owner] = state * jnp.exp(end) + lax.dot_general(
                value, ending, BY_ROWS, preferred_element_type=jnp.float32
            )
            scale = lax.rsqrt(jnp.mean(raw * raw, axis=-1, keepdims=True) + EPS)
            out_ref[at, base : base + values] = (raw * scale * gain_ref[...]).astype(out_ref.dtype)


def linear_heads(place, lin, head, half, query_key, value, running, own, other, gain):
    rows, width = query_key.shape
    whole = lambda a: pl.BlockSpec(a.shape, lambda i, place: (0,) * a.ndim)
    block = pl.BlockSpec((rows, 2 * LOOKUP_FEATURES), lambda i, place: (0, head))
    return _call(
        functools.partial(linear_kernel, lin, head, half),
        "linear_heads",
        jax.ShapeDtypeStruct((rows, width), jnp.bfloat16),
        2 * 10**9,
        2**21,
        grid_spec=_prefetch(
            1,
            (1,),
            [whole(query_key), whole(value), block, whole(own), whole(other), whole(gain)],
            pl.BlockSpec((rows, width), lambda i, place: (0, 0)),
        ),
    )(place, query_key, value, running, own, other, gain)


def window_kernel(group, half, place_ref, slope_ref, sink_ref, key_value_ref, query_ref, out_ref):
    me = place_ref[0]
    rows = query_ref.shape[0]
    owners, groups = slope_ref.shape
    pair = key_value_ref.shape[1] // (2 * owners)
    from_query = lax.broadcasted_iota(jnp.int32, (WINDOW, WINDOW), 0)
    from_key = lax.broadcasted_iota(jnp.int32, (WINDOW, WINDOW), 1)
    present = from_key <= from_query
    distance = jnp.where(present, from_query - from_key, from_query - from_key + WINDOW).astype(jnp.float32)
    unit = min(half, WINDOW)

    def places(block):
        out = []
        for piece in range(WINDOW // unit):
            start = block * WINDOW + piece * unit
            device, inside = start // (2 * half), start % (2 * half)
            apart = jnp.where(me == inside // half, 0, rows // 2)
            out.append(pl.ds(pl.multiple_of(apart + device * half + inside % half, unit), unit))
        return out

    for owner in range(owners):
        key_at = owner * 2 * pair + group * HD
        value_at = key_at + pair
        base = owner * groups * HD
        biases = [slope_ref[owner, head] * distance for head in range(groups)]
        past_keys, past_values = None, None
        for block in range(rows // WINDOW):
            first = block == 0
            at = places(block)
            keys = jnp.concatenate([key_value_ref[a, key_at : key_at + HD] for a in at], axis=0)
            values = jnp.concatenate([key_value_ref[a, value_at : value_at + HD] for a in at], axis=0)
            band_keys = keys if first else jnp.concatenate([past_keys, keys], axis=0)
            band_values = values if first else jnp.concatenate([past_values, values], axis=0)
            past_keys, past_values = keys, values
            queries = jnp.concatenate(
                [query_ref[a, base + head * HD : base + (head + 1) * HD] for head in range(groups) for a in at],
                axis=0,
            )
            scores = lax.dot_general(queries, band_keys, BY_COLUMNS, preferred_element_type=jnp.float32)
            probs = []
            for head in range(groups):
                mine = scores[head * WINDOW : (head + 1) * WINDOW]
                if first:
                    weight = jnp.where(present, jnp.exp(mine * HD ** (-0.5) - biases[head]), 0.0)
                else:
                    score = jnp.where(present, mine[:, WINDOW:], mine[:, :WINDOW])
                    weight = jnp.exp(score * HD ** (-0.5) - biases[head])
                total = jnp.sum(weight, axis=-1, keepdims=True) + sink_ref[owner, head]
                share = weight / total
                if first:
                    probs.append(share.astype(jnp.bfloat16))
                else:
                    probs.append(
                        jnp.concatenate(
                            [
                                jnp.where(present, 0.0, share).astype(jnp.bfloat16),
                                jnp.where(present, share, 0.0).astype(jnp.bfloat16),
                            ],
                            axis=1,
                        )
                    )
            outs = jnp.dot(jnp.concatenate(probs, axis=0), band_values, preferred_element_type=jnp.float32)
            joined = jnp.concatenate(
                [outs[head * WINDOW : (head + 1) * WINDOW] for head in range(groups)], axis=1
            ).astype(out_ref.dtype)
            for piece, a in enumerate(at):
                out_ref[a, base : base + groups * HD] = joined[piece * unit : (piece + 1) * unit]


def window_heads(place, group, half, slopes, sinks, key_value, query):
    return _call(
        functools.partial(window_kernel, group, half),
        "window_heads",
        jax.ShapeDtypeStruct(query.shape, jnp.bfloat16),
        2 * 10**9,
        2**21,
        in_specs=[SMEM, SMEM, SMEM, VMEM, VMEM],
        out_specs=VMEM,
    )(place, slopes, sinks, key_value, query)


def output_kernel(pieces, hops, place_ref, *refs):
    passed = refs[: pieces + hops]
    own_ref, other_ref = refs[pieces + hops : pieces + hops + 2]
    before = refs[pieces + hops + 2 : -3]
    out_ref, held, arrival = refs[-3:]
    depth = place_ref[2]
    for at in range(hops + 1):

        @pl.when(depth == at)
        def _():
            for piece in range(pieces):
                pltpu.make_async_copy(passed[piece + at], held.at[piece], arrival.at[piece]).start()

    for piece in range(pieces):
        pltpu.make_async_copy(passed[piece], held.at[piece], arrival.at[piece]).wait()
    width = held.shape[2] // 2
    rows = held.shape[1]
    columns = out_ref.shape[1]
    block = columns // 4
    for part in range(4):
        span = slice(part * block, (part + 1) * block)
        total = before[0][:, span] if before else jnp.zeros((rows, block), jnp.float32)
        for piece in range(pieces):
            lines = slice(piece * width, (piece + 1) * width)
            total = total + jnp.dot(held[piece, :, :width], own_ref[lines, span], preferred_element_type=jnp.float32)
            total = total + jnp.dot(held[piece, :, width:], other_ref[lines, span], preferred_element_type=jnp.float32)
        out_ref[:, span] = total.astype(out_ref.dtype)


def output_sum(place, passed, hops, own, other, before, kind):
    rows, width = passed[0].shape
    pieces = len(passed) - hops
    lines, columns = other.shape
    whole = pl.BlockSpec((rows, columns), lambda i, place: (0, 0))
    return _call(
        functools.partial(output_kernel, pieces, hops),
        "output_sum",
        jax.ShapeDtypeStruct((rows, columns), kind),
        4 * rows * columns * lines,
        8 * rows * columns,
        grid_spec=_prefetch(
            1,
            (1,),
            [ANY] * len(passed)
            + [
                pl.BlockSpec((lines, columns), lambda i, place: (place[1], 0)),
                pl.BlockSpec((lines, columns), lambda i, place: (0, 0)),
            ]
            + ([] if before is None else [whole]),
            whole,
            [pltpu.VMEM((pieces, rows, width), jnp.bfloat16), pltpu.SemaphoreType.DMA((pieces,))],
        ),
    )(place, *passed, own, other, *([] if before is None else [before]))


def resident(
    activations,
    input_norm_gain,
    window_query_weight,
    window_key_weight,
    window_value_weight,
    linear_query_weight,
    linear_key_weight,
    linear_value_weight,
    decay_down_factor,
    decay_up_factor,
    decay_offset_bias,
    extra_fading_exponent,
    starting_state,
    head_sink_logit,
    linear_head_gain,
    window_output_weight,
    linear_output_weight,
):
    peers = lax.axis_size("sp")
    hops = peers - 1
    line, me = lax.axis_index("sp"), lax.axis_index("tp")
    depth = jnp.where(me == 0, line, hops - line)
    far, near = 1 - me, me
    place = jnp.stack([me, far, hops - depth]).astype(jnp.int32)
    rows, half_model = activations.shape
    half = rows // 2
    bf16, f32 = jnp.bfloat16, jnp.float32
    lin = extra_fading_exponent.shape[1] // 2
    key_heads = window_key_weight.shape[1] // HD // 2
    query_heads = window_query_weight.shape[1] // HD // 2
    groups = query_heads // key_heads
    rank = decay_down_factor.shape[1]
    swap = lambda value: lax.ppermute(value, "tp", SWAP)

    high = lax.reduce_precision(extra_fading_exponent, 8, 7)
    rest = extra_fading_exponent - high
    middle = lax.reduce_precision(rest, 8, 7)
    fade = jnp.concatenate([high, middle, rest - middle], axis=1).astype(bf16)
    message = jnp.concatenate([activations, fade], axis=1)
    message = jnp.pad(message, ((0, 0), (0, LOOKUP_FEATURES - fade.shape[1])))
    mate = swap(lax.dynamic_slice_in_dim(message, far * half, half, axis=0))
    wide = 2 * half_model // peers + LOOKUP_FEATURES
    outgoing = _call(
        norm_kernel,
        "norm",
        jax.ShapeDtypeStruct((peers, half, wide), bf16),
        10**9,
        2**21,
        in_specs=[SMEM] + [VMEM] * 5,
        out_specs=VMEM,
    )(place, activations, fade, mate, input_norm_gain.reshape(1, -1), decay_down_factor)

    (
        outgoing,
        matrices,
        window_output_weight,
        linear_output_weight,
        starting_state,
        decay_up_factor,
        decay_offset_bias,
        head_sink_logit,
    ) = lax.optimization_barrier(
        (
            outgoing,
            (
                window_query_weight,
                window_key_weight,
                window_value_weight,
                linear_query_weight,
                linear_key_weight,
                linear_value_weight,
            ),
            window_output_weight,
            linear_output_weight,
            starting_state,
            decay_up_factor,
            decay_offset_bias,
            head_sink_logit,
        )
    )
    incoming = lax.all_to_all(outgoing, "sp", 0, 0, tiled=True)
    other_in = swap(pack_items(near.reshape(1), lin, key_heads, matrices))
    own_in = pack_items(far.reshape(1), lin, key_heads, matrices)
    features = decay_up_factor.shape[1]
    own_small = jnp.concatenate(
        [
            decay_up_factor.astype(f32),
            decay_offset_bias.reshape(1, features),
            jnp.pad(head_sink_logit, (0, features - head_sink_logit.shape[0])).reshape(1, features),
            jnp.zeros((6, features), f32),
        ],
        axis=0,
    )
    other_small = swap(own_small)
    other_state = swap(starting_state)
    lines = linear_output_weight.shape[0] // 2
    other_linear = swap(lax.dynamic_slice_in_dim(linear_output_weight, near * lines, lines, axis=0))
    lines = window_output_weight.shape[0] // 2
    other_window = swap(lax.dynamic_slice_in_dim(window_output_weight, near * lines, lines, axis=0))

    mine = incoming.reshape(peers * half, wide)
    theirs = swap(incoming).reshape(peers * half, wide)

    count = 1 + key_heads + 2 * lin
    arrived, finals = {}, []
    for step in range(count + 2 * hops):
        index = jnp.clip(step - 2 * depth, 0, count - 1).astype(jnp.int32).reshape(1)
        value = partial_sum(index, mine, theirs, own_in, other_in, arrived.get(step - 2))
        depths = [d for d in range(hops) if 0 <= step - 2 * d < count]
        if depths:
            arrived[step] = lax.ppermute(value, ("sp", "tp"), _pairs(peers, depths, 0))
        if step >= 2 * hops:
            finals.append(value)

    running = decay_sums(place, lin, rank, mine, theirs, own_small, other_small)
    sinks = jnp.stack(
        [
            lax.dynamic_slice_in_dim(small[rank + 1], far * query_heads, query_heads).reshape(key_heads, groups)
            for small in (own_small, other_small)
        ]
    )
    sinks = jnp.exp(sinks)
    attended = []
    for group in range(key_heads):
        number = jnp.stack([me, 1 - me])[:, None] * (2 * query_heads) + (
            far * query_heads + group * groups + jnp.arange(groups, dtype=jnp.int32)
        )
        slopes = jnp.exp2(-8.0 * (number + 1).astype(f32) / QH)
        attended.append(
            window_heads(place, group, half, slopes, sinks[:, group], finals[0], finals[1 + group])
        )
    for head in range(lin):
        first = 1 + key_heads + 2 * head
        attended.append(
            linear_heads(
                place,
                lin,
                head,
                half,
                finals[first],
                finals[first + 1],
                running,
                starting_state,
                other_state,
                linear_head_gain.reshape(1, DV),
            )
        )

    pieces = len(attended)
    passed = []
    for step in range(pieces + hops):
        if step == 0:
            now = attended[0]
        elif step < pieces:
            now = jnp.where(depth == hops, attended[step], back)
        else:
            now = back
        passed.append(now)
        depths = [d for d in range(hops) if 0 <= step - d < pieces]
        if depths:
            back = lax.ppermute(now, ("sp", "tp"), _pairs(peers, depths, 1))
    terms = output_sum(
        place, passed[: key_heads + hops], hops, window_output_weight, other_window, None, f32
    )
    terms = output_sum(place, passed[key_heads:], hops, linear_output_weight, other_linear, terms, bf16)

    kept, given = terms[: peers * half], swap(terms[peers * half :])
    result = (kept.astype(f32) + given.astype(f32)).astype(bf16)
    return lax.all_to_all(result, "sp", 0, 1, tiled=True)


def fits(mesh):
    return mesh.shape["tp"] == 2 and mesh.shape["sp"] > 1


def solution(mesh):
    placed = (
        P(("fs", "sp"), "tp"),
        P(),
        P("sp", "tp"),
        P("sp", "tp"),
        P("sp", "tp"),
        P("sp", "tp"),
        P("sp", "tp"),
        P("sp", "tp"),
        P(),
        P(None, "tp"),
        P("tp"),
        P(("fs", "sp"), "tp"),
        P("tp", None, None),
        P("tp"),
        P(),
        P("tp", "sp"),
        P("tp", "sp"),
    )
    return jax.shard_map(
        resident if fits(mesh) else local,
        mesh=mesh, in_specs=placed, out_specs=P(("fs", "sp", "tp"), None), check_vma=False
    )
```

```python
import functools

import jax
import jax.numpy as jnp
from jax import lax
from jax.experimental import pallas as pl
from jax.experimental.pallas import tpu as pltpu
from jax.sharding import PartitionSpec as P


QH = 32
HD = 64
WINDOW = 128
LOOKUP_FEATURES = 128
DV = 256
SPAN = 64


EPS = 1e-05
FADING_SOFTNESS = 16.0
HIGH_PRECISION = lax.Precision.HIGHEST


def passed_along(value, axis, steps):
    count = lax.axis_size(axis)
    leading, last = (max(0, -steps), min(count, count - steps))
    return lax.ppermute(value, axis, [(source, source + steps) for source in range(leading, last)])


def prefix(x, axis, combine, identity):
    peers, place = (lax.axis_size(axis), lax.axis_index(axis))
    everything = jax.tree.map(
        lambda part, kind: lax.all_gather(part.astype(kind), axis), x, (jnp.bfloat16, jnp.bfloat16)
    )
    start = jax.tree.map(
        lambda part, zero: jnp.broadcast_to(jnp.asarray(zero, part.dtype), part.shape), x, identity
    )

    def hop(k, before):
        reached = k < place
        new = combine(
            before, jax.tree.map(lambda part, own: part[k].astype(own.dtype), everything, x)
        )
        return jax.tree.map(lambda a, b: jnp.where(reached, a, b), new, before)

    return lax.fori_loop(0, peers, hop, start)


def window_attention(near_query, near_keys, near_values, head_sink_logit):
    stream_extent = near_query.shape[0]
    key_heads = near_keys.shape[1] // HD
    heads_here = near_query.shape[1] // HD
    groups = heads_here // key_heads
    blocks = stream_extent // WINDOW
    tail_rows = jnp.stack([near_keys, near_values])
    before = passed_along(tail_rows, "sp", 1)

    def banded(previous, current):
        extended = jnp.concatenate([previous, current], axis=0)
        earlier = extended[:stream_extent].reshape(blocks, WINDOW, key_heads, HD)
        present = extended[WINDOW:].reshape(blocks, WINDOW, key_heads, HD)
        return jnp.concatenate([earlier, present], axis=1)

    key_band = banded(before[0], near_keys)
    value_band = banded(before[1], near_values)
    queries = near_query.reshape(blocks, WINDOW, key_heads, groups, HD)
    scores = jnp.einsum(
        "nqhgd,nkhd->hgnqk", queries, key_band, preferred_element_type=jnp.float32
    ) * HD ** (-0.5)
    head_ids = lax.axis_index("tp") * heads_here + jnp.arange(heads_here, dtype=jnp.int32)
    slopes = jnp.exp2(-8.0 * (head_ids + 1).astype(jnp.float32) / QH).reshape(key_heads, groups)
    query_pos = jnp.arange(WINDOW, dtype=jnp.int32)
    key_pos = jnp.arange(2 * WINDOW, dtype=jnp.int32)
    distance = query_pos[:, None] - key_pos[None, :] + WINDOW
    start_pos = (
        lax.axis_index("sp") * stream_extent + (jnp.arange(blocks, dtype=jnp.int32) - 1) * WINDOW
    )
    absolute = start_pos[:, None] + key_pos[None, :]
    allowed = ((distance >= 0) & (distance < WINDOW))[None] & (absolute >= 0)[:, None, :]
    biased = scores - slopes[:, :, None, None, None] * distance.astype(jnp.float32)
    weights = jnp.where(allowed, jnp.exp(biased), 0.0)
    denominator = (
        jnp.sum(weights, axis=-1, keepdims=True)
        + jnp.exp(head_sink_logit.reshape(key_heads, groups))[:, :, None, None, None]
    )
    attention = (weights / denominator).astype(jnp.bfloat16)
    attended = jnp.einsum(
        "hgnqk,nkhd->nqhgd", attention, value_band, preferred_element_type=jnp.float32
    )
    return attended.reshape(stream_extent, heads_here * HD).astype(jnp.bfloat16)


def linear_attention(
    gated_query, gated_keys, gated_values, fading_exponent, linear_head_gain, starting_state
):
    stream_extent = gated_query.shape[0]
    head_total = gated_query.shape[1] // LOOKUP_FEATURES
    span_count = stream_extent // SPAN
    scaled_query = gated_query.astype(jnp.float32).reshape(
        span_count, SPAN, head_total, LOOKUP_FEATURES
    ) * LOOKUP_FEATURES ** (-0.5)
    keys_wide = gated_keys.astype(jnp.float32).reshape(
        span_count, SPAN, head_total, LOOKUP_FEATURES
    )
    values_wide = gated_values.astype(jnp.float32).reshape(span_count, SPAN, head_total, DV)
    running = jnp.cumsum(
        fading_exponent.reshape(span_count, SPAN, head_total, LOOKUP_FEATURES), axis=1
    )
    span_end = running[:, -1]
    query_with_decay = scaled_query * jnp.exp(running)
    inverse_keys = keys_wide * jnp.exp(-running)
    ending_keys = keys_wide * jnp.exp(span_end[:, None] - running)
    inner = jnp.einsum("nchk,nshk->nhcs", query_with_decay, inverse_keys, precision=HIGH_PRECISION)
    lower = jnp.tril(jnp.ones((SPAN, SPAN), dtype=bool))
    inner = jnp.where(lower, inner, 0.0)
    within = jnp.einsum("nhcs,nshv->nchv", inner, values_wide, precision=HIGH_PRECISION)

    def advance(running_state, inputs):
        query_portion, key_portion, value_portion, scale_factor = inputs
        layer_output = jnp.einsum(
            "fmy,mys->fms", query_portion, running_state, precision=HIGH_PRECISION
        )
        running_state = running_state * scale_factor[..., None] + jnp.einsum(
            "gxp,gxz->xpz", key_portion, value_portion, precision=HIGH_PRECISION
        )
        return (running_state, layer_output)

    start_state = jnp.zeros((head_total, LOOKUP_FEATURES, DV), jnp.float32)
    state_end, carried = lax.scan(
        advance, start_state, (query_with_decay, ending_keys, values_wide, jnp.exp(span_end))
    )
    device_decay = jnp.exp(jnp.sum(span_end, axis=0))
    prefix_sums = jnp.cumsum(span_end, axis=0) - span_end

    def combine(earlier, later):
        return (earlier[0] * later[0], later[0][..., None] * earlier[1] + later[1])

    decay_before, state_before = prefix(
        (device_decay, state_end),
        "sp",
        combine,
        (jnp.ones_like(device_decay), jnp.zeros_like(state_end)),
    )
    incoming_rows = state_before + decay_before[..., None] * starting_state
    crossing = jnp.einsum(
        "qwso,soz->qwsz",
        query_with_decay * jnp.exp(prefix_sums)[:, None],
        incoming_rows,
        precision=HIGH_PRECISION,
    )
    flat = (within + carried + crossing).reshape(stream_extent, head_total, DV)
    normal = (
        flat * lax.rsqrt(jnp.mean(flat * flat, axis=-1, keepdims=True) + EPS) * linear_head_gain
    )
    return normal.reshape(stream_extent, head_total * DV).astype(jnp.bfloat16)


def local(
    activations,
    input_norm_gain,
    window_query_weight,
    window_key_weight,
    window_value_weight,
    linear_query_weight,
    linear_key_weight,
    linear_value_weight,
    decay_down_factor,
    decay_up_factor,
    decay_offset_bias,
    extra_fading_exponent,
    starting_state,
    head_sink_logit,
    linear_head_gain,
    window_output_weight,
    linear_output_weight,
):
    gathered = lax.all_gather(activations, "tp", axis=1, tiled=True)
    widened = gathered.astype(jnp.float32)
    normed = (
        widened
        * lax.rsqrt(jnp.mean(widened * widened, axis=1, keepdims=True) + EPS)
        * input_norm_gain
    ).astype(jnp.bfloat16)
    row_total = normed.shape[0]
    matrices = (
        window_query_weight,
        window_key_weight,
        window_value_weight,
        linear_query_weight,
        linear_key_weight,
        linear_value_weight,
    )
    segments = (
        lax.all_gather(matrices[0], "sp", axis=0, tiled=True),
        lax.all_gather(matrices[1], "sp", axis=0, tiled=True),
        lax.all_gather(matrices[2], "sp", axis=0, tiled=True),
        lax.all_gather(matrices[3], "sp", axis=0, tiled=True),
        lax.all_gather(matrices[4], "sp", axis=0, tiled=True),
        lax.all_gather(matrices[5], "sp", axis=0, tiled=True),
    )
    projected = tuple(
        (jnp.dot(normed, segment, preferred_element_type=jnp.float32) for segment in segments)
    )
    near_query, near_keys, near_values, gated_query, gated_keys, gated_values = [
        product.astype(jnp.bfloat16) for product in projected
    ]
    low_rank = jnp.dot(normed, decay_down_factor, preferred_element_type=jnp.float32).astype(
        jnp.bfloat16
    )
    attention_energies = (
        jnp.dot(low_rank, decay_up_factor, preferred_element_type=jnp.float32) + decay_offset_bias
    )
    head_total = extra_fading_exponent.shape[1]
    fading_exponent = (jax.nn.log_sigmoid(attention_energies) / FADING_SOFTNESS).reshape(
        row_total, head_total, LOOKUP_FEATURES
    ) + extra_fading_exponent[:, :, None]
    near_out = window_attention(near_query, near_keys, near_values, head_sink_logit)
    gated_out = linear_attention(
        gated_query, gated_keys, gated_values, fading_exponent, linear_head_gain, starting_state
    )
    window_full, linear_full = (
        lax.all_gather(window_output_weight, "sp", axis=1, tiled=True),
        lax.all_gather(linear_output_weight, "sp", axis=1, tiled=True),
    )
    return lax.psum_scatter(
        (
            jnp.dot(near_out, window_full, preferred_element_type=jnp.float32)
            + jnp.dot(gated_out, linear_full, preferred_element_type=jnp.float32)
        ).astype(jnp.bfloat16),
        "tp",
        scatter_dimension=0,
        tiled=True,
    )


def _pairs(peers, depths, core):
    out = []
    for d in depths:
        out.append((d * 2 + core, (d + 1) * 2 + core))
        out.append(((peers - 1 - d) * 2 + 1 - core, (peers - 2 - d) * 2 + 1 - core))
    return out


SWAP = [(0, 1), (1, 0)]
VMEM = pl.BlockSpec(memory_space=pltpu.VMEM)
SMEM = pl.BlockSpec(memory_space=pltpu.SMEM)
ANY = pl.BlockSpec(memory_space=pl.ANY)
BY_COLUMNS = (((1,), (1,)), ((), ()))
BY_ROWS = (((0,), (0,)), ((), ()))


def _call(kernel, out_shape, flops, moved, **kw):
    return pl.pallas_call(
        kernel,
        out_shape=out_shape,
        compiler_params=pltpu.CompilerParams(vmem_limit_bytes=58 * 1024 * 1024),
        cost_estimate=pl.CostEstimate(flops=flops, bytes_accessed=moved, transcendentals=0),
        **kw,
    )


def _prefetch(scalars, grid, in_specs, out_specs, scratch=()):
    return pltpu.PrefetchScalarGridSpec(
        num_scalar_prefetch=scalars, grid=grid, in_specs=in_specs, out_specs=out_specs, scratch_shapes=scratch
    )


def norm_kernel(place_ref, x_ref, fade_ref, mate_ref, gain_ref, down_ref, *out_refs):
    me, line = place_ref[0], place_ref[3]
    pieces = len(out_refs)
    rows, wide = out_refs[0].shape
    half_model = x_ref.shape[1]
    cut = 2 * half_model // pieces
    fades = fade_ref.shape[1]
    own = x_ref[pl.ds(pl.multiple_of(me * rows, rows), rows), :].astype(jnp.float32)
    mate = mate_ref[:, :half_model].astype(jnp.float32)
    square = jnp.sum(own * own, axis=1, keepdims=True) + jnp.sum(mate * mate, axis=1, keepdims=True)
    scale = lax.rsqrt(square / (2 * half_model) + EPS)
    low_rank = None
    for side, value in ((me, own), (1 - me, mate)):
        start = pl.multiple_of(side * half_model, half_model)
        normed = (value * scale * gain_ref[:, pl.ds(start, half_model)]).astype(jnp.bfloat16)
        part = jnp.dot(normed, down_ref[pl.ds(start, half_model), :], preferred_element_type=jnp.float32)
        low_rank = part if low_rank is None else low_rank + part
        for k in range(pieces // 2):
            away = lax.rem(side * (pieces // 2) + k - line + pieces, pieces)
            for offset, out_ref in enumerate(out_refs):

                @pl.when(away == offset)
                def _():
                    out_ref[:, :cut] = normed[:, k * cut : (k + 1) * cut]

    mine = fade_ref[pl.ds(pl.multiple_of(me * rows, rows), rows), :]
    theirs = mate_ref[:, half_model : half_model + fades]
    tail = jnp.concatenate(
        [
            low_rank.astype(jnp.bfloat16).astype(jnp.float32),
            jnp.where(me == 0, mine, theirs).astype(jnp.float32),
            jnp.where(me == 0, theirs, mine).astype(jnp.float32),
            jnp.zeros((rows, wide - cut - low_rank.shape[1] - 2 * fades), jnp.float32),
        ],
        axis=1,
    ).astype(jnp.bfloat16)
    for out_ref in out_refs:
        out_ref[:, cut:] = tail


def collect_kernel(place_ref, *refs):
    pieces = len(refs) - 1
    for offset in range(pieces):
        refs[-1][lax.rem(place_ref[3] - offset + pieces, pieces)] = refs[offset][...]


def collect(place, parts):
    rows, wide = parts[0].shape
    return _call(
        collect_kernel,
        jax.ShapeDtypeStruct((len(parts), rows, wide), parts[0].dtype),
        10**8,
        2**21,
        in_specs=[SMEM] + [VMEM] * len(parts),
        out_specs=VMEM,
    )(place, *parts)


def join_kernel(place_ref, kept_ref, given_ref, *out_refs):
    pieces = len(out_refs)
    rows = out_refs[0].shape[0]
    for offset, out_ref in enumerate(out_refs):
        at = pl.ds(pl.multiple_of(lax.rem(place_ref[3] + offset, pieces) * rows, rows), rows)
        out_ref[...] = (kept_ref[at].astype(jnp.float32) + given_ref[at].astype(jnp.float32)).astype(out_ref.dtype)


def join(place, kept, given, pieces):
    rows, columns = kept.shape
    return _call(
        join_kernel,
        [jax.ShapeDtypeStruct((rows // pieces, columns), kept.dtype)] * pieces,
        10**8,
        2**21,
        in_specs=[SMEM, VMEM, VMEM],
        out_specs=[VMEM] * pieces,
    )(place, kept, given)


def spread_kernel(place_ref, *refs):
    pieces = len(refs) - 1
    columns = refs[0].shape[1]
    for offset in range(pieces):
        start = lax.rem(place_ref[3] - offset + pieces, pieces) * columns
        refs[-1][:, pl.ds(pl.multiple_of(start, columns), columns)] = refs[offset][...]


def spread(place, parts):
    rows, columns = parts[0].shape
    return _call(
        spread_kernel,
        jax.ShapeDtypeStruct((rows, len(parts) * columns), parts[0].dtype),
        10**8,
        2**21,
        in_specs=[SMEM] + [VMEM] * len(parts),
        out_specs=VMEM,
    )(place, *parts)


def to_offsets(parts):
    peers = len(parts)
    out = [parts[0]]
    for k in range(1, peers):
        out.append(lax.ppermute(parts[k], "sp", [(i, (i + k) % peers) for i in range(peers)]))
    return out


def pack_kernel(key_heads, side_ref, wq, wk, wv, lq, lk, lv, out_ref):
    step = pl.program_id(0)
    half = out_ref.shape[2] // 2
    keys_and_values = step == 0
    queries = (step > 0) & (step <= key_heads)
    head_items = (step > key_heads) & ((step - key_heads) % 2 == 1)
    head_values = (step > key_heads) & ((step - key_heads) % 2 == 0)

    @pl.when(keys_and_values)
    def _():
        out_ref[0, :, :half] = wk[...]
        out_ref[0, :, half:] = wv[...]

    @pl.when(queries)
    def _():
        out_ref[0] = wq[...]

    @pl.when(head_items)
    def _():
        out_ref[0, :, :half] = lq[...]
        out_ref[0, :, half:] = lk[...]

    @pl.when(head_values)
    def _():
        out_ref[0] = lv[...]


def pack_items(side, lin, key_heads, matrices):
    depth = matrices[0].shape[0]
    width = 2 * LOOKUP_FEATURES
    count = 1 + key_heads + 2 * lin
    fixed = pl.BlockSpec((depth, width // 2), lambda i, side: (0, side[0]))
    query = pl.BlockSpec(
        (depth, width), lambda i, side: (0, side[0] * key_heads + jnp.clip(i - 1, 0, key_heads - 1))
    )
    head = lambda i, side: (0, side[0] * lin + jnp.clip((i - 1 - key_heads) // 2, 0, lin - 1))
    narrow, full = pl.BlockSpec((depth, width // 2), head), pl.BlockSpec((depth, width), head)
    return _call(
        functools.partial(pack_kernel, key_heads),
        jax.ShapeDtypeStruct((count, depth, width), jnp.bfloat16),
        10**9,
        4 * count * depth * width,
        grid_spec=_prefetch(
            1,
            (count,),
            [query, fixed, fixed, narrow, narrow, full],
            pl.BlockSpec((1, depth, width), lambda i, side: (i, 0, 0)),
        ),
    )(side, *matrices)


def partial_kernel(index_ref, mine_ref, theirs_ref, own_ref, other_ref, *rest):
    out_ref = rest[-1]
    width = own_ref.shape[-1]
    rows = mine_ref.shape[0]
    for top, x_ref in enumerate((mine_ref, theirs_ref)):
        for half, weight in enumerate((own_ref, other_ref)):
            at = slice(top * rows, (top + 1) * rows)
            span = slice(half * width, (half + 1) * width)
            total = jnp.dot(x_ref[...], weight[0], preferred_element_type=jnp.float32)
            if len(rest) == 2:
                total = total + rest[0][at, span].astype(jnp.float32)
            out_ref[at, span] = total.astype(out_ref.dtype)


def partial_sum(index, mine, theirs, own, other, arrived):
    rows = mine.shape[0]
    _, depth, width = own.shape
    operands = [mine, theirs, own, other] + ([] if arrived is None else [arrived])
    whole = pl.BlockSpec((2 * rows, 2 * width), lambda i, index: (0, 0))
    tokens = pl.BlockSpec((rows, depth), lambda i, index: (0, 0))
    block = pl.BlockSpec((1, depth, width), lambda i, index: (index[0], 0, 0))
    return _call(
        partial_kernel,
        jax.ShapeDtypeStruct((2 * rows, 2 * width), jnp.bfloat16),
        8 * rows * depth * width,
        4 * depth * (rows + width),
        grid_spec=_prefetch(
            1, (1,), [tokens, tokens, block, block] + ([] if arrived is None else [whole]), whole
        ),
    )(index, *operands)


def decay_kernel(lin, rank, place_ref, mine_ref, theirs_ref, own_ref, other_ref, out_ref):
    me, side = place_ref[0], place_ref[1]
    rows = mine_ref.shape[0]
    features = LOOKUP_FEATURES
    lower = (
        lax.broadcasted_iota(jnp.int32, (SPAN, SPAN), 0) >= lax.broadcasted_iota(jnp.int32, (SPAN, SPAN), 1)
    ).astype(jnp.bfloat16)
    for top, tail_ref in enumerate((mine_ref, theirs_ref)):
        tail = tail_ref[...]
        low_rank = tail[:, :rank]
        parts = [
            tail[:, rank + k * 2 * lin : rank + (k + 1) * 2 * lin].astype(jnp.float32) for k in range(6)
        ]
        by_core = [parts[0] + parts[1] + parts[2], parts[3] + parts[4] + parts[5]]
        fades = [jnp.where(me == 0, by_core[0], by_core[1]), jnp.where(me == 0, by_core[1], by_core[0])]
        for head in range(lin):
            for owner, small_ref in enumerate((own_ref, other_ref)):
                at = pl.ds(pl.multiple_of((side * lin + head) * features, features), features)
                up = small_ref[:rank, at].astype(jnp.bfloat16)
                energy = jnp.dot(low_rank, up, preferred_element_type=jnp.float32) + small_ref[rank : rank + 1, at]
                soft = jnp.minimum(energy, 0.0) - jnp.log1p(jnp.exp(-jnp.abs(energy)))
                both = fades[owner]
                fade = jnp.where(side == 0, both[:, head : head + 1], both[:, lin + head : lin + head + 1])
                step = soft * (1.0 / FADING_SOFTNESS) + fade
                high = step.astype(jnp.bfloat16)
                rest = step - high.astype(jnp.float32)
                middle = rest.astype(jnp.bfloat16)
                low = (rest - middle.astype(jnp.float32)).astype(jnp.bfloat16)
                column = (2 * head + owner) * features
                for span in range(rows // SPAN):
                    cut = slice(span * SPAN, (span + 1) * SPAN)
                    out_ref[top * rows + span * SPAN : top * rows + (span + 1) * SPAN, column : column + features] = (
                        jnp.dot(lower, high[cut], preferred_element_type=jnp.float32)
                        + jnp.dot(lower, middle[cut], preferred_element_type=jnp.float32)
                        + jnp.dot(lower, low[cut], preferred_element_type=jnp.float32)
                    )


def decay_sums(place, lin, rank, mine, theirs, own, other):
    rows, wide = mine.shape
    lanes = LOOKUP_FEATURES
    tail = pl.BlockSpec((rows, lanes), lambda i, place: (0, wide // lanes - 1))
    whole = lambda shape: pl.BlockSpec(shape, lambda i, place: (0, 0))
    out = (2 * rows, 2 * lin * LOOKUP_FEATURES)
    return _call(
        functools.partial(decay_kernel, lin, rank),
        jax.ShapeDtypeStruct(out, jnp.float32),
        10**9,
        2**20,
        grid_spec=_prefetch(
            1, (1,), [tail, tail, whole(own.shape), whole(other.shape)], whole(out)
        ),
    )(place, mine, theirs, own, other)


def linear_kernel(lin, head, half, place_ref, query_key_ref, value_ref, running_ref, own_ref, other_ref, gain_ref, out_ref):
    me, side = place_ref[0], place_ref[1]
    rows, width = query_key_ref.shape
    features = LOOKUP_FEATURES
    values = width // 2
    lower = lax.broadcasted_iota(jnp.int32, (SPAN, SPAN), 0) >= lax.broadcasted_iota(
        jnp.int32, (SPAN, SPAN), 1
    )
    states = [state_ref[side * lin + head].T for state_ref in (own_ref, other_ref)]
    for span in range(rows // SPAN):
        per = half // SPAN
        device, inside = span // (2 * per), span % (2 * per)
        apart = jnp.where(me == inside // per, 0, rows // 2)
        at = pl.ds(pl.multiple_of(apart + device * half + (inside % per) * SPAN, SPAN), SPAN)
        for owner in range(2):
            base = owner * values
            running = running_ref[at, owner * features : (owner + 1) * features]
            query = query_key_ref[at, base : base + features].astype(jnp.float32)
            key = query_key_ref[at, base + features : base + 2 * features].astype(jnp.float32)
            value = value_ref[at, base : base + values]
            end = running[SPAN - 1 : SPAN]
            scaled = (query * features ** (-0.5) * jnp.exp(running)).astype(jnp.bfloat16)
            inverse = (key * jnp.exp(-running)).astype(jnp.bfloat16)
            ending = (key * jnp.exp(end - running)).astype(jnp.bfloat16)
            inner = lax.dot_general(scaled, inverse, BY_COLUMNS, preferred_element_type=jnp.float32)
            inner = jnp.where(lower, inner, 0.0).astype(jnp.bfloat16)
            state = states[owner]
            raw = jnp.dot(inner, value, preferred_element_type=jnp.float32) + lax.dot_general(
                scaled, state.astype(jnp.bfloat16), BY_COLUMNS, preferred_element_type=jnp.float32
            )
            states[owner] = state * jnp.exp(end) + lax.dot_general(
                value, ending, BY_ROWS, preferred_element_type=jnp.float32
            )
            scale = lax.rsqrt(jnp.mean(raw * raw, axis=-1, keepdims=True) + EPS)
            out_ref[at, base : base + values] = (raw * scale * gain_ref[...]).astype(out_ref.dtype)


def linear_heads(place, lin, head, half, query_key, value, running, own, other, gain):
    rows, width = query_key.shape
    whole = lambda a: pl.BlockSpec(a.shape, lambda i, place: (0,) * a.ndim)
    block = pl.BlockSpec((rows, 2 * LOOKUP_FEATURES), lambda i, place: (0, head))
    return _call(
        functools.partial(linear_kernel, lin, head, half),
        jax.ShapeDtypeStruct((rows, width), jnp.bfloat16),
        2 * 10**9,
        2**21,
        grid_spec=_prefetch(
            1,
            (1,),
            [whole(query_key), whole(value), block, whole(own), whole(other), whole(gain)],
            pl.BlockSpec((rows, width), lambda i, place: (0, 0)),
        ),
    )(place, query_key, value, running, own, other, gain)


def window_kernel(group, half, place_ref, slope_ref, sink_ref, key_value_ref, query_ref, out_ref):
    me = place_ref[0]
    rows = query_ref.shape[0]
    owners, groups = slope_ref.shape
    pair = key_value_ref.shape[1] // (2 * owners)
    from_query = lax.broadcasted_iota(jnp.int32, (WINDOW, WINDOW), 0)
    from_key = lax.broadcasted_iota(jnp.int32, (WINDOW, WINDOW), 1)
    present = from_key <= from_query
    distance = jnp.where(present, from_query - from_key, from_query - from_key + WINDOW).astype(jnp.float32)
    unit = min(half, WINDOW)

    def places(block):
        out = []
        for piece in range(WINDOW // unit):
            start = block * WINDOW + piece * unit
            device, inside = start // (2 * half), start % (2 * half)
            apart = jnp.where(me == inside // half, 0, rows // 2)
            out.append(pl.ds(pl.multiple_of(apart + device * half + inside % half, unit), unit))
        return out

    for owner in range(owners):
        key_at = owner * 2 * pair + group * HD
        value_at = key_at + pair
        base = owner * groups * HD
        biases = [slope_ref[owner, head] * distance for head in range(groups)]
        past_keys, past_values = None, None
        for block in range(rows // WINDOW):
            first = block == 0
            at = places(block)
            keys = jnp.concatenate([key_value_ref[a, key_at : key_at + HD] for a in at], axis=0)
            values = jnp.concatenate([key_value_ref[a, value_at : value_at + HD] for a in at], axis=0)
            band_keys = keys if first else jnp.concatenate([past_keys, keys], axis=0)
            band_values = values if first else jnp.concatenate([past_values, values], axis=0)
            past_keys, past_values = keys, values
            queries = jnp.concatenate(
                [query_ref[a, base + head * HD : base + (head + 1) * HD] for head in range(groups) for a in at],
                axis=0,
            )
            scores = lax.dot_general(queries, band_keys, BY_COLUMNS, preferred_element_type=jnp.float32)
            probs = []
            for head in range(groups):
                mine = scores[head * WINDOW : (head + 1) * WINDOW]
                if first:
                    weight = jnp.where(present, jnp.exp(mine * HD ** (-0.5) - biases[head]), 0.0)
                else:
                    score = jnp.where(present, mine[:, WINDOW:], mine[:, :WINDOW])
                    weight = jnp.exp(score * HD ** (-0.5) - biases[head])
                total = jnp.sum(weight, axis=-1, keepdims=True) + sink_ref[owner, head]
                share = weight / total
                if first:
                    probs.append(share.astype(jnp.bfloat16))
                else:
                    probs.append(
                        jnp.concatenate(
                            [
                                jnp.where(present, 0.0, share).astype(jnp.bfloat16),
                                jnp.where(present, share, 0.0).astype(jnp.bfloat16),
                            ],
                            axis=1,
                        )
                    )
            outs = jnp.dot(jnp.concatenate(probs, axis=0), band_values, preferred_element_type=jnp.float32)
            joined = jnp.concatenate(
                [outs[head * WINDOW : (head + 1) * WINDOW] for head in range(groups)], axis=1
            ).astype(out_ref.dtype)
            for piece, a in enumerate(at):
                out_ref[a, base : base + groups * HD] = joined[piece * unit : (piece + 1) * unit]


def window_heads(place, group, half, slopes, sinks, key_value, query):
    return _call(
        functools.partial(window_kernel, group, half),
        jax.ShapeDtypeStruct(query.shape, jnp.bfloat16),
        2 * 10**9,
        2**21,
        in_specs=[SMEM, SMEM, SMEM, VMEM, VMEM],
        out_specs=VMEM,
    )(place, slopes, sinks, key_value, query)


def output_kernel(sources, place_ref, *refs):
    count = 1 + max(max(row) for row in sources)
    pieces = len(sources)
    passed = refs[:count]
    own_ref, other_ref = refs[count : count + 2]
    held, arrival = refs[-2:]
    rest = refs[count + 2 : -2]
    split = rest[-1].shape[0] != held.shape[1]
    outs = rest[-2:] if split else rest[-1:]
    before = rest[: len(rest) - len(outs)]
    depth = place_ref[2]
    for at in range(len(sources[0])):

        @pl.when(depth == at)
        def _():
            for piece in range(pieces):
                pltpu.make_async_copy(passed[sources[piece][at]], held.at[piece], arrival.at[piece]).start()

    for piece in range(pieces):
        pltpu.make_async_copy(passed[0], held.at[piece], arrival.at[piece]).wait()
    width = held.shape[2] // 2
    rows = outs[0].shape[0]
    columns = outs[0].shape[1]
    block = columns // 2
    for top, out_ref in enumerate(outs):
        at = slice(top * rows, (top + 1) * rows)
        for part in range(2):
            span = slice(part * block, (part + 1) * block)
            total = before[0][at, span] if before else jnp.zeros((rows, block), jnp.float32)
            for piece in range(pieces):
                lines = slice(piece * width, (piece + 1) * width)
                total = total + jnp.dot(
                    held[piece, at, :width], own_ref[lines, span], preferred_element_type=jnp.float32
                )
                total = total + jnp.dot(
                    held[piece, at, width:], other_ref[lines, span], preferred_element_type=jnp.float32
                )
            out_ref[:, span] = total.astype(out_ref.dtype)


def output_sum(place, passed, sources, own, other, before, split):
    rows, width = passed[0].shape
    pieces = len(sources)
    lines, columns = other.shape
    kind, parts = (jnp.bfloat16, 2) if split else (jnp.float32, 1)
    whole = pl.BlockSpec((rows, columns), lambda i, place: (0, 0))
    out = pl.BlockSpec((rows // parts, columns), lambda i, place: (0, 0))
    return _call(
        functools.partial(output_kernel, sources),
        [jax.ShapeDtypeStruct((rows // parts, columns), kind)] * parts,
        4 * rows * columns * lines,
        8 * rows * columns,
        grid_spec=_prefetch(
            1,
            (1,),
            [ANY] * len(passed)
            + [
                pl.BlockSpec((lines, columns), lambda i, place: (place[1], 0)),
                pl.BlockSpec((lines, columns), lambda i, place: (0, 0)),
            ]
            + ([] if before is None else [whole]),
            [out] * parts,
            [pltpu.VMEM((pieces, rows, width), jnp.bfloat16), pltpu.SemaphoreType.DMA((pieces,))],
        ),
    )(place, *passed, own, other, *([] if before is None else [before]))


def resident(
    activations,
    input_norm_gain,
    window_query_weight,
    window_key_weight,
    window_value_weight,
    linear_query_weight,
    linear_key_weight,
    linear_value_weight,
    decay_down_factor,
    decay_up_factor,
    decay_offset_bias,
    extra_fading_exponent,
    starting_state,
    head_sink_logit,
    linear_head_gain,
    window_output_weight,
    linear_output_weight,
):
    peers = lax.axis_size("sp")
    hops = peers - 1
    line, me = lax.axis_index("sp"), lax.axis_index("tp")
    depth = jnp.where(me == 0, line, hops - line)
    far, near = 1 - me, me
    place = jnp.stack([me, far, hops - depth, line]).astype(jnp.int32)
    rows, half_model = activations.shape
    half = rows // 2
    bf16, f32 = jnp.bfloat16, jnp.float32
    lin = extra_fading_exponent.shape[1] // 2
    key_heads = window_key_weight.shape[1] // HD // 2
    query_heads = window_query_weight.shape[1] // HD // 2
    groups = query_heads // key_heads
    rank = decay_down_factor.shape[1]
    swap = lambda value: lax.ppermute(value, "tp", SWAP)

    high = lax.reduce_precision(extra_fading_exponent, 8, 7)
    rest = extra_fading_exponent - high
    middle = lax.reduce_precision(rest, 8, 7)
    fade = jnp.concatenate([high, middle, rest - middle], axis=1).astype(bf16)
    message = jnp.concatenate([activations, fade], axis=1)
    message = jnp.pad(message, ((0, 0), (0, LOOKUP_FEATURES - fade.shape[1])))
    mate = swap(lax.dynamic_slice_in_dim(message, far * half, half, axis=0))
    wide = 2 * half_model // peers + LOOKUP_FEATURES
    outgoing = _call(
        norm_kernel,
        [jax.ShapeDtypeStruct((half, wide), bf16)] * peers,
        10**9,
        2**21,
        in_specs=[SMEM] + [VMEM] * 5,
        out_specs=[VMEM] * peers,
    )(place, activations, fade, mate, input_norm_gain.reshape(1, -1), decay_down_factor)

    (
        outgoing,
        matrices,
        window_output_weight,
        linear_output_weight,
        starting_state,
        decay_up_factor,
        decay_offset_bias,
        head_sink_logit,
    ) = lax.optimization_barrier(
        (
            outgoing,
            (
                window_query_weight,
                window_key_weight,
                window_value_weight,
                linear_query_weight,
                linear_key_weight,
                linear_value_weight,
            ),
            window_output_weight,
            linear_output_weight,
            starting_state,
            decay_up_factor,
            decay_offset_bias,
            head_sink_logit,
        )
    )
    incoming = to_offsets(outgoing)
    packed = pack_items(near.reshape(1), lin, key_heads, matrices)
    other_in = swap(packed)
    own_in = pack_items(far.reshape(1), lin, key_heads, matrices)
    features = decay_up_factor.shape[1]
    own_small = jnp.concatenate(
        [
            decay_up_factor.astype(f32),
            decay_offset_bias.reshape(1, features),
            jnp.pad(head_sink_logit, (0, features - head_sink_logit.shape[0])).reshape(1, features),
            jnp.zeros((6, features), f32),
        ],
        axis=0,
    )
    other_small = swap(own_small)
    other_state = swap(starting_state)
    lines = linear_output_weight.shape[0] // 2
    other_linear = swap(lax.dynamic_slice_in_dim(linear_output_weight, near * lines, lines, axis=0))
    lines = window_output_weight.shape[0] // 2
    other_window = swap(lax.dynamic_slice_in_dim(window_output_weight, near * lines, lines, axis=0))

    incoming = collect(place, incoming)
    mine = incoming.reshape(peers * half, wide)
    theirs = swap(incoming).reshape(peers * half, wide)

    count = 1 + key_heads + 2 * lin
    arrived, finals = {}, []
    for step in range(count + 2 * hops):
        index = jnp.clip(step - 2 * depth, 0, count - 1).astype(jnp.int32).reshape(1)
        value = partial_sum(index, mine, theirs, own_in, other_in, arrived.get(step - 2))
        depths = [d for d in range(hops) if 0 <= step - 2 * d < count]
        if depths:
            arrived[step] = lax.ppermute(value, ("sp", "tp"), _pairs(peers, depths, 0))
        if step >= 2 * hops:
            finals.append(value)

    running = decay_sums(place, lin, rank, mine, theirs, own_small, other_small)
    sinks = jnp.stack(
        [
            lax.dynamic_slice_in_dim(small[rank + 1], far * query_heads, query_heads).reshape(key_heads, groups)
            for small in (own_small, other_small)
        ]
    )
    sinks = jnp.exp(sinks)
    attended = []
    for group in range(key_heads):
        number = jnp.stack([me, 1 - me])[:, None] * (2 * query_heads) + (
            far * query_heads + group * groups + jnp.arange(groups, dtype=jnp.int32)
        )
        slopes = jnp.exp2(-8.0 * (number + 1).astype(f32) / QH)
        attended.append(
            window_heads(place, group, half, slopes, sinks[:, group], finals[0], finals[1 + group])
        )
    for head in range(lin):
        first = 1 + key_heads + 2 * head
        attended.append(
            linear_heads(
                place,
                lin,
                head,
                half,
                finals[first],
                finals[first + 1],
                running,
                starting_state,
                other_state,
                linear_head_gain.reshape(1, DV),
            )
        )

    pieces = len(attended)
    held = []
    for piece in range(pieces):
        seen = [attended[piece]]
        for hop in range(hops):
            if piece < pieces - 1:
                seen.append(lax.ppermute(seen[-1], ("sp", "tp"), _pairs(peers, [hop], 1)))
            else:
                last = hops - hop
                straight = [(hops * 2, (hops - last) * 2), (1, last * 2 + 1)]
                seen.insert(1, lax.ppermute(seen[0], ("sp", "tp"), straight))
        held.append(seen)
    table = lambda count: tuple(tuple(range(k * peers, (k + 1) * peers)) for k in range(count))
    flat = lambda lists: [value for seen in lists for value in seen]
    (terms,) = output_sum(
        place, flat(held[:key_heads]), table(key_heads), window_output_weight, other_window, None, False
    )
    kept, given = output_sum(
        place, flat(held[key_heads:]), table(lin), linear_output_weight, other_linear, terms, True
    )

    return spread(place, to_offsets(join(place, kept, swap(given), peers)))


def fits(mesh):
    return mesh.shape["tp"] == 2 and mesh.shape["sp"] > 1


def solution(mesh):
    placed = (
        P(("fs", "sp"), "tp"),
        P(),
        P("sp", "tp"),
        P("sp", "tp"),
        P("sp", "tp"),
        P("sp", "tp"),
        P("sp", "tp"),
        P("sp", "tp"),
        P(),
        P(None, "tp"),
        P("tp"),
        P(("fs", "sp"), "tp"),
        P("tp", None, None),
        P("tp"),
        P(),
        P("tp", "sp"),
        P("tp", "sp"),
    )
    if not fits(mesh):
        return jax.shard_map(
            local, mesh=mesh, in_specs=placed, out_specs=P(("fs", "sp", "tp"), None), check_vma=False
        )

    return jax.shard_map(resident, mesh=mesh, in_specs=placed, out_specs=P(("fs", "sp", "tp"), None), check_vma=False)
```

```python
import functools

import jax
import jax.numpy as jnp
from jax import lax
from jax.experimental import pallas as pl
from jax.experimental.pallas import tpu as pltpu
from jax.sharding import PartitionSpec as P


QH = 32
HD = 64
WINDOW = 128
LOOKUP_FEATURES = 128
DV = 256
SPAN = 64


EPS = 1e-05
FADING_SOFTNESS = 16.0
HIGH_PRECISION = lax.Precision.HIGHEST


def passed_along(value, axis, steps):
    count = lax.axis_size(axis)
    leading, last = (max(0, -steps), min(count, count - steps))
    return lax.ppermute(value, axis, [(source, source + steps) for source in range(leading, last)])


def prefix(x, axis, combine, identity):
    peers, place = (lax.axis_size(axis), lax.axis_index(axis))
    everything = jax.tree.map(
        lambda part, kind: lax.all_gather(part.astype(kind), axis), x, (jnp.bfloat16, jnp.bfloat16)
    )
    start = jax.tree.map(
        lambda part, zero: jnp.broadcast_to(jnp.asarray(zero, part.dtype), part.shape), x, identity
    )

    def hop(k, before):
        reached = k < place
        new = combine(
            before, jax.tree.map(lambda part, own: part[k].astype(own.dtype), everything, x)
        )
        return jax.tree.map(lambda a, b: jnp.where(reached, a, b), new, before)

    return lax.fori_loop(0, peers, hop, start)


def window_attention(near_query, near_keys, near_values, head_sink_logit):
    stream_extent = near_query.shape[0]
    key_heads = near_keys.shape[1] // HD
    heads_here = near_query.shape[1] // HD
    groups = heads_here // key_heads
    blocks = stream_extent // WINDOW
    tail_rows = jnp.stack([near_keys, near_values])
    before = passed_along(tail_rows, "sp", 1)

    def banded(previous, current):
        extended = jnp.concatenate([previous, current], axis=0)
        earlier = extended[:stream_extent].reshape(blocks, WINDOW, key_heads, HD)
        present = extended[WINDOW:].reshape(blocks, WINDOW, key_heads, HD)
        return jnp.concatenate([earlier, present], axis=1)

    key_band = banded(before[0], near_keys)
    value_band = banded(before[1], near_values)
    queries = near_query.reshape(blocks, WINDOW, key_heads, groups, HD)
    scores = jnp.einsum(
        "nqhgd,nkhd->hgnqk", queries, key_band, preferred_element_type=jnp.float32
    ) * HD ** (-0.5)
    head_ids = lax.axis_index("tp") * heads_here + jnp.arange(heads_here, dtype=jnp.int32)
    slopes = jnp.exp2(-8.0 * (head_ids + 1).astype(jnp.float32) / QH).reshape(key_heads, groups)
    query_pos = jnp.arange(WINDOW, dtype=jnp.int32)
    key_pos = jnp.arange(2 * WINDOW, dtype=jnp.int32)
    distance = query_pos[:, None] - key_pos[None, :] + WINDOW
    start_pos = (
        lax.axis_index("sp") * stream_extent + (jnp.arange(blocks, dtype=jnp.int32) - 1) * WINDOW
    )
    absolute = start_pos[:, None] + key_pos[None, :]
    allowed = ((distance >= 0) & (distance < WINDOW))[None] & (absolute >= 0)[:, None, :]
    biased = scores - slopes[:, :, None, None, None] * distance.astype(jnp.float32)
    weights = jnp.where(allowed, jnp.exp(biased), 0.0)
    denominator = (
        jnp.sum(weights, axis=-1, keepdims=True)
        + jnp.exp(head_sink_logit.reshape(key_heads, groups))[:, :, None, None, None]
    )
    attention = (weights / denominator).astype(jnp.bfloat16)
    attended = jnp.einsum(
        "hgnqk,nkhd->nqhgd", attention, value_band, preferred_element_type=jnp.float32
    )
    return attended.reshape(stream_extent, heads_here * HD).astype(jnp.bfloat16)


def linear_attention(
    gated_query, gated_keys, gated_values, fading_exponent, linear_head_gain, starting_state
):
    stream_extent = gated_query.shape[0]
    head_total = gated_query.shape[1] // LOOKUP_FEATURES
    span_count = stream_extent // SPAN
    scaled_query = gated_query.astype(jnp.float32).reshape(
        span_count, SPAN, head_total, LOOKUP_FEATURES
    ) * LOOKUP_FEATURES ** (-0.5)
    keys_wide = gated_keys.astype(jnp.float32).reshape(
        span_count, SPAN, head_total, LOOKUP_FEATURES
    )
    values_wide = gated_values.astype(jnp.float32).reshape(span_count, SPAN, head_total, DV)
    running = jnp.cumsum(
        fading_exponent.reshape(span_count, SPAN, head_total, LOOKUP_FEATURES), axis=1
    )
    span_end = running[:, -1]
    query_with_decay = scaled_query * jnp.exp(running)
    inverse_keys = keys_wide * jnp.exp(-running)
    ending_keys = keys_wide * jnp.exp(span_end[:, None] - running)
    inner = jnp.einsum("nchk,nshk->nhcs", query_with_decay, inverse_keys, precision=HIGH_PRECISION)
    lower = jnp.tril(jnp.ones((SPAN, SPAN), dtype=bool))
    inner = jnp.where(lower, inner, 0.0)
    within = jnp.einsum("nhcs,nshv->nchv", inner, values_wide, precision=HIGH_PRECISION)

    def advance(running_state, inputs):
        query_portion, key_portion, value_portion, scale_factor = inputs
        layer_output = jnp.einsum(
            "fmy,mys->fms", query_portion, running_state, precision=HIGH_PRECISION
        )
        running_state = running_state * scale_factor[..., None] + jnp.einsum(
            "gxp,gxz->xpz", key_portion, value_portion, precision=HIGH_PRECISION
        )
        return (running_state, layer_output)

    start_state = jnp.zeros((head_total, LOOKUP_FEATURES, DV), jnp.float32)
    state_end, carried = lax.scan(
        advance, start_state, (query_with_decay, ending_keys, values_wide, jnp.exp(span_end))
    )
    device_decay = jnp.exp(jnp.sum(span_end, axis=0))
    prefix_sums = jnp.cumsum(span_end, axis=0) - span_end

    def combine(earlier, later):
        return (earlier[0] * later[0], later[0][..., None] * earlier[1] + later[1])

    decay_before, state_before = prefix(
        (device_decay, state_end),
        "sp",
        combine,
        (jnp.ones_like(device_decay), jnp.zeros_like(state_end)),
    )
    incoming_rows = state_before + decay_before[..., None] * starting_state
    crossing = jnp.einsum(
        "qwso,soz->qwsz",
        query_with_decay * jnp.exp(prefix_sums)[:, None],
        incoming_rows,
        precision=HIGH_PRECISION,
    )
    flat = (within + carried + crossing).reshape(stream_extent, head_total, DV)
    normal = (
        flat * lax.rsqrt(jnp.mean(flat * flat, axis=-1, keepdims=True) + EPS) * linear_head_gain
    )
    return normal.reshape(stream_extent, head_total * DV).astype(jnp.bfloat16)


def local(
    activations,
    input_norm_gain,
    window_query_weight,
    window_key_weight,
    window_value_weight,
    linear_query_weight,
    linear_key_weight,
    linear_value_weight,
    decay_down_factor,
    decay_up_factor,
    decay_offset_bias,
    extra_fading_exponent,
    starting_state,
    head_sink_logit,
    linear_head_gain,
    window_output_weight,
    linear_output_weight,
):
    gathered = lax.all_gather(activations, "tp", axis=1, tiled=True)
    widened = gathered.astype(jnp.float32)
    normed = (
        widened
        * lax.rsqrt(jnp.mean(widened * widened, axis=1, keepdims=True) + EPS)
        * input_norm_gain
    ).astype(jnp.bfloat16)
    row_total = normed.shape[0]
    matrices = (
        window_query_weight,
        window_key_weight,
        window_value_weight,
        linear_query_weight,
        linear_key_weight,
        linear_value_weight,
    )
    segments = (
        lax.all_gather(matrices[0], "sp", axis=0, tiled=True),
        lax.all_gather(matrices[1], "sp", axis=0, tiled=True),
        lax.all_gather(matrices[2], "sp", axis=0, tiled=True),
        lax.all_gather(matrices[3], "sp", axis=0, tiled=True),
        lax.all_gather(matrices[4], "sp", axis=0, tiled=True),
        lax.all_gather(matrices[5], "sp", axis=0, tiled=True),
    )
    projected = tuple(
        (jnp.dot(normed, segment, preferred_element_type=jnp.float32) for segment in segments)
    )
    near_query, near_keys, near_values, gated_query, gated_keys, gated_values = [
        product.astype(jnp.bfloat16) for product in projected
    ]
    low_rank = jnp.dot(normed, decay_down_factor, preferred_element_type=jnp.float32).astype(
        jnp.bfloat16
    )
    attention_energies = (
        jnp.dot(low_rank, decay_up_factor, preferred_element_type=jnp.float32) + decay_offset_bias
    )
    head_total = extra_fading_exponent.shape[1]
    fading_exponent = (jax.nn.log_sigmoid(attention_energies) / FADING_SOFTNESS).reshape(
        row_total, head_total, LOOKUP_FEATURES
    ) + extra_fading_exponent[:, :, None]
    near_out = window_attention(near_query, near_keys, near_values, head_sink_logit)
    gated_out = linear_attention(
        gated_query, gated_keys, gated_values, fading_exponent, linear_head_gain, starting_state
    )
    window_full, linear_full = (
        lax.all_gather(window_output_weight, "sp", axis=1, tiled=True),
        lax.all_gather(linear_output_weight, "sp", axis=1, tiled=True),
    )
    return lax.psum_scatter(
        (
            jnp.dot(near_out, window_full, preferred_element_type=jnp.float32)
            + jnp.dot(gated_out, linear_full, preferred_element_type=jnp.float32)
        ).astype(jnp.bfloat16),
        "tp",
        scatter_dimension=0,
        tiled=True,
    )


def _pairs(peers, depths, core):
    out = []
    for d in depths:
        out.append((d * 2 + core, (d + 1) * 2 + core))
        out.append(((peers - 1 - d) * 2 + 1 - core, (peers - 2 - d) * 2 + 1 - core))
    return out


SWAP = [(0, 1), (1, 0)]
VMEM = pl.BlockSpec(memory_space=pltpu.VMEM)
SMEM = pl.BlockSpec(memory_space=pltpu.SMEM)
ANY = pl.BlockSpec(memory_space=pl.ANY)
BY_COLUMNS = (((1,), (1,)), ((), ()))
BY_ROWS = (((0,), (0,)), ((), ()))


def _call(kernel, out_shape, flops, moved, grant=24, **kw):
    return pl.pallas_call(
        kernel,
        out_shape=out_shape,
        compiler_params=pltpu.CompilerParams(vmem_limit_bytes=grant * 1024 * 1024),
        cost_estimate=pl.CostEstimate(flops=flops, bytes_accessed=moved, transcendentals=0),
        **kw,
    )


def _prefetch(scalars, grid, in_specs, out_specs, scratch=()):
    return pltpu.PrefetchScalarGridSpec(
        num_scalar_prefetch=scalars, grid=grid, in_specs=in_specs, out_specs=out_specs, scratch_shapes=scratch
    )


def message_kernel(place_ref, x_ref, fade_ref, out_ref):
    rows, wide = out_ref.shape
    half_model = x_ref.shape[1]
    at = pl.ds(pl.multiple_of(place_ref[1] * rows, rows), rows)
    out_ref[:, :half_model] = x_ref[at, :]
    out_ref[:, half_model:] = jnp.concatenate(
        [_parts(fade_ref[at, :]), jnp.zeros((rows, wide - half_model - 3 * fade_ref.shape[1]), jnp.float32)], axis=1
    ).astype(out_ref.dtype)


def _parts(value):
    high = value.astype(jnp.bfloat16).astype(jnp.float32)
    rest = value - high
    middle = rest.astype(jnp.bfloat16).astype(jnp.float32)
    return jnp.concatenate([high, middle, rest - middle], axis=1)


def norm_kernel(place_ref, x_ref, fade_ref, mate_ref, gain_ref, down_ref, *out_refs):
    me, line = place_ref[0], place_ref[3]
    pieces = len(out_refs)
    rows, wide = out_refs[0].shape
    half_model = x_ref.shape[1]
    cut = 2 * half_model // pieces
    fades = 3 * fade_ref.shape[1]
    own = x_ref[pl.ds(pl.multiple_of(me * rows, rows), rows), :].astype(jnp.float32)
    mate = mate_ref[:, :half_model].astype(jnp.float32)
    square = jnp.sum(own * own, axis=1, keepdims=True) + jnp.sum(mate * mate, axis=1, keepdims=True)
    scale = lax.rsqrt(square / (2 * half_model) + EPS)
    low_rank = None
    for side, value in ((me, own), (1 - me, mate)):
        start = pl.multiple_of(side * half_model, half_model)
        normed = (value * scale * gain_ref[:, pl.ds(start, half_model)]).astype(jnp.bfloat16)
        part = lax.dot_general(
            normed, down_ref[:, pl.ds(start, half_model)], BY_COLUMNS, preferred_element_type=jnp.float32
        )
        low_rank = part if low_rank is None else low_rank + part
        for k in range(pieces // 2):
            away = lax.rem(side * (pieces // 2) + k - line + pieces, pieces)
            for offset, out_ref in enumerate(out_refs):

                @pl.when(away == offset)
                def _():
                    out_ref[:, :cut] = normed[:, k * cut : (k + 1) * cut]

    mine = _parts(fade_ref[pl.ds(pl.multiple_of(me * rows, rows), rows), :])
    theirs = mate_ref[:, half_model : half_model + fades].astype(jnp.float32)
    tail = jnp.concatenate(
        [
            low_rank.astype(jnp.bfloat16).astype(jnp.float32),
            jnp.where(me == 0, mine, theirs),
            jnp.where(me == 0, theirs, mine),
            jnp.zeros((rows, wide - cut - low_rank.shape[1] - 2 * fades), jnp.float32),
        ],
        axis=1,
    ).astype(jnp.bfloat16)
    for out_ref in out_refs:
        out_ref[:, cut:] = tail


def collect_kernel(place_ref, *refs):
    pieces = len(refs) - 1
    for offset in range(pieces):
        refs[-1][lax.rem(place_ref[3] - offset + pieces, pieces)] = refs[offset][...]


def collect(place, parts):
    rows, wide = parts[0].shape
    return _call(
        collect_kernel,
        jax.ShapeDtypeStruct((len(parts), rows, wide), parts[0].dtype),
        10**8,
        2**21,
        in_specs=[SMEM] + [VMEM] * len(parts),
        out_specs=VMEM,
    )(place, *parts)


def join_kernel(place_ref, kept_ref, given_ref, *out_refs):
    pieces = len(out_refs)
    rows = out_refs[0].shape[0]
    for offset, out_ref in enumerate(out_refs):
        at = pl.ds(pl.multiple_of(lax.rem(place_ref[3] + offset, pieces) * rows, rows), rows)
        out_ref[...] = (kept_ref[at].astype(jnp.float32) + given_ref[at].astype(jnp.float32)).astype(out_ref.dtype)


def join(place, kept, given, pieces):
    rows, columns = kept.shape
    return _call(
        join_kernel,
        [jax.ShapeDtypeStruct((rows // pieces, columns), kept.dtype)] * pieces,
        10**8,
        2**21,
        in_specs=[SMEM, VMEM, VMEM],
        out_specs=[VMEM] * pieces,
    )(place, kept, given)


def spread_kernel(place_ref, *refs):
    pieces = len(refs) - 1
    columns = refs[0].shape[1]
    for offset in range(pieces):
        start = lax.rem(place_ref[3] - offset + pieces, pieces) * columns
        refs[-1][:, pl.ds(pl.multiple_of(start, columns), columns)] = refs[offset][...]


def spread(place, parts):
    rows, columns = parts[0].shape
    return _call(
        spread_kernel,
        jax.ShapeDtypeStruct((rows, len(parts) * columns), parts[0].dtype),
        10**8,
        2**21,
        in_specs=[SMEM] + [VMEM] * len(parts),
        out_specs=VMEM,
    )(place, *parts)


def to_offsets(parts):
    peers = len(parts)
    out = [parts[0]]
    for k in range(1, peers):
        out.append(lax.ppermute(parts[k], "sp", [(i, (i + k) % peers) for i in range(peers)]))
    return out


def pack_kernel(key_heads, side_ref, wq, wk, wv, lq, lk, lv, out_ref):
    step = pl.program_id(0)
    half = out_ref.shape[2] // 2
    keys_and_values = step == 0
    queries = (step > 0) & (step <= key_heads)
    head_items = (step > key_heads) & ((step - key_heads) % 2 == 1)
    head_values = (step > key_heads) & ((step - key_heads) % 2 == 0)

    @pl.when(keys_and_values)
    def _():
        out_ref[0, :, :half] = wk[...]
        out_ref[0, :, half:] = wv[...]

    @pl.when(queries)
    def _():
        out_ref[0] = wq[...]

    @pl.when(head_items)
    def _():
        out_ref[0, :, :half] = lq[...]
        out_ref[0, :, half:] = lk[...]

    @pl.when(head_values)
    def _():
        out_ref[0] = lv[...]


def pack_items(side, lin, key_heads, matrices):
    depth = matrices[0].shape[0]
    width = 2 * LOOKUP_FEATURES
    count = 1 + key_heads + 2 * lin
    fixed = pl.BlockSpec((depth, width // 2), lambda i, side: (0, side[0]))
    query = pl.BlockSpec(
        (depth, width), lambda i, side: (0, side[0] * key_heads + jnp.clip(i - 1, 0, key_heads - 1))
    )
    head = lambda i, side: (0, side[0] * lin + jnp.clip((i - 1 - key_heads) // 2, 0, lin - 1))
    narrow, full = pl.BlockSpec((depth, width // 2), head), pl.BlockSpec((depth, width), head)
    return _call(
        functools.partial(pack_kernel, key_heads),
        jax.ShapeDtypeStruct((count, depth, width), jnp.bfloat16),
        10**9,
        4 * count * depth * width,
        grid_spec=_prefetch(
            1,
            (count,),
            [query, fixed, fixed, narrow, narrow, full],
            pl.BlockSpec((1, depth, width), lambda i, side: (i, 0, 0)),
        ),
    )(side, *matrices)


def partial_kernel(index_ref, mine_ref, theirs_ref, own_ref, other_ref, *rest):
    out_ref = rest[-1]
    rows = mine_ref.shape[0]
    _, depth, width = own_ref.shape
    for half, source in enumerate((own_ref, other_ref)):
        weight = source[index_ref[0]]
        for top, x_ref in enumerate((mine_ref, theirs_ref)):
            at = slice(top * rows, (top + 1) * rows)
            span = slice(half * width, (half + 1) * width)
            total = jnp.dot(x_ref[:, :depth], weight, preferred_element_type=jnp.float32)
            if len(rest) == 2:
                total = total + rest[0][at, span].astype(jnp.float32)
            out_ref[at, span] = total.astype(out_ref.dtype)


def partial_sum(index, mine, theirs, own, other, arrived):
    rows = mine.shape[0]
    _, depth, width = own.shape
    operands = [mine, theirs, own, other] + ([] if arrived is None else [arrived])
    return _call(
        partial_kernel,
        jax.ShapeDtypeStruct((2 * rows, 2 * width), jnp.bfloat16),
        160 * rows * depth * width,
        4 * depth * (rows + width),
        in_specs=[SMEM] + [VMEM] * (len(operands)),
        out_specs=VMEM,
    )(index, *operands)


def decay_kernel(lin, rank, place_ref, mine_ref, theirs_ref, own_ref, other_ref, *out_refs):
    me, side = place_ref[0], place_ref[1]
    rows = mine_ref.shape[0]
    features = LOOKUP_FEATURES
    lower = (
        lax.broadcasted_iota(jnp.int32, (SPAN, SPAN), 0) >= lax.broadcasted_iota(jnp.int32, (SPAN, SPAN), 1)
    ).astype(jnp.bfloat16)
    for top, tail_ref in enumerate((mine_ref, theirs_ref)):
        tail = tail_ref[:, tail_ref.shape[1] - features :]
        low_rank = tail[:, :rank]
        parts = [
            tail[:, rank + k * 2 * lin : rank + (k + 1) * 2 * lin].astype(jnp.float32) for k in range(6)
        ]
        by_core = [parts[0] + parts[1] + parts[2], parts[3] + parts[4] + parts[5]]
        fades = [jnp.where(me == 0, by_core[0], by_core[1]), jnp.where(me == 0, by_core[1], by_core[0])]
        for head in range(lin):
            for owner, small_ref in enumerate((own_ref, other_ref)):
                at = pl.ds(pl.multiple_of((side * lin + head) * features, features), features)
                up = small_ref[:rank, at].astype(jnp.bfloat16)
                energy = jnp.dot(low_rank, up, preferred_element_type=jnp.float32) + small_ref[rank : rank + 1, at]
                soft = jnp.minimum(energy, 0.0) - jnp.log1p(jnp.exp(-jnp.abs(energy)))
                both = fades[owner]
                fade = jnp.where(side == 0, both[:, head : head + 1], both[:, lin + head : lin + head + 1])
                step = soft * (1.0 / FADING_SOFTNESS) + fade
                high = step.astype(jnp.bfloat16)
                rest = step - high.astype(jnp.float32)
                middle = rest.astype(jnp.bfloat16)
                low = (rest - middle.astype(jnp.float32)).astype(jnp.bfloat16)
                column = owner * features
                out_ref = out_refs[head]
                for span in range(rows // SPAN):
                    cut = slice(span * SPAN, (span + 1) * SPAN)
                    out_ref[top * rows + span * SPAN : top * rows + (span + 1) * SPAN, column : column + features] = (
                        jnp.dot(lower, high[cut], preferred_element_type=jnp.float32)
                        + jnp.dot(lower, middle[cut], preferred_element_type=jnp.float32)
                        + jnp.dot(lower, low[cut], preferred_element_type=jnp.float32)
                    )


def decay_sums(place, lin, rank, mine, theirs, own, other):
    return _call(
        functools.partial(decay_kernel, lin, rank),
        [jax.ShapeDtypeStruct((2 * mine.shape[0], 2 * LOOKUP_FEATURES), jnp.float32)] * lin,
        10**9,
        2**20,
        in_specs=[SMEM] + [VMEM] * 4,
        out_specs=[VMEM] * lin,
    )(place, mine, theirs, own, other)


def linear_kernel(lin, head, half, place_ref, query_key_ref, value_ref, running_ref, own_ref, other_ref, gain_ref, out_ref):
    me, side = place_ref[0], place_ref[1]
    rows, width = query_key_ref.shape
    features = LOOKUP_FEATURES
    values = width // 2
    lower = lax.broadcasted_iota(jnp.int32, (SPAN, SPAN), 0) >= lax.broadcasted_iota(
        jnp.int32, (SPAN, SPAN), 1
    )
    states = [state_ref[side * lin + head].T for state_ref in (own_ref, other_ref)]
    for span in range(rows // SPAN):
        per = half // SPAN
        device, inside = span // (2 * per), span % (2 * per)
        apart = jnp.where(me == inside // per, 0, rows // 2)
        at = pl.ds(pl.multiple_of(apart + device * half + (inside % per) * SPAN, SPAN), SPAN)
        for owner in range(2):
            base = owner * values
            running = running_ref[at, owner * features : (owner + 1) * features]
            query = query_key_ref[at, base : base + features].astype(jnp.float32)
            key = query_key_ref[at, base + features : base + 2 * features].astype(jnp.float32)
            value = value_ref[at, base : base + values]
            end = running[SPAN - 1 : SPAN]
            scaled = (query * features ** (-0.5) * jnp.exp(running)).astype(jnp.bfloat16)
            inverse = (key * jnp.exp(-running)).astype(jnp.bfloat16)
            ending = (key * jnp.exp(end - running)).astype(jnp.bfloat16)
            inner = lax.dot_general(scaled, inverse, BY_COLUMNS, preferred_element_type=jnp.float32)
            inner = jnp.where(lower, inner, 0.0).astype(jnp.bfloat16)
            state = states[owner]
            raw = jnp.dot(inner, value, preferred_element_type=jnp.float32) + lax.dot_general(
                scaled, state.astype(jnp.bfloat16), BY_COLUMNS, preferred_element_type=jnp.float32
            )
            states[owner] = state * jnp.exp(end) + lax.dot_general(
                value, ending, BY_ROWS, preferred_element_type=jnp.float32
            )
            scale = lax.rsqrt(jnp.mean(raw * raw, axis=-1, keepdims=True) + EPS)
            out_ref[at, base : base + values] = (raw * scale * gain_ref[...]).astype(out_ref.dtype)


def linear_heads(place, lin, head, half, query_key, value, running, own, other, gain):
    return _call(
        functools.partial(linear_kernel, lin, head, half),
        jax.ShapeDtypeStruct(query_key.shape, jnp.bfloat16),
        2 * 10**9,
        2**21,
        in_specs=[SMEM] + [VMEM] * 6,
        out_specs=VMEM,
    )(place, query_key, value, running, own, other, gain)


def window_kernel(group, half, place_ref, slope_ref, sink_ref, key_value_ref, query_ref, out_ref):
    me = place_ref[0]
    rows = query_ref.shape[0]
    owners, groups = slope_ref.shape
    pair = key_value_ref.shape[1] // (2 * owners)
    from_query = lax.broadcasted_iota(jnp.int32, (WINDOW, WINDOW), 0)
    from_key = lax.broadcasted_iota(jnp.int32, (WINDOW, WINDOW), 1)
    present = from_key <= from_query
    distance = jnp.where(present, from_query - from_key, from_query - from_key + WINDOW).astype(jnp.float32)
    unit = min(half, WINDOW)

    def places(block):
        out = []
        for piece in range(WINDOW // unit):
            start = block * WINDOW + piece * unit
            device, inside = start // (2 * half), start % (2 * half)
            apart = jnp.where(me == inside // half, 0, rows // 2)
            out.append(pl.ds(pl.multiple_of(apart + device * half + inside % half, unit), unit))
        return out

    for owner in range(owners):
        key_at = owner * 2 * pair + group * HD
        value_at = key_at + pair
        base = owner * groups * HD
        biases = [slope_ref[owner, head] * distance for head in range(groups)]
        past_keys, past_values = None, None
        for block in range(rows // WINDOW):
            first = block == 0
            at = places(block)
            keys = jnp.concatenate([key_value_ref[a, key_at : key_at + HD] for a in at], axis=0)
            values = jnp.concatenate([key_value_ref[a, value_at : value_at + HD] for a in at], axis=0)
            band_keys = keys if first else jnp.concatenate([past_keys, keys], axis=0)
            band_values = values if first else jnp.concatenate([past_values, values], axis=0)
            past_keys, past_values = keys, values
            queries = jnp.concatenate(
                [query_ref[a, base + head * HD : base + (head + 1) * HD] for head in range(groups) for a in at],
                axis=0,
            )
            scores = lax.dot_general(queries, band_keys, BY_COLUMNS, preferred_element_type=jnp.float32)
            probs = []
            for head in range(groups):
                mine = scores[head * WINDOW : (head + 1) * WINDOW]
                if first:
                    weight = jnp.where(present, jnp.exp(mine * HD ** (-0.5) - biases[head]), 0.0)
                else:
                    score = jnp.where(present, mine[:, WINDOW:], mine[:, :WINDOW])
                    weight = jnp.exp(score * HD ** (-0.5) - biases[head])
                total = jnp.sum(weight, axis=-1, keepdims=True) + sink_ref[owner, head]
                share = weight / total
                if first:
                    probs.append(share.astype(jnp.bfloat16))
                else:
                    probs.append(
                        jnp.concatenate(
                            [
                                jnp.where(present, 0.0, share).astype(jnp.bfloat16),
                                jnp.where(present, share, 0.0).astype(jnp.bfloat16),
                            ],
                            axis=1,
                        )
                    )
            outs = jnp.dot(jnp.concatenate(probs, axis=0), band_values, preferred_element_type=jnp.float32)
            joined = jnp.concatenate(
                [outs[head * WINDOW : (head + 1) * WINDOW] for head in range(groups)], axis=1
            ).astype(out_ref.dtype)
            for piece, a in enumerate(at):
                out_ref[a, base : base + groups * HD] = joined[piece * unit : (piece + 1) * unit]


def window_heads(place, group, half, slopes, sinks, key_value, query):
    return _call(
        functools.partial(window_kernel, group, half),
        jax.ShapeDtypeStruct(query.shape, jnp.bfloat16),
        2 * 10**9,
        2**21,
        in_specs=[SMEM, SMEM, SMEM, VMEM, VMEM],
        out_specs=VMEM,
    )(place, slopes, sinks, key_value, query)


def output_kernel(sources, place_ref, *refs):
    count = 1 + max(max(row) for row in sources)
    pieces = len(sources)
    passed = refs[:count]
    own_ref, other_ref = refs[count : count + 2]
    held, arrival = refs[-2:]
    rest = refs[count + 2 : -2]
    split = rest[-1].shape[0] != held.shape[1]
    outs = rest[-2:] if split else rest[-1:]
    before = rest[: len(rest) - len(outs)]
    depth = place_ref[2]
    for at in range(len(sources[0])):

        @pl.when(depth == at)
        def _():
            for piece in range(pieces):
                pltpu.make_async_copy(passed[sources[piece][at]], held.at[piece], arrival.at[piece]).start()

    for piece in range(pieces):
        pltpu.make_async_copy(passed[0], held.at[piece], arrival.at[piece]).wait()
    width = held.shape[2] // 2
    rows = outs[0].shape[0]
    columns = outs[0].shape[1]
    block = columns // 2
    for top, out_ref in enumerate(outs):
        at = slice(top * rows, (top + 1) * rows)
        for part in range(2):
            span = slice(part * block, (part + 1) * block)
            total = before[0][at, span] if before else jnp.zeros((rows, block), jnp.float32)
            for piece in range(pieces):
                lines = slice(piece * width, (piece + 1) * width)
                total = total + jnp.dot(
                    held[piece, at, :width], own_ref[lines, span], preferred_element_type=jnp.float32
                )
                total = total + jnp.dot(
                    held[piece, at, width:], other_ref[lines, span], preferred_element_type=jnp.float32
                )
            out_ref[:, span] = total.astype(out_ref.dtype)


def output_sum(place, passed, sources, own, other, before, split):
    rows, width = passed[0].shape
    pieces = len(sources)
    lines, columns = other.shape
    kind, parts = (jnp.bfloat16, 2) if split else (jnp.float32, 1)
    whole = pl.BlockSpec((rows, columns), lambda i, place: (0, 0))
    out = pl.BlockSpec((rows // parts, columns), lambda i, place: (0, 0))
    return _call(
        functools.partial(output_kernel, sources),
        [jax.ShapeDtypeStruct((rows // parts, columns), kind)] * parts,
        4 * rows * columns * lines,
        8 * rows * columns,
        grid_spec=_prefetch(
            1,
            (1,),
            [ANY] * len(passed)
            + [
                pl.BlockSpec((lines, columns), lambda i, place: (place[1], 0)),
                pl.BlockSpec((lines, columns), lambda i, place: (0, 0)),
            ]
            + ([] if before is None else [whole]),
            [out] * parts,
            [pltpu.VMEM((pieces, rows, width), jnp.bfloat16), pltpu.SemaphoreType.DMA((pieces,))],
        ),
    )(place, *passed, own, other, *([] if before is None else [before]))


def resident(
    activations,
    input_norm_gain,
    window_query_weight,
    window_key_weight,
    window_value_weight,
    linear_query_weight,
    linear_key_weight,
    linear_value_weight,
    decay_down_factor,
    decay_up_factor,
    decay_offset_bias,
    extra_fading_exponent,
    starting_state,
    head_sink_logit,
    linear_head_gain,
    window_output_weight,
    linear_output_weight,
):
    peers = lax.axis_size("sp")
    hops = peers - 1
    line, me = lax.axis_index("sp"), lax.axis_index("tp")
    depth = jnp.where(me == 0, line, hops - line)
    far, near = 1 - me, me
    place = jnp.stack([me, far, hops - depth, line]).astype(jnp.int32)
    rows, half_model = activations.shape
    half = rows // 2
    bf16, f32 = jnp.bfloat16, jnp.float32
    lin = extra_fading_exponent.shape[1] // 2
    key_heads = window_key_weight.shape[1] // HD // 2
    query_heads = window_query_weight.shape[1] // HD // 2
    groups = query_heads // key_heads
    rank = decay_down_factor.shape[1]

    def swap(value):
        return lax.ppermute(value, "tp", SWAP)


    message = _call(
        message_kernel,
        jax.ShapeDtypeStruct((half, half_model + LOOKUP_FEATURES), bf16),
        10**8,
        2**20,
        in_specs=[SMEM, VMEM, VMEM],
        out_specs=VMEM,
    )(place, activations, extra_fading_exponent)
    mate = swap(message)
    wide = 2 * half_model // peers + LOOKUP_FEATURES
    outgoing = _call(
        norm_kernel,
        [jax.ShapeDtypeStruct((half, wide), bf16)] * peers,
        10**9,
        2**21,
        in_specs=[SMEM] + [VMEM] * 5,
        out_specs=[VMEM] * peers,
    )(place, activations, extra_fading_exponent, mate, input_norm_gain.reshape(1, -1), decay_down_factor.T)

    (
        outgoing,
        matrices,
        window_output_weight,
        linear_output_weight,
        starting_state,
        decay_up_factor,
        decay_offset_bias,
        head_sink_logit,
    ) = lax.optimization_barrier(
        (
            outgoing,
            (
                window_query_weight,
                window_key_weight,
                window_value_weight,
                linear_query_weight,
                linear_key_weight,
                linear_value_weight,
            ),
            window_output_weight,
            linear_output_weight,
            starting_state,
            decay_up_factor,
            decay_offset_bias,
            head_sink_logit,
        )
    )
    incoming = to_offsets(outgoing)
    packed = pack_items(near.reshape(1), lin, key_heads, matrices)
    other_in = swap(packed)
    own_in = pack_items(far.reshape(1), lin, key_heads, matrices)
    features = decay_up_factor.shape[1]
    own_small = jnp.concatenate(
        [
            decay_up_factor.astype(f32),
            decay_offset_bias.reshape(1, features),
            jnp.pad(head_sink_logit, (0, features - head_sink_logit.shape[0])).reshape(1, features),
            jnp.zeros((6, features), f32),
        ],
        axis=0,
    )
    other_small = swap(own_small)
    other_state = swap(starting_state)
    lines = linear_output_weight.shape[0] // 2
    other_linear = swap(lax.dynamic_slice_in_dim(linear_output_weight, near * lines, lines, axis=0))
    lines = window_output_weight.shape[0] // 2
    other_window = swap(lax.dynamic_slice_in_dim(window_output_weight, near * lines, lines, axis=0))

    incoming = collect(place, incoming)
    mine = incoming.reshape(peers * half, wide)
    theirs = swap(incoming).reshape(peers * half, wide)

    count = 1 + key_heads + 2 * lin
    arrived, finals = {}, []
    for step in range(count + 2 * hops):
        index = jnp.clip(step - 2 * depth, 0, count - 1).astype(jnp.int32).reshape(1)
        value = partial_sum(index, mine, theirs, own_in, other_in, arrived.get(step - 2))
        depths = [d for d in range(hops) if 0 <= step - 2 * d < count]
        if depths:
            arrived[step] = lax.ppermute(value, ("sp", "tp"), _pairs(peers, depths, 0))
        if step >= 2 * hops:
            finals.append(value)

    running = decay_sums(place, lin, rank, mine, theirs, own_small, other_small)
    sinks = jnp.stack(
        [
            lax.dynamic_slice_in_dim(small[rank + 1], far * query_heads, query_heads).reshape(key_heads, groups)
            for small in (own_small, other_small)
        ]
    )
    sinks = jnp.exp(sinks)
    attended = []
    for group in range(key_heads):
        number = jnp.stack([me, 1 - me])[:, None] * (2 * query_heads) + (
            far * query_heads + group * groups + jnp.arange(groups, dtype=jnp.int32)
        )
        slopes = jnp.exp2(-8.0 * (number + 1).astype(f32) / QH)
        attended.append(
            window_heads(place, group, half, slopes, sinks[:, group], finals[0], finals[1 + group])
        )
    for head in range(lin):
        first = 1 + key_heads + 2 * head
        attended.append(
            linear_heads(
                place,
                lin,
                head,
                half,
                finals[first],
                finals[first + 1],
                running[head],
                starting_state,
                other_state,
                linear_head_gain.reshape(1, DV),
            )
        )

    pieces = len(attended)
    chained = pieces - 1
    passed, back = [], None
    for step in range(chained + hops):
        if step == 0:
            now = attended[0]
        elif step < chained:
            now = jnp.where(depth == hops, attended[step], back)
        else:
            now = back
        passed.append(now)
        depths = [d for d in range(hops) if 0 <= step - d < chained]
        if depths:
            back = lax.ppermute(now, ("sp", "tp"), _pairs(peers, depths, 1))
    straight = [attended[-1]]
    for far_hop in range(hops, 0, -1):
        pairs = [(hops * 2, (hops - far_hop) * 2), (1, far_hop * 2 + 1)]
        straight.insert(1, lax.ppermute(attended[-1], ("sp", "tp"), pairs))
    (terms,) = output_sum(
        place,
        passed[: key_heads + hops],
        tuple(tuple(range(k, k + peers)) for k in range(key_heads)),
        window_output_weight,
        other_window,
        None,
        False,
    )
    late = passed[key_heads:]
    kept, given = output_sum(
        place,
        late + straight,
        tuple(tuple(range(k, k + peers)) for k in range(lin - 1)) + (tuple(len(late) + k for k in range(peers)),),
        linear_output_weight,
        other_linear,
        terms,
        True,
    )

    return spread(place, to_offsets(join(place, kept, swap(given), peers)))


def fits(mesh):
    return mesh.shape["tp"] == 2 and mesh.shape["sp"] > 1


def solution(mesh):
    placed = (
        P(("fs", "sp"), "tp"),
        P(),
        P("sp", "tp"),
        P("sp", "tp"),
        P("sp", "tp"),
        P("sp", "tp"),
        P("sp", "tp"),
        P("sp", "tp"),
        P(),
        P(None, "tp"),
        P("tp"),
        P(("fs", "sp"), "tp"),
        P("tp", None, None),
        P("tp"),
        P(),
        P("tp", "sp"),
        P("tp", "sp"),
    )
    if not fits(mesh):
        return jax.shard_map(
            local, mesh=mesh, in_specs=placed, out_specs=P(("fs", "sp", "tp"), None), check_vma=False
        )

    return jax.shard_map(resident, mesh=mesh, in_specs=placed, out_specs=P(("fs", "sp", "tp"), None), check_vma=False)
```

```python
import functools

import jax
import jax.numpy as jnp
from jax import lax
from jax.experimental import pallas as pl
from jax.experimental.pallas import tpu as pltpu
from jax.sharding import PartitionSpec as P


QH = 32
HD = 64
WINDOW = 128
LOOKUP_FEATURES = 128
DV = 256
SPAN = 64


EPS = 1e-05
FADING_SOFTNESS = 16.0
HIGH_PRECISION = lax.Precision.HIGHEST


def passed_along(value, axis, steps):
    count = lax.axis_size(axis)
    leading, last = (max(0, -steps), min(count, count - steps))
    return lax.ppermute(value, axis, [(source, source + steps) for source in range(leading, last)])


def prefix(x, axis, combine, identity):
    peers, place = (lax.axis_size(axis), lax.axis_index(axis))
    everything = jax.tree.map(
        lambda part, kind: lax.all_gather(part.astype(kind), axis), x, (jnp.bfloat16, jnp.bfloat16)
    )
    start = jax.tree.map(
        lambda part, zero: jnp.broadcast_to(jnp.asarray(zero, part.dtype), part.shape), x, identity
    )

    def hop(k, before):
        reached = k < place
        new = combine(
            before, jax.tree.map(lambda part, own: part[k].astype(own.dtype), everything, x)
        )
        return jax.tree.map(lambda a, b: jnp.where(reached, a, b), new, before)

    return lax.fori_loop(0, peers, hop, start)


def window_attention(near_query, near_keys, near_values, head_sink_logit):
    stream_extent = near_query.shape[0]
    key_heads = near_keys.shape[1] // HD
    heads_here = near_query.shape[1] // HD
    groups = heads_here // key_heads
    blocks = stream_extent // WINDOW
    tail_rows = jnp.stack([near_keys, near_values])
    before = passed_along(tail_rows, "sp", 1)

    def banded(previous, current):
        extended = jnp.concatenate([previous, current], axis=0)
        earlier = extended[:stream_extent].reshape(blocks, WINDOW, key_heads, HD)
        present = extended[WINDOW:].reshape(blocks, WINDOW, key_heads, HD)
        return jnp.concatenate([earlier, present], axis=1)

    key_band = banded(before[0], near_keys)
    value_band = banded(before[1], near_values)
    queries = near_query.reshape(blocks, WINDOW, key_heads, groups, HD)
    scores = jnp.einsum(
        "nqhgd,nkhd->hgnqk", queries, key_band, preferred_element_type=jnp.float32
    ) * HD ** (-0.5)
    head_ids = lax.axis_index("tp") * heads_here + jnp.arange(heads_here, dtype=jnp.int32)
    slopes = jnp.exp2(-8.0 * (head_ids + 1).astype(jnp.float32) / QH).reshape(key_heads, groups)
    query_pos = jnp.arange(WINDOW, dtype=jnp.int32)
    key_pos = jnp.arange(2 * WINDOW, dtype=jnp.int32)
    distance = query_pos[:, None] - key_pos[None, :] + WINDOW
    start_pos = (
        lax.axis_index("sp") * stream_extent + (jnp.arange(blocks, dtype=jnp.int32) - 1) * WINDOW
    )
    absolute = start_pos[:, None] + key_pos[None, :]
    allowed = ((distance >= 0) & (distance < WINDOW))[None] & (absolute >= 0)[:, None, :]
    biased = scores - slopes[:, :, None, None, None] * distance.astype(jnp.float32)
    weights = jnp.where(allowed, jnp.exp(biased), 0.0)
    denominator = (
        jnp.sum(weights, axis=-1, keepdims=True)
        + jnp.exp(head_sink_logit.reshape(key_heads, groups))[:, :, None, None, None]
    )
    attention = (weights / denominator).astype(jnp.bfloat16)
    attended = jnp.einsum(
        "hgnqk,nkhd->nqhgd", attention, value_band, preferred_element_type=jnp.float32
    )
    return attended.reshape(stream_extent, heads_here * HD).astype(jnp.bfloat16)


def linear_attention(
    gated_query, gated_keys, gated_values, fading_exponent, linear_head_gain, starting_state
):
    stream_extent = gated_query.shape[0]
    head_total = gated_query.shape[1] // LOOKUP_FEATURES
    span_count = stream_extent // SPAN
    scaled_query = gated_query.astype(jnp.float32).reshape(
        span_count, SPAN, head_total, LOOKUP_FEATURES
    ) * LOOKUP_FEATURES ** (-0.5)
    keys_wide = gated_keys.astype(jnp.float32).reshape(
        span_count, SPAN, head_total, LOOKUP_FEATURES
    )
    values_wide = gated_values.astype(jnp.float32).reshape(span_count, SPAN, head_total, DV)
    running = jnp.cumsum(
        fading_exponent.reshape(span_count, SPAN, head_total, LOOKUP_FEATURES), axis=1
    )
    span_end = running[:, -1]
    query_with_decay = scaled_query * jnp.exp(running)
    inverse_keys = keys_wide * jnp.exp(-running)
    ending_keys = keys_wide * jnp.exp(span_end[:, None] - running)
    inner = jnp.einsum("nchk,nshk->nhcs", query_with_decay, inverse_keys, precision=HIGH_PRECISION)
    lower = jnp.tril(jnp.ones((SPAN, SPAN), dtype=bool))
    inner = jnp.where(lower, inner, 0.0)
    within = jnp.einsum("nhcs,nshv->nchv", inner, values_wide, precision=HIGH_PRECISION)

    def advance(running_state, inputs):
        query_portion, key_portion, value_portion, scale_factor = inputs
        layer_output = jnp.einsum(
            "fmy,mys->fms", query_portion, running_state, precision=HIGH_PRECISION
        )
        running_state = running_state * scale_factor[..., None] + jnp.einsum(
            "gxp,gxz->xpz", key_portion, value_portion, precision=HIGH_PRECISION
        )
        return (running_state, layer_output)

    start_state = jnp.zeros((head_total, LOOKUP_FEATURES, DV), jnp.float32)
    state_end, carried = lax.scan(
        advance, start_state, (query_with_decay, ending_keys, values_wide, jnp.exp(span_end))
    )
    device_decay = jnp.exp(jnp.sum(span_end, axis=0))
    prefix_sums = jnp.cumsum(span_end, axis=0) - span_end

    def combine(earlier, later):
        return (earlier[0] * later[0], later[0][..., None] * earlier[1] + later[1])

    decay_before, state_before = prefix(
        (device_decay, state_end),
        "sp",
        combine,
        (jnp.ones_like(device_decay), jnp.zeros_like(state_end)),
    )
    incoming_rows = state_before + decay_before[..., None] * starting_state
    crossing = jnp.einsum(
        "qwso,soz->qwsz",
        query_with_decay * jnp.exp(prefix_sums)[:, None],
        incoming_rows,
        precision=HIGH_PRECISION,
    )
    flat = (within + carried + crossing).reshape(stream_extent, head_total, DV)
    normal = (
        flat * lax.rsqrt(jnp.mean(flat * flat, axis=-1, keepdims=True) + EPS) * linear_head_gain
    )
    return normal.reshape(stream_extent, head_total * DV).astype(jnp.bfloat16)


def local(
    activations,
    input_norm_gain,
    window_query_weight,
    window_key_weight,
    window_value_weight,
    linear_query_weight,
    linear_key_weight,
    linear_value_weight,
    decay_down_factor,
    decay_up_factor,
    decay_offset_bias,
    extra_fading_exponent,
    starting_state,
    head_sink_logit,
    linear_head_gain,
    window_output_weight,
    linear_output_weight,
):
    gathered = lax.all_gather(activations, "tp", axis=1, tiled=True)
    widened = gathered.astype(jnp.float32)
    normed = (
        widened
        * lax.rsqrt(jnp.mean(widened * widened, axis=1, keepdims=True) + EPS)
        * input_norm_gain
    ).astype(jnp.bfloat16)
    row_total = normed.shape[0]
    matrices = (
        window_query_weight,
        window_key_weight,
        window_value_weight,
        linear_query_weight,
        linear_key_weight,
        linear_value_weight,
    )
    segments = (
        lax.all_gather(matrices[0], "sp", axis=0, tiled=True),
        lax.all_gather(matrices[1], "sp", axis=0, tiled=True),
        lax.all_gather(matrices[2], "sp", axis=0, tiled=True),
        lax.all_gather(matrices[3], "sp", axis=0, tiled=True),
        lax.all_gather(matrices[4], "sp", axis=0, tiled=True),
        lax.all_gather(matrices[5], "sp", axis=0, tiled=True),
    )
    projected = tuple(
        (jnp.dot(normed, segment, preferred_element_type=jnp.float32) for segment in segments)
    )
    near_query, near_keys, near_values, gated_query, gated_keys, gated_values = [
        product.astype(jnp.bfloat16) for product in projected
    ]
    low_rank = jnp.dot(normed, decay_down_factor, preferred_element_type=jnp.float32).astype(
        jnp.bfloat16
    )
    attention_energies = (
        jnp.dot(low_rank, decay_up_factor, preferred_element_type=jnp.float32) + decay_offset_bias
    )
    head_total = extra_fading_exponent.shape[1]
    fading_exponent = (jax.nn.log_sigmoid(attention_energies) / FADING_SOFTNESS).reshape(
        row_total, head_total, LOOKUP_FEATURES
    ) + extra_fading_exponent[:, :, None]
    near_out = window_attention(near_query, near_keys, near_values, head_sink_logit)
    gated_out = linear_attention(
        gated_query, gated_keys, gated_values, fading_exponent, linear_head_gain, starting_state
    )
    window_full, linear_full = (
        lax.all_gather(window_output_weight, "sp", axis=1, tiled=True),
        lax.all_gather(linear_output_weight, "sp", axis=1, tiled=True),
    )
    return lax.psum_scatter(
        (
            jnp.dot(near_out, window_full, preferred_element_type=jnp.float32)
            + jnp.dot(gated_out, linear_full, preferred_element_type=jnp.float32)
        ).astype(jnp.bfloat16),
        "tp",
        scatter_dimension=0,
        tiled=True,
    )


def _pairs(peers, depths, core):
    out = []
    for d in depths:
        out.append((d * 2 + core, (d + 1) * 2 + core))
        out.append(((peers - 1 - d) * 2 + 1 - core, (peers - 2 - d) * 2 + 1 - core))
    return out


SWAP = [(0, 1), (1, 0)]
VMEM = pl.BlockSpec(memory_space=pltpu.VMEM)
SMEM = pl.BlockSpec(memory_space=pltpu.SMEM)
ANY = pl.BlockSpec(memory_space=pl.ANY)
BY_COLUMNS = (((1,), (1,)), ((), ()))
BY_ROWS = (((0,), (0,)), ((), ()))


def _call(kernel, out_shape, flops, moved, grant=24, **kw):
    return pl.pallas_call(
        kernel,
        out_shape=out_shape,
        compiler_params=pltpu.CompilerParams(vmem_limit_bytes=grant * 1024 * 1024),
        cost_estimate=pl.CostEstimate(flops=flops, bytes_accessed=moved, transcendentals=0),
        **kw,
    )


def _prefetch(scalars, grid, in_specs, out_specs, scratch=()):
    return pltpu.PrefetchScalarGridSpec(
        num_scalar_prefetch=scalars, grid=grid, in_specs=in_specs, out_specs=out_specs, scratch_shapes=scratch
    )


def message_kernel(place_ref, x_ref, fade_ref, out_ref):
    rows, wide = out_ref.shape
    half_model = x_ref.shape[1]
    at = pl.ds(pl.multiple_of(place_ref[1] * rows, rows), rows)
    out_ref[:, :half_model] = x_ref[at, :]
    out_ref[:, half_model:] = jnp.concatenate(
        [_parts(fade_ref[at, :]), jnp.zeros((rows, wide - half_model - 3 * fade_ref.shape[1]), jnp.float32)], axis=1
    ).astype(out_ref.dtype)


def _parts(value):
    high = value.astype(jnp.bfloat16).astype(jnp.float32)
    rest = value - high
    middle = rest.astype(jnp.bfloat16).astype(jnp.float32)
    return jnp.concatenate([high, middle, rest - middle], axis=1)


def norm_kernel(place_ref, x_ref, fade_ref, mate_ref, gain_ref, down_ref, *out_refs):
    me, line = place_ref[0], place_ref[3]
    pieces = len(out_refs)
    rows, wide = out_refs[0].shape
    half_model = x_ref.shape[1]
    cut = 2 * half_model // pieces
    fades = 3 * fade_ref.shape[1]
    own = x_ref[pl.ds(pl.multiple_of(me * rows, rows), rows), :].astype(jnp.float32)
    mate = mate_ref[:, :half_model].astype(jnp.float32)
    square = jnp.sum(own * own, axis=1, keepdims=True) + jnp.sum(mate * mate, axis=1, keepdims=True)
    scale = lax.rsqrt(square / (2 * half_model) + EPS)
    low_rank = None
    for side, value in ((me, own), (1 - me, mate)):
        start = pl.multiple_of(side * half_model, half_model)
        normed = (value * scale * gain_ref[:, pl.ds(start, half_model)]).astype(jnp.bfloat16)
        part = lax.dot_general(
            normed, down_ref[:, pl.ds(start, half_model)], BY_COLUMNS, preferred_element_type=jnp.float32
        )
        low_rank = part if low_rank is None else low_rank + part
        for k in range(pieces // 2):
            away = lax.rem(side * (pieces // 2) + k - line + pieces, pieces)
            for offset, out_ref in enumerate(out_refs):

                @pl.when(away == offset)
                def _():
                    out_ref[:, :cut] = normed[:, k * cut : (k + 1) * cut]

    mine = _parts(fade_ref[pl.ds(pl.multiple_of(me * rows, rows), rows), :])
    theirs = mate_ref[:, half_model : half_model + fades].astype(jnp.float32)
    tail = jnp.concatenate(
        [
            low_rank.astype(jnp.bfloat16).astype(jnp.float32),
            jnp.where(me == 0, mine, theirs),
            jnp.where(me == 0, theirs, mine),
            jnp.zeros((rows, wide - cut - low_rank.shape[1] - 2 * fades), jnp.float32),
        ],
        axis=1,
    ).astype(jnp.bfloat16)
    for out_ref in out_refs:
        out_ref[:, cut:] = tail


def collect_kernel(place_ref, *refs):
    pieces = len(refs) - 1
    for offset in range(pieces):
        refs[-1][lax.rem(place_ref[3] - offset + pieces, pieces)] = refs[offset][...]


def collect(place, parts):
    rows, wide = parts[0].shape
    return _call(
        collect_kernel,
        jax.ShapeDtypeStruct((len(parts), rows, wide), parts[0].dtype),
        10**8,
        2**21,
        in_specs=[SMEM] + [VMEM] * len(parts),
        out_specs=VMEM,
    )(place, *parts)


def join_kernel(place_ref, kept_ref, given_ref, *out_refs):
    pieces = len(out_refs)
    rows = out_refs[0].shape[0]
    for offset, out_ref in enumerate(out_refs):
        at = pl.ds(pl.multiple_of(lax.rem(place_ref[3] + offset, pieces) * rows, rows), rows)
        out_ref[...] = (kept_ref[at].astype(jnp.float32) + given_ref[at].astype(jnp.float32)).astype(out_ref.dtype)


def join(place, kept, given, pieces):
    rows, columns = kept.shape
    return _call(
        join_kernel,
        [jax.ShapeDtypeStruct((rows // pieces, columns), kept.dtype)] * pieces,
        10**8,
        2**21,
        in_specs=[SMEM, VMEM, VMEM],
        out_specs=[VMEM] * pieces,
    )(place, kept, given)


def spread_kernel(place_ref, *refs):
    pieces = len(refs) - 1
    columns = refs[0].shape[1]
    for offset in range(pieces):
        start = lax.rem(place_ref[3] - offset + pieces, pieces) * columns
        refs[-1][:, pl.ds(pl.multiple_of(start, columns), columns)] = refs[offset][...]


def spread(place, parts):
    rows, columns = parts[0].shape
    return _call(
        spread_kernel,
        jax.ShapeDtypeStruct((rows, len(parts) * columns), parts[0].dtype),
        10**8,
        2**21,
        in_specs=[SMEM] + [VMEM] * len(parts),
        out_specs=VMEM,
    )(place, *parts)


def to_offsets(parts):
    peers = len(parts)
    out = [parts[0]]
    for k in range(1, peers):
        out.append(lax.ppermute(parts[k], "sp", [(i, (i + k) % peers) for i in range(peers)]))
    return out


def pack_kernel(key_heads, lin, side_ref, wq, wk, wv, lq, lk, lv, out_ref):
    step = pl.program_id(0)
    half = out_ref.shape[2] // 2
    keys_and_values = step == 0
    queries = (step > 0) & (step <= key_heads)
    head_items = (step > key_heads) & (step <= key_heads + lin)
    head_values = step > key_heads + lin

    @pl.when(keys_and_values)
    def _():
        out_ref[0, :, :half] = wk[...]
        out_ref[0, :, half:] = wv[...]

    @pl.when(queries)
    def _():
        out_ref[0] = wq[...]

    @pl.when(head_items)
    def _():
        out_ref[0, :, :half] = lq[...]
        out_ref[0, :, half:] = lk[...]

    @pl.when(head_values)
    def _():
        out_ref[0] = lv[...]


def pack_items(side, lin, key_heads, matrices):
    depth = matrices[0].shape[0]
    width = 2 * LOOKUP_FEATURES
    count = 1 + key_heads + 2 * lin
    fixed = pl.BlockSpec((depth, width // 2), lambda i, side: (0, side[0]))
    query = pl.BlockSpec(
        (depth, width), lambda i, side: (0, side[0] * key_heads + jnp.clip(i - 1, 0, key_heads - 1))
    )
    head = lambda past: lambda i, side: (0, side[0] * lin + jnp.clip(i - 1 - key_heads - past, 0, lin - 1))
    narrow, full = pl.BlockSpec((depth, width // 2), head(0)), pl.BlockSpec((depth, width), head(lin))
    return _call(
        functools.partial(pack_kernel, key_heads, lin),
        jax.ShapeDtypeStruct((count, depth, width), jnp.bfloat16),
        10**11,
        4 * count * depth * width,
        grid_spec=_prefetch(
            1,
            (count,),
            [query, fixed, fixed, narrow, narrow, full],
            pl.BlockSpec((1, depth, width), lambda i, side: (i, 0, 0)),
        ),
    )(side, *matrices)


def partial_kernel(index_ref, mine_ref, theirs_ref, own_ref, other_ref, *rest):
    out_ref, weight, arrival = rest[-3:]
    rows = mine_ref.shape[0]
    depth, width = weight.shape
    copy = pltpu.make_async_copy(other_ref.at[index_ref[0]], weight, arrival)
    copy.start()
    for half in range(2):
        if half == 1:
            copy.wait()
        for top, x_ref in enumerate((mine_ref, theirs_ref)):
            at = slice(top * rows, (top + 1) * rows)
            span = slice(half * width, (half + 1) * width)
            matrix = own_ref[index_ref[0]] if half == 0 else weight[...]
            total = jnp.dot(x_ref[:, :depth], matrix, preferred_element_type=jnp.float32)
            if len(rest) == 4:
                total = total + rest[0][at, span].astype(jnp.float32)
            out_ref[at, span] = total.astype(out_ref.dtype)


def partial_sum(index, mine, theirs, own, other, arrived):
    rows = mine.shape[0]
    _, depth, width = own.shape
    operands = [mine, theirs, own, other] + ([] if arrived is None else [arrived])
    return _call(
        partial_kernel,
        jax.ShapeDtypeStruct((2 * rows, 2 * width), jnp.bfloat16),
        160 * rows * depth * width,
        4 * depth * (rows + width),
        in_specs=[SMEM, VMEM, VMEM, VMEM, ANY] + [VMEM] * (len(operands) - 4),
        out_specs=VMEM,
        scratch_shapes=[pltpu.VMEM((depth, width), jnp.bfloat16), pltpu.SemaphoreType.DMA],
    )(index, *operands)


def decay_kernel(lin, rank, place_ref, mine_ref, theirs_ref, own_ref, other_ref, *out_refs):
    me, side = place_ref[0], place_ref[1]
    rows = mine_ref.shape[0]
    features = LOOKUP_FEATURES
    lower = (
        lax.broadcasted_iota(jnp.int32, (SPAN, SPAN), 0) >= lax.broadcasted_iota(jnp.int32, (SPAN, SPAN), 1)
    ).astype(jnp.bfloat16)
    for top, tail_ref in enumerate((mine_ref, theirs_ref)):
        tail = tail_ref[:, tail_ref.shape[1] - features :]
        low_rank = tail[:, :rank]
        parts = [
            tail[:, rank + k * 2 * lin : rank + (k + 1) * 2 * lin].astype(jnp.float32) for k in range(6)
        ]
        by_core = [parts[0] + parts[1] + parts[2], parts[3] + parts[4] + parts[5]]
        fades = [jnp.where(me == 0, by_core[0], by_core[1]), jnp.where(me == 0, by_core[1], by_core[0])]
        for head in range(lin):
            for owner, small_ref in enumerate((own_ref, other_ref)):
                at = pl.ds(pl.multiple_of((side * lin + head) * features, features), features)
                up = small_ref[:rank, at].astype(jnp.bfloat16)
                energy = jnp.dot(low_rank, up, preferred_element_type=jnp.float32) + small_ref[rank : rank + 1, at]
                soft = jnp.minimum(energy, 0.0) - jnp.log1p(jnp.exp(-jnp.abs(energy)))
                both = fades[owner]
                fade = jnp.where(side == 0, both[:, head : head + 1], both[:, lin + head : lin + head + 1])
                step = soft * (1.0 / FADING_SOFTNESS) + fade
                high = step.astype(jnp.bfloat16)
                rest = step - high.astype(jnp.float32)
                middle = rest.astype(jnp.bfloat16)
                low = (rest - middle.astype(jnp.float32)).astype(jnp.bfloat16)
                column = owner * features
                out_ref = out_refs[head]
                for span in range(rows // SPAN):
                    cut = slice(span * SPAN, (span + 1) * SPAN)
                    out_ref[top * rows + span * SPAN : top * rows + (span + 1) * SPAN, column : column + features] = (
                        jnp.dot(lower, high[cut], preferred_element_type=jnp.float32)
                        + jnp.dot(lower, middle[cut], preferred_element_type=jnp.float32)
                        + jnp.dot(lower, low[cut], preferred_element_type=jnp.float32)
                    )


def decay_sums(place, lin, rank, mine, theirs, own, other):
    return _call(
        functools.partial(decay_kernel, lin, rank),
        [jax.ShapeDtypeStruct((2 * mine.shape[0], 2 * LOOKUP_FEATURES), jnp.float32)] * lin,
        10**9,
        2**20,
        in_specs=[SMEM] + [VMEM] * 4,
        out_specs=[VMEM] * lin,
    )(place, mine, theirs, own, other)


def linear_kernel(lin, head, half, place_ref, query_key_ref, value_ref, rest_ref, running_ref, own_ref, other_ref, gain_ref, out_ref):
    me, side = place_ref[0], place_ref[1]
    rows, width = query_key_ref.shape
    features = LOOKUP_FEATURES
    values = width // 2
    lower = lax.broadcasted_iota(jnp.int32, (SPAN, SPAN), 0) >= lax.broadcasted_iota(
        jnp.int32, (SPAN, SPAN), 1
    )
    states = [state_ref[side * lin + head].T for state_ref in (own_ref, other_ref)]
    for span in range(rows // SPAN):
        per = half // SPAN
        device, inside = span // (2 * per), span % (2 * per)
        apart = jnp.where(me == inside // per, 0, rows // 2)
        at = pl.ds(pl.multiple_of(apart + device * half + (inside % per) * SPAN, SPAN), SPAN)
        for owner in range(2):
            base = owner * values
            running = running_ref[at, owner * features : (owner + 1) * features]
            query = query_key_ref[at, base : base + features].astype(jnp.float32)
            key = query_key_ref[at, base + features : base + 2 * features].astype(jnp.float32)
            value = (
                value_ref[at, base : base + values].astype(jnp.float32)
                + rest_ref[at, base : base + values].astype(jnp.float32)
            ).astype(jnp.bfloat16)
            end = running[SPAN - 1 : SPAN]
            scaled = (query * features ** (-0.5) * jnp.exp(running)).astype(jnp.bfloat16)
            inverse = (key * jnp.exp(-running)).astype(jnp.bfloat16)
            ending = (key * jnp.exp(end - running)).astype(jnp.bfloat16)
            inner = lax.dot_general(scaled, inverse, BY_COLUMNS, preferred_element_type=jnp.float32)
            inner = jnp.where(lower, inner, 0.0).astype(jnp.bfloat16)
            state = states[owner]
            raw = jnp.dot(inner, value, preferred_element_type=jnp.float32) + lax.dot_general(
                scaled, state.astype(jnp.bfloat16), BY_COLUMNS, preferred_element_type=jnp.float32
            )
            states[owner] = state * jnp.exp(end) + lax.dot_general(
                value, ending, BY_ROWS, preferred_element_type=jnp.float32
            )
            scale = lax.rsqrt(jnp.mean(raw * raw, axis=-1, keepdims=True) + EPS)
            out_ref[at, base : base + values] = (raw * scale * gain_ref[...]).astype(out_ref.dtype)


def linear_heads(place, lin, head, half, query_key, value, rest, running, own, other, gain):
    return _call(
        functools.partial(linear_kernel, lin, head, half),
        jax.ShapeDtypeStruct(query_key.shape, jnp.bfloat16),
        2 * 10**9,
        2**21,
        in_specs=[SMEM] + [VMEM] * 7,
        out_specs=VMEM,
    )(place, query_key, value, rest, running, own, other, gain)


def window_kernel(group, half, place_ref, slope_ref, sink_ref, key_value_ref, query_ref, out_ref):
    me = place_ref[0]
    rows = query_ref.shape[0]
    owners, groups = slope_ref.shape
    pair = key_value_ref.shape[1] // (2 * owners)
    from_query = lax.broadcasted_iota(jnp.int32, (WINDOW, WINDOW), 0)
    from_key = lax.broadcasted_iota(jnp.int32, (WINDOW, WINDOW), 1)
    present = from_key <= from_query
    distance = jnp.where(present, from_query - from_key, from_query - from_key + WINDOW).astype(jnp.float32)
    unit = min(half, WINDOW)

    def places(block):
        out = []
        for piece in range(WINDOW // unit):
            start = block * WINDOW + piece * unit
            device, inside = start // (2 * half), start % (2 * half)
            apart = jnp.where(me == inside // half, 0, rows // 2)
            out.append(pl.ds(pl.multiple_of(apart + device * half + inside % half, unit), unit))
        return out

    for owner in range(owners):
        key_at = owner * 2 * pair + group * HD
        value_at = key_at + pair
        base = owner * groups * HD
        biases = [slope_ref[owner, head] * distance for head in range(groups)]
        past_keys, past_values = None, None
        for block in range(rows // WINDOW):
            first = block == 0
            at = places(block)
            keys = jnp.concatenate([key_value_ref[a, key_at : key_at + HD] for a in at], axis=0)
            values = jnp.concatenate([key_value_ref[a, value_at : value_at + HD] for a in at], axis=0)
            band_keys = keys if first else jnp.concatenate([past_keys, keys], axis=0)
            band_values = values if first else jnp.concatenate([past_values, values], axis=0)
            past_keys, past_values = keys, values
            queries = jnp.concatenate(
                [query_ref[a, base + head * HD : base + (head + 1) * HD] for head in range(groups) for a in at],
                axis=0,
            )
            scores = lax.dot_general(queries, band_keys, BY_COLUMNS, preferred_element_type=jnp.float32)
            probs = []
            for head in range(groups):
                mine = scores[head * WINDOW : (head + 1) * WINDOW]
                if first:
                    weight = jnp.where(present, jnp.exp(mine * HD ** (-0.5) - biases[head]), 0.0)
                else:
                    score = jnp.where(present, mine[:, WINDOW:], mine[:, :WINDOW])
                    weight = jnp.exp(score * HD ** (-0.5) - biases[head])
                total = jnp.sum(weight, axis=-1, keepdims=True) + sink_ref[owner, head]
                share = weight / total
                if first:
                    probs.append(share.astype(jnp.bfloat16))
                else:
                    probs.append(
                        jnp.concatenate(
                            [
                                jnp.where(present, 0.0, share).astype(jnp.bfloat16),
                                jnp.where(present, share, 0.0).astype(jnp.bfloat16),
                            ],
                            axis=1,
                        )
                    )
            outs = jnp.dot(jnp.concatenate(probs, axis=0), band_values, preferred_element_type=jnp.float32)
            joined = jnp.concatenate(
                [outs[head * WINDOW : (head + 1) * WINDOW] for head in range(groups)], axis=1
            ).astype(out_ref.dtype)
            for piece, a in enumerate(at):
                out_ref[a, base : base + groups * HD] = joined[piece * unit : (piece + 1) * unit]


def window_heads(place, group, half, slopes, sinks, key_value, query):
    return _call(
        functools.partial(window_kernel, group, half),
        jax.ShapeDtypeStruct(query.shape, jnp.bfloat16),
        2 * 10**9,
        2**21,
        in_specs=[SMEM, SMEM, SMEM, VMEM, VMEM],
        out_specs=VMEM,
    )(place, slopes, sinks, key_value, query)


def output_kernel(sources, place_ref, *refs):
    count = 1 + max(max(row) for row in sources)
    pieces = len(sources)
    passed = refs[:count]
    own_ref, other_ref = refs[count : count + 2]
    held, arrival = refs[-2:]
    rest = refs[count + 2 : -2]
    split = rest[-1].shape[0] != held.shape[1]
    outs = rest[-2:] if split else rest[-1:]
    before = rest[: len(rest) - len(outs)]
    depth = place_ref[2]
    for at in range(len(sources[0])):

        @pl.when(depth == at)
        def _():
            for piece in range(pieces):
                pltpu.make_async_copy(passed[sources[piece][at]], held.at[piece], arrival.at[piece]).start()

    for piece in range(pieces):
        pltpu.make_async_copy(passed[0], held.at[piece], arrival.at[piece]).wait()
    width = held.shape[2] // 2
    rows = outs[0].shape[0]
    columns = outs[0].shape[1]
    block = columns // 2
    for top, out_ref in enumerate(outs):
        at = slice(top * rows, (top + 1) * rows)
        for part in range(2):
            span = slice(part * block, (part + 1) * block)
            total = before[0][at, span] if before else jnp.zeros((rows, block), jnp.float32)
            for piece in range(pieces):
                lines = slice(piece * width, (piece + 1) * width)
                total = total + jnp.dot(
                    held[piece, at, :width], own_ref[lines, span], preferred_element_type=jnp.float32
                )
                total = total + jnp.dot(
                    held[piece, at, width:], other_ref[lines, span], preferred_element_type=jnp.float32
                )
            out_ref[:, span] = total.astype(out_ref.dtype)


def output_sum(place, passed, sources, own, other, before, split):
    rows, width = passed[0].shape
    pieces = len(sources)
    lines, columns = other.shape
    kind, parts = (jnp.bfloat16, 2) if split else (jnp.float32, 1)
    whole = pl.BlockSpec((rows, columns), lambda i, place: (0, 0))
    out = pl.BlockSpec((rows // parts, columns), lambda i, place: (0, 0))
    return _call(
        functools.partial(output_kernel, sources),
        [jax.ShapeDtypeStruct((rows // parts, columns), kind)] * parts,
        4 * rows * columns * lines,
        8 * rows * columns,
        grid_spec=_prefetch(
            1,
            (1,),
            [ANY] * len(passed)
            + [
                pl.BlockSpec((lines, columns), lambda i, place: (place[1], 0)),
                pl.BlockSpec((lines, columns), lambda i, place: (0, 0)),
            ]
            + ([] if before is None else [whole]),
            [out] * parts,
            [pltpu.VMEM((pieces, rows, width), jnp.bfloat16), pltpu.SemaphoreType.DMA((pieces,))],
        ),
    )(place, *passed, own, other, *([] if before is None else [before]))


def resident(
    activations,
    input_norm_gain,
    window_query_weight,
    window_key_weight,
    window_value_weight,
    linear_query_weight,
    linear_key_weight,
    linear_value_weight,
    decay_down_factor,
    decay_up_factor,
    decay_offset_bias,
    extra_fading_exponent,
    starting_state,
    head_sink_logit,
    linear_head_gain,
    window_output_weight,
    linear_output_weight,
):
    peers = lax.axis_size("sp")
    hops = peers - 1
    line, me = lax.axis_index("sp"), lax.axis_index("tp")
    depth = jnp.where(me == 0, line, hops - line)
    far, near = 1 - me, me
    place = jnp.stack([me, far, hops - depth, line]).astype(jnp.int32)
    rows, half_model = activations.shape
    half = rows // 2
    bf16, f32 = jnp.bfloat16, jnp.float32
    lin = extra_fading_exponent.shape[1] // 2
    key_heads = window_key_weight.shape[1] // HD // 2
    query_heads = window_query_weight.shape[1] // HD // 2
    groups = query_heads // key_heads
    rank = decay_down_factor.shape[1]

    def swap(value):
        return lax.ppermute(value, "tp", SWAP)


    message = _call(
        message_kernel,
        jax.ShapeDtypeStruct((half, half_model + LOOKUP_FEATURES), bf16),
        10**8,
        2**20,
        in_specs=[SMEM, VMEM, VMEM],
        out_specs=VMEM,
    )(place, activations, extra_fading_exponent)
    mate = swap(message)
    wide = 2 * half_model // peers + LOOKUP_FEATURES
    outgoing = _call(
        norm_kernel,
        [jax.ShapeDtypeStruct((half, wide), bf16)] * peers,
        10**9,
        2**21,
        in_specs=[SMEM] + [VMEM] * 5,
        out_specs=[VMEM] * peers,
    )(place, activations, extra_fading_exponent, mate, input_norm_gain.reshape(1, -1), decay_down_factor.T)

    (
        outgoing,
        matrices,
        window_output_weight,
        linear_output_weight,
        starting_state,
        decay_up_factor,
        decay_offset_bias,
        head_sink_logit,
    ) = lax.optimization_barrier(
        (
            outgoing,
            (
                window_query_weight,
                window_key_weight,
                window_value_weight,
                linear_query_weight,
                linear_key_weight,
                linear_value_weight,
            ),
            window_output_weight,
            linear_output_weight,
            starting_state,
            decay_up_factor,
            decay_offset_bias,
            head_sink_logit,
        )
    )
    incoming = to_offsets(outgoing)
    packed = pack_items(near.reshape(1), lin, key_heads, matrices)
    other_in = swap(packed)
    own_in = pack_items(far.reshape(1), lin, key_heads, matrices)
    features = decay_up_factor.shape[1]
    own_small = jnp.concatenate(
        [
            decay_up_factor.astype(f32),
            decay_offset_bias.reshape(1, features),
            jnp.pad(head_sink_logit, (0, features - head_sink_logit.shape[0])).reshape(1, features),
            jnp.zeros((6, features), f32),
        ],
        axis=0,
    )
    other_small = swap(own_small)
    other_state = swap(starting_state)
    lines = linear_output_weight.shape[0] // 2
    other_linear = lax.dynamic_slice_in_dim(linear_output_weight, near * lines, lines, axis=0)
    other_linear = swap(other_linear)
    lines = window_output_weight.shape[0] // 2
    other_window = lax.dynamic_slice_in_dim(window_output_weight, near * lines, lines, axis=0)
    other_window = swap(other_window)

    incoming = collect(place, incoming)
    mine = incoming.reshape(peers * half, wide)
    theirs = swap(incoming).reshape(peers * half, wide)

    count = 1 + key_heads + 2 * lin
    chained = count - lin
    arrived, sums, direct = {}, [], []
    for step in range(chained + 2 * hops):
        turn = step - 2 * depth
        index = jnp.where(turn >= 0, turn, count + turn)
        index = jnp.clip(index, 0, count - 1).astype(jnp.int32).reshape(1)
        value = partial_sum(index, mine, theirs, own_in, other_in, arrived.get(step - 2))
        sums.append(value)
        if chained <= step < count:
            pairs = [(0, hops * 2), (hops * 2 + 1, 1)]
            direct.append(lax.ppermute(value, ("sp", "tp"), pairs))
        depths = [d for d in range(hops) if 0 <= step - 2 * d < chained or (d and -lin <= step - 2 * d < 0)]
        if depths:
            arrived[step] = lax.ppermute(value, ("sp", "tp"), _pairs(peers, depths, 0))
    finals = sums[2 * hops :]

    running = decay_sums(place, lin, rank, mine, theirs, own_small, other_small)
    sinks = jnp.stack(
        [
            lax.dynamic_slice_in_dim(small[rank + 1], far * query_heads, query_heads).reshape(key_heads, groups)
            for small in (own_small, other_small)
        ]
    )
    sinks = jnp.exp(sinks)
    attended = []
    for group in range(key_heads):
        number = jnp.stack([me, 1 - me])[:, None] * (2 * query_heads) + (
            far * query_heads + group * groups + jnp.arange(groups, dtype=jnp.int32)
        )
        slopes = jnp.exp2(-8.0 * (number + 1).astype(f32) / QH)
        attended.append(
            window_heads(place, group, half, slopes, sinks[:, group], finals[0], finals[1 + group])
        )
    for head in range(lin):
        attended.append(
            linear_heads(
                place,
                lin,
                head,
                half,
                finals[1 + key_heads + head],
                sums[2 * (hops - 1) + head],
                direct[head],
                running[head],
                starting_state,
                other_state,
                linear_head_gain.reshape(1, DV),
            )
        )

    pieces = len(attended)
    held = []
    for piece in range(pieces):
        seen = [attended[piece]]
        for hop in range(hops):
            if piece < pieces - 1:
                seen.append(lax.ppermute(seen[-1], ("sp", "tp"), _pairs(peers, [hop], 1)))
            else:
                last = hops - hop
                pairs = [(hops * 2, (hops - last) * 2), (1, last * 2 + 1)]
                seen.insert(1, lax.ppermute(seen[0], ("sp", "tp"), pairs))
        held.append(seen)
    table = lambda count: tuple(tuple(range(k * peers, (k + 1) * peers)) for k in range(count))
    flat = lambda lists: [value for seen in lists for value in seen]
    (terms,) = output_sum(
        place, flat(held[:key_heads]), table(key_heads), window_output_weight, other_window, None, False
    )
    kept, given = output_sum(
        place, flat(held[key_heads:]), table(lin), linear_output_weight, other_linear, terms, True
    )

    return spread(place, to_offsets(join(place, kept, swap(given), peers)))


def fits(mesh):
    return mesh.shape["tp"] == 2 and mesh.shape["sp"] > 1


def solution(mesh):
    placed = (
        P(("fs", "sp"), "tp"),
        P(),
        P("sp", "tp"),
        P("sp", "tp"),
        P("sp", "tp"),
        P("sp", "tp"),
        P("sp", "tp"),
        P("sp", "tp"),
        P(),
        P(None, "tp"),
        P("tp"),
        P(("fs", "sp"), "tp"),
        P("tp", None, None),
        P("tp"),
        P(),
        P("tp", "sp"),
        P("tp", "sp"),
    )
    if not fits(mesh):
        return jax.shard_map(
            local, mesh=mesh, in_specs=placed, out_specs=P(("fs", "sp", "tp"), None), check_vma=False
        )

    return jax.shard_map(resident, mesh=mesh, in_specs=placed, out_specs=P(("fs", "sp", "tp"), None), check_vma=False)
```

```python
import functools

import jax
import jax.numpy as jnp
from jax import lax
from jax.experimental import pallas as pl
from jax.experimental.pallas import tpu as pltpu
from jax.sharding import PartitionSpec as P


QH = 32
HD = 64
WINDOW = 128
LOOKUP_FEATURES = 128
DV = 256
SPAN = 64


EPS = 1e-05
FADING_SOFTNESS = 16.0
HIGH_PRECISION = lax.Precision.HIGHEST


def passed_along(value, axis, steps):
    count = lax.axis_size(axis)
    leading, last = (max(0, -steps), min(count, count - steps))
    return lax.ppermute(value, axis, [(source, source + steps) for source in range(leading, last)])


def prefix(x, axis, combine, identity):
    peers, place = (lax.axis_size(axis), lax.axis_index(axis))
    everything = jax.tree.map(
        lambda part, kind: lax.all_gather(part.astype(kind), axis), x, (jnp.bfloat16, jnp.bfloat16)
    )
    start = jax.tree.map(
        lambda part, zero: jnp.broadcast_to(jnp.asarray(zero, part.dtype), part.shape), x, identity
    )

    def hop(k, before):
        reached = k < place
        new = combine(
            before, jax.tree.map(lambda part, own: part[k].astype(own.dtype), everything, x)
        )
        return jax.tree.map(lambda a, b: jnp.where(reached, a, b), new, before)

    return lax.fori_loop(0, peers, hop, start)


def window_attention(near_query, near_keys, near_values, head_sink_logit):
    stream_extent = near_query.shape[0]
    key_heads = near_keys.shape[1] // HD
    heads_here = near_query.shape[1] // HD
    groups = heads_here // key_heads
    blocks = stream_extent // WINDOW
    tail_rows = jnp.stack([near_keys, near_values])
    before = passed_along(tail_rows, "sp", 1)

    def banded(previous, current):
        extended = jnp.concatenate([previous, current], axis=0)
        earlier = extended[:stream_extent].reshape(blocks, WINDOW, key_heads, HD)
        present = extended[WINDOW:].reshape(blocks, WINDOW, key_heads, HD)
        return jnp.concatenate([earlier, present], axis=1)

    key_band = banded(before[0], near_keys)
    value_band = banded(before[1], near_values)
    queries = near_query.reshape(blocks, WINDOW, key_heads, groups, HD)
    scores = jnp.einsum(
        "nqhgd,nkhd->hgnqk", queries, key_band, preferred_element_type=jnp.float32
    ) * HD ** (-0.5)
    head_ids = lax.axis_index("tp") * heads_here + jnp.arange(heads_here, dtype=jnp.int32)
    slopes = jnp.exp2(-8.0 * (head_ids + 1).astype(jnp.float32) / QH).reshape(key_heads, groups)
    query_pos = jnp.arange(WINDOW, dtype=jnp.int32)
    key_pos = jnp.arange(2 * WINDOW, dtype=jnp.int32)
    distance = query_pos[:, None] - key_pos[None, :] + WINDOW
    start_pos = (
        lax.axis_index("sp") * stream_extent + (jnp.arange(blocks, dtype=jnp.int32) - 1) * WINDOW
    )
    absolute = start_pos[:, None] + key_pos[None, :]
    allowed = ((distance >= 0) & (distance < WINDOW))[None] & (absolute >= 0)[:, None, :]
    biased = scores - slopes[:, :, None, None, None] * distance.astype(jnp.float32)
    weights = jnp.where(allowed, jnp.exp(biased), 0.0)
    denominator = (
        jnp.sum(weights, axis=-1, keepdims=True)
        + jnp.exp(head_sink_logit.reshape(key_heads, groups))[:, :, None, None, None]
    )
    attention = (weights / denominator).astype(jnp.bfloat16)
    attended = jnp.einsum(
        "hgnqk,nkhd->nqhgd", attention, value_band, preferred_element_type=jnp.float32
    )
    return attended.reshape(stream_extent, heads_here * HD).astype(jnp.bfloat16)


def linear_attention(
    gated_query, gated_keys, gated_values, fading_exponent, linear_head_gain, starting_state
):
    stream_extent = gated_query.shape[0]
    head_total = gated_query.shape[1] // LOOKUP_FEATURES
    span_count = stream_extent // SPAN
    scaled_query = gated_query.astype(jnp.float32).reshape(
        span_count, SPAN, head_total, LOOKUP_FEATURES
    ) * LOOKUP_FEATURES ** (-0.5)
    keys_wide = gated_keys.astype(jnp.float32).reshape(
        span_count, SPAN, head_total, LOOKUP_FEATURES
    )
    values_wide = gated_values.astype(jnp.float32).reshape(span_count, SPAN, head_total, DV)
    running = jnp.cumsum(
        fading_exponent.reshape(span_count, SPAN, head_total, LOOKUP_FEATURES), axis=1
    )
    span_end = running[:, -1]
    query_with_decay = scaled_query * jnp.exp(running)
    inverse_keys = keys_wide * jnp.exp(-running)
    ending_keys = keys_wide * jnp.exp(span_end[:, None] - running)
    inner = jnp.einsum("nchk,nshk->nhcs", query_with_decay, inverse_keys, precision=HIGH_PRECISION)
    lower = jnp.tril(jnp.ones((SPAN, SPAN), dtype=bool))
    inner = jnp.where(lower, inner, 0.0)
    within = jnp.einsum("nhcs,nshv->nchv", inner, values_wide, precision=HIGH_PRECISION)

    def advance(running_state, inputs):
        query_portion, key_portion, value_portion, scale_factor = inputs
        layer_output = jnp.einsum(
            "fmy,mys->fms", query_portion, running_state, precision=HIGH_PRECISION
        )
        running_state = running_state * scale_factor[..., None] + jnp.einsum(
            "gxp,gxz->xpz", key_portion, value_portion, precision=HIGH_PRECISION
        )
        return (running_state, layer_output)

    start_state = jnp.zeros((head_total, LOOKUP_FEATURES, DV), jnp.float32)
    state_end, carried = lax.scan(
        advance, start_state, (query_with_decay, ending_keys, values_wide, jnp.exp(span_end))
    )
    device_decay = jnp.exp(jnp.sum(span_end, axis=0))
    prefix_sums = jnp.cumsum(span_end, axis=0) - span_end

    def combine(earlier, later):
        return (earlier[0] * later[0], later[0][..., None] * earlier[1] + later[1])

    decay_before, state_before = prefix(
        (device_decay, state_end),
        "sp",
        combine,
        (jnp.ones_like(device_decay), jnp.zeros_like(state_end)),
    )
    incoming_rows = state_before + decay_before[..., None] * starting_state
    crossing = jnp.einsum(
        "qwso,soz->qwsz",
        query_with_decay * jnp.exp(prefix_sums)[:, None],
        incoming_rows,
        precision=HIGH_PRECISION,
    )
    flat = (within + carried + crossing).reshape(stream_extent, head_total, DV)
    normal = (
        flat * lax.rsqrt(jnp.mean(flat * flat, axis=-1, keepdims=True) + EPS) * linear_head_gain
    )
    return normal.reshape(stream_extent, head_total * DV).astype(jnp.bfloat16)


def local(
    activations,
    input_norm_gain,
    window_query_weight,
    window_key_weight,
    window_value_weight,
    linear_query_weight,
    linear_key_weight,
    linear_value_weight,
    decay_down_factor,
    decay_up_factor,
    decay_offset_bias,
    extra_fading_exponent,
    starting_state,
    head_sink_logit,
    linear_head_gain,
    window_output_weight,
    linear_output_weight,
):
    gathered = lax.all_gather(activations, "tp", axis=1, tiled=True)
    widened = gathered.astype(jnp.float32)
    normed = (
        widened
        * lax.rsqrt(jnp.mean(widened * widened, axis=1, keepdims=True) + EPS)
        * input_norm_gain
    ).astype(jnp.bfloat16)
    row_total = normed.shape[0]
    matrices = (
        window_query_weight,
        window_key_weight,
        window_value_weight,
        linear_query_weight,
        linear_key_weight,
        linear_value_weight,
    )
    segments = (
        lax.all_gather(matrices[0], "sp", axis=0, tiled=True),
        lax.all_gather(matrices[1], "sp", axis=0, tiled=True),
        lax.all_gather(matrices[2], "sp", axis=0, tiled=True),
        lax.all_gather(matrices[3], "sp", axis=0, tiled=True),
        lax.all_gather(matrices[4], "sp", axis=0, tiled=True),
        lax.all_gather(matrices[5], "sp", axis=0, tiled=True),
    )
    projected = tuple(
        (jnp.dot(normed, segment, preferred_element_type=jnp.float32) for segment in segments)
    )
    near_query, near_keys, near_values, gated_query, gated_keys, gated_values = [
        product.astype(jnp.bfloat16) for product in projected
    ]
    low_rank = jnp.dot(normed, decay_down_factor, preferred_element_type=jnp.float32).astype(
        jnp.bfloat16
    )
    attention_energies = (
        jnp.dot(low_rank, decay_up_factor, preferred_element_type=jnp.float32) + decay_offset_bias
    )
    head_total = extra_fading_exponent.shape[1]
    fading_exponent = (jax.nn.log_sigmoid(attention_energies) / FADING_SOFTNESS).reshape(
        row_total, head_total, LOOKUP_FEATURES
    ) + extra_fading_exponent[:, :, None]
    near_out = window_attention(near_query, near_keys, near_values, head_sink_logit)
    gated_out = linear_attention(
        gated_query, gated_keys, gated_values, fading_exponent, linear_head_gain, starting_state
    )
    window_full, linear_full = (
        lax.all_gather(window_output_weight, "sp", axis=1, tiled=True),
        lax.all_gather(linear_output_weight, "sp", axis=1, tiled=True),
    )
    return lax.psum_scatter(
        (
            jnp.dot(near_out, window_full, preferred_element_type=jnp.float32)
            + jnp.dot(gated_out, linear_full, preferred_element_type=jnp.float32)
        ).astype(jnp.bfloat16),
        "tp",
        scatter_dimension=0,
        tiled=True,
    )


def _pairs(peers, depths, core):
    out = []
    for d in depths:
        out.append((d * 2 + core, (d + 1) * 2 + core))
        out.append(((peers - 1 - d) * 2 + 1 - core, (peers - 2 - d) * 2 + 1 - core))
    return out


SWAP = [(0, 1), (1, 0)]
VMEM = pl.BlockSpec(memory_space=pltpu.VMEM)
SMEM = pl.BlockSpec(memory_space=pltpu.SMEM)
ANY = pl.BlockSpec(memory_space=pl.ANY)
BY_COLUMNS = (((1,), (1,)), ((), ()))
BY_ROWS = (((0,), (0,)), ((), ()))


def _call(kernel, out_shape, flops, moved, grant=24, **kw):
    return pl.pallas_call(
        kernel,
        out_shape=out_shape,
        compiler_params=pltpu.CompilerParams(vmem_limit_bytes=grant * 1024 * 1024),
        cost_estimate=pl.CostEstimate(flops=flops, bytes_accessed=moved, transcendentals=0),
        **kw,
    )


def _prefetch(scalars, grid, in_specs, out_specs, scratch=()):
    return pltpu.PrefetchScalarGridSpec(
        num_scalar_prefetch=scalars, grid=grid, in_specs=in_specs, out_specs=out_specs, scratch_shapes=scratch
    )


def message_kernel(place_ref, x_ref, fade_ref, out_ref):
    rows, wide = out_ref.shape
    half_model = x_ref.shape[1]
    at = pl.ds(pl.multiple_of(place_ref[1] * rows, rows), rows)
    out_ref[:, :half_model] = x_ref[at, :]
    out_ref[:, half_model:] = jnp.concatenate(
        [_parts(fade_ref[at, :]), jnp.zeros((rows, wide - half_model - 3 * fade_ref.shape[1]), jnp.float32)], axis=1
    ).astype(out_ref.dtype)


def _parts(value):
    high = value.astype(jnp.bfloat16).astype(jnp.float32)
    rest = value - high
    middle = rest.astype(jnp.bfloat16).astype(jnp.float32)
    return jnp.concatenate([high, middle, rest - middle], axis=1)


def norm_kernel(place_ref, x_ref, fade_ref, mate_ref, gain_ref, down_ref, *out_refs):
    me, line = place_ref[0], place_ref[3]
    pieces = len(out_refs)
    rows, wide = out_refs[0].shape
    half_model = x_ref.shape[1]
    cut = 2 * half_model // pieces
    fades = 3 * fade_ref.shape[1]
    own = x_ref[pl.ds(pl.multiple_of(me * rows, rows), rows), :].astype(jnp.float32)
    mate = mate_ref[:, :half_model].astype(jnp.float32)
    square = jnp.sum(own * own, axis=1, keepdims=True) + jnp.sum(mate * mate, axis=1, keepdims=True)
    scale = lax.rsqrt(square / (2 * half_model) + EPS)
    low_rank = None
    for side, value in ((me, own), (1 - me, mate)):
        start = pl.multiple_of(side * half_model, half_model)
        normed = (value * scale * gain_ref[:, pl.ds(start, half_model)]).astype(jnp.bfloat16)
        part = lax.dot_general(
            normed, down_ref[:, pl.ds(start, half_model)], BY_COLUMNS, preferred_element_type=jnp.float32
        )
        low_rank = part if low_rank is None else low_rank + part
        for k in range(pieces // 2):
            away = lax.rem(side * (pieces // 2) + k - line + pieces, pieces)
            for offset, out_ref in enumerate(out_refs):

                @pl.when(away == offset)
                def _():
                    out_ref[:, :cut] = normed[:, k * cut : (k + 1) * cut]

    mine = _parts(fade_ref[pl.ds(pl.multiple_of(me * rows, rows), rows), :])
    theirs = mate_ref[:, half_model : half_model + fades].astype(jnp.float32)
    tail = jnp.concatenate(
        [
            low_rank.astype(jnp.bfloat16).astype(jnp.float32),
            jnp.where(me == 0, mine, theirs),
            jnp.where(me == 0, theirs, mine),
            jnp.zeros((rows, wide - cut - low_rank.shape[1] - 2 * fades), jnp.float32),
        ],
        axis=1,
    ).astype(jnp.bfloat16)
    for out_ref in out_refs:
        out_ref[:, cut:] = tail


def collect_kernel(place_ref, *refs):
    pieces = len(refs) - 1
    for offset in range(pieces):
        refs[-1][lax.rem(place_ref[3] - offset + pieces, pieces)] = refs[offset][...]


def collect(place, parts):
    rows, wide = parts[0].shape
    return _call(
        collect_kernel,
        jax.ShapeDtypeStruct((len(parts), rows, wide), parts[0].dtype),
        10**8,
        2**21,
        in_specs=[SMEM] + [VMEM] * len(parts),
        out_specs=VMEM,
    )(place, *parts)


def join_kernel(place_ref, kept_ref, given_ref, *out_refs):
    pieces = len(out_refs)
    rows = out_refs[0].shape[0]
    for offset, out_ref in enumerate(out_refs):
        at = pl.ds(pl.multiple_of(lax.rem(place_ref[3] + offset, pieces) * rows, rows), rows)
        out_ref[...] = (kept_ref[at].astype(jnp.float32) + given_ref[at].astype(jnp.float32)).astype(out_ref.dtype)


def join(place, kept, given, pieces):
    rows, columns = kept.shape
    return _call(
        join_kernel,
        [jax.ShapeDtypeStruct((rows // pieces, columns), kept.dtype)] * pieces,
        10**8,
        2**21,
        in_specs=[SMEM, VMEM, VMEM],
        out_specs=[VMEM] * pieces,
    )(place, kept, given)


def spread_kernel(place_ref, *refs):
    pieces = len(refs) - 1
    columns = refs[0].shape[1]
    for offset in range(pieces):
        start = lax.rem(place_ref[3] - offset + pieces, pieces) * columns
        refs[-1][:, pl.ds(pl.multiple_of(start, columns), columns)] = refs[offset][...]


def spread(place, parts):
    rows, columns = parts[0].shape
    return _call(
        spread_kernel,
        jax.ShapeDtypeStruct((rows, len(parts) * columns), parts[0].dtype),
        10**8,
        2**21,
        in_specs=[SMEM] + [VMEM] * len(parts),
        out_specs=VMEM,
    )(place, *parts)


def to_offsets(parts):
    peers = len(parts)
    out = [parts[0]]
    for k in range(1, peers):
        out.append(lax.ppermute(parts[k], "sp", [(i, (i + k) % peers) for i in range(peers)]))
    return out


def pack_kernel(key_heads, side_ref, wq, wk, wv, lq, lk, lv, out_ref):
    step = pl.program_id(0)
    half = out_ref.shape[2] // 2
    keys_and_values = step == 0
    queries = (step > 0) & (step <= key_heads)
    head_items = (step > key_heads) & ((step - key_heads) % 2 == 1)
    head_values = (step > key_heads) & ((step - key_heads) % 2 == 0)

    @pl.when(keys_and_values)
    def _():
        out_ref[0, :, :half] = wk[...]
        out_ref[0, :, half:] = wv[...]

    @pl.when(queries)
    def _():
        out_ref[0] = wq[...]

    @pl.when(head_items)
    def _():
        out_ref[0, :, :half] = lq[...]
        out_ref[0, :, half:] = lk[...]

    @pl.when(head_values)
    def _():
        out_ref[0] = lv[...]


def pack_items(side, lin, key_heads, matrices):
    depth = matrices[0].shape[0]
    width = 2 * LOOKUP_FEATURES
    count = 1 + key_heads + 2 * lin
    fixed = pl.BlockSpec((depth, width // 2), lambda i, side: (0, side[0]))
    query = pl.BlockSpec(
        (depth, width), lambda i, side: (0, side[0] * key_heads + jnp.clip(i - 1, 0, key_heads - 1))
    )
    head = lambda i, side: (0, side[0] * lin + jnp.clip((i - 1 - key_heads) // 2, 0, lin - 1))
    narrow, full = pl.BlockSpec((depth, width // 2), head), pl.BlockSpec((depth, width), head)
    return _call(
        functools.partial(pack_kernel, key_heads),
        jax.ShapeDtypeStruct((count, depth, width), jnp.bfloat16),
        10**11,
        4 * count * depth * width,
        grid_spec=_prefetch(
            1,
            (count,),
            [query, fixed, fixed, narrow, narrow, full],
            pl.BlockSpec((1, depth, width), lambda i, side: (i, 0, 0)),
        ),
    )(side, *matrices)


def partial_kernel(index_ref, mine_ref, theirs_ref, own_ref, other_ref, *rest):
    out_ref, weight, arrival = rest[-3:]
    rows = mine_ref.shape[0]
    depth, width = weight.shape
    copy = pltpu.make_async_copy(other_ref.at[index_ref[0]], weight, arrival)
    copy.start()
    for half in range(2):
        if half == 1:
            copy.wait()
        for top, x_ref in enumerate((mine_ref, theirs_ref)):
            at = slice(top * rows, (top + 1) * rows)
            span = slice(half * width, (half + 1) * width)
            matrix = own_ref[index_ref[0]] if half == 0 else weight[...]
            total = jnp.dot(x_ref[:, :depth], matrix, preferred_element_type=jnp.float32)
            if len(rest) == 4:
                total = total + rest[0][at, span].astype(jnp.float32)
            out_ref[at, span] = total.astype(out_ref.dtype)


def partial_sum(index, mine, theirs, own, other, arrived):
    rows = mine.shape[0]
    _, depth, width = own.shape
    operands = [mine, theirs, own, other] + ([] if arrived is None else [arrived])
    return _call(
        partial_kernel,
        jax.ShapeDtypeStruct((2 * rows, 2 * width), jnp.bfloat16),
        160 * rows * depth * width,
        4 * depth * (rows + width),
        in_specs=[SMEM, VMEM, VMEM, VMEM, ANY] + [VMEM] * (len(operands) - 4),
        out_specs=VMEM,
        scratch_shapes=[pltpu.VMEM((depth, width), jnp.bfloat16), pltpu.SemaphoreType.DMA],
    )(index, *operands)


def decay_kernel(lin, rank, place_ref, mine_ref, theirs_ref, own_ref, other_ref, *out_refs):
    me, side = place_ref[0], place_ref[1]
    rows = mine_ref.shape[0]
    features = LOOKUP_FEATURES
    lower = (
        lax.broadcasted_iota(jnp.int32, (SPAN, SPAN), 0) >= lax.broadcasted_iota(jnp.int32, (SPAN, SPAN), 1)
    ).astype(jnp.bfloat16)
    for top, tail_ref in enumerate((mine_ref, theirs_ref)):
        tail = tail_ref[:, tail_ref.shape[1] - features :]
        low_rank = tail[:, :rank]
        parts = [
            tail[:, rank + k * 2 * lin : rank + (k + 1) * 2 * lin].astype(jnp.float32) for k in range(6)
        ]
        by_core = [parts[0] + parts[1] + parts[2], parts[3] + parts[4] + parts[5]]
        fades = [jnp.where(me == 0, by_core[0], by_core[1]), jnp.where(me == 0, by_core[1], by_core[0])]
        for head in range(lin):
            for owner, small_ref in enumerate((own_ref, other_ref)):
                at = pl.ds(pl.multiple_of((side * lin + head) * features, features), features)
                up = small_ref[:rank, at].astype(jnp.bfloat16)
                energy = jnp.dot(low_rank, up, preferred_element_type=jnp.float32) + small_ref[rank : rank + 1, at]
                soft = jnp.minimum(energy, 0.0) - jnp.log1p(jnp.exp(-jnp.abs(energy)))
                both = fades[owner]
                fade = jnp.where(side == 0, both[:, head : head + 1], both[:, lin + head : lin + head + 1])
                step = soft * (1.0 / FADING_SOFTNESS) + fade
                high = step.astype(jnp.bfloat16)
                rest = step - high.astype(jnp.float32)
                middle = rest.astype(jnp.bfloat16)
                low = (rest - middle.astype(jnp.float32)).astype(jnp.bfloat16)
                column = owner * features
                out_ref = out_refs[head]
                for span in range(rows // SPAN):
                    cut = slice(span * SPAN, (span + 1) * SPAN)
                    out_ref[top * rows + span * SPAN : top * rows + (span + 1) * SPAN, column : column + features] = (
                        jnp.dot(lower, high[cut], preferred_element_type=jnp.float32)
                        + jnp.dot(lower, middle[cut], preferred_element_type=jnp.float32)
                        + jnp.dot(lower, low[cut], preferred_element_type=jnp.float32)
                    )


def decay_sums(place, lin, rank, mine, theirs, own, other):
    return _call(
        functools.partial(decay_kernel, lin, rank),
        [jax.ShapeDtypeStruct((2 * mine.shape[0], 2 * LOOKUP_FEATURES), jnp.float32)] * lin,
        10**9,
        2**20,
        in_specs=[SMEM] + [VMEM] * 4,
        out_specs=[VMEM] * lin,
    )(place, mine, theirs, own, other)


def linear_kernel(lin, head, half, place_ref, query_key_ref, value_ref, running_ref, own_ref, other_ref, gain_ref, out_ref):
    me, side = place_ref[0], place_ref[1]
    rows, width = query_key_ref.shape
    features = LOOKUP_FEATURES
    values = width // 2
    lower = lax.broadcasted_iota(jnp.int32, (SPAN, SPAN), 0) >= lax.broadcasted_iota(
        jnp.int32, (SPAN, SPAN), 1
    )
    states = [state_ref[side * lin + head].T for state_ref in (own_ref, other_ref)]
    for span in range(rows // SPAN):
        per = half // SPAN
        device, inside = span // (2 * per), span % (2 * per)
        apart = jnp.where(me == inside // per, 0, rows // 2)
        at = pl.ds(pl.multiple_of(apart + device * half + (inside % per) * SPAN, SPAN), SPAN)
        for owner in range(2):
            base = owner * values
            running = running_ref[at, owner * features : (owner + 1) * features]
            query = query_key_ref[at, base : base + features].astype(jnp.float32)
            key = query_key_ref[at, base + features : base + 2 * features].astype(jnp.float32)
            value = value_ref[at, base : base + values]
            end = running[SPAN - 1 : SPAN]
            scaled = (query * features ** (-0.5) * jnp.exp(running)).astype(jnp.bfloat16)
            inverse = (key * jnp.exp(-running)).astype(jnp.bfloat16)
            ending = (key * jnp.exp(end - running)).astype(jnp.bfloat16)
            inner = lax.dot_general(scaled, inverse, BY_COLUMNS, preferred_element_type=jnp.float32)
            inner = jnp.where(lower, inner, 0.0).astype(jnp.bfloat16)
            state = states[owner]
            raw = jnp.dot(inner, value, preferred_element_type=jnp.float32) + lax.dot_general(
                scaled, state.astype(jnp.bfloat16), BY_COLUMNS, preferred_element_type=jnp.float32
            )
            states[owner] = state * jnp.exp(end) + lax.dot_general(
                value, ending, BY_ROWS, preferred_element_type=jnp.float32
            )
            scale = lax.rsqrt(jnp.mean(raw * raw, axis=-1, keepdims=True) + EPS)
            out_ref[at, base : base + values] = (raw * scale * gain_ref[...]).astype(out_ref.dtype)


def linear_heads(place, lin, head, half, query_key, value, running, own, other, gain):
    return _call(
        functools.partial(linear_kernel, lin, head, half),
        jax.ShapeDtypeStruct(query_key.shape, jnp.bfloat16),
        2 * 10**9,
        2**21,
        in_specs=[SMEM] + [VMEM] * 6,
        out_specs=VMEM,
    )(place, query_key, value, running, own, other, gain)


def window_kernel(group, half, place_ref, slope_ref, sink_ref, key_value_ref, query_ref, out_ref):
    me = place_ref[0]
    rows = query_ref.shape[0]
    owners, groups = slope_ref.shape
    pair = key_value_ref.shape[1] // (2 * owners)
    from_query = lax.broadcasted_iota(jnp.int32, (WINDOW, WINDOW), 0)
    from_key = lax.broadcasted_iota(jnp.int32, (WINDOW, WINDOW), 1)
    present = from_key <= from_query
    distance = jnp.where(present, from_query - from_key, from_query - from_key + WINDOW).astype(jnp.float32)
    unit = min(half, WINDOW)

    def places(block):
        out = []
        for piece in range(WINDOW // unit):
            start = block * WINDOW + piece * unit
            device, inside = start // (2 * half), start % (2 * half)
            apart = jnp.where(me == inside // half, 0, rows // 2)
            out.append(pl.ds(pl.multiple_of(apart + device * half + inside % half, unit), unit))
        return out

    for owner in range(owners):
        key_at = owner * 2 * pair + group * HD
        value_at = key_at + pair
        base = owner * groups * HD
        biases = [slope_ref[owner, head] * distance for head in range(groups)]
        past_keys, past_values = None, None
        for block in range(rows // WINDOW):
            first = block == 0
            at = places(block)
            keys = jnp.concatenate([key_value_ref[a, key_at : key_at + HD] for a in at], axis=0)
            values = jnp.concatenate([key_value_ref[a, value_at : value_at + HD] for a in at], axis=0)
            band_keys = keys if first else jnp.concatenate([past_keys, keys], axis=0)
            band_values = values if first else jnp.concatenate([past_values, values], axis=0)
            past_keys, past_values = keys, values
            queries = jnp.concatenate(
                [query_ref[a, base + head * HD : base + (head + 1) * HD] for head in range(groups) for a in at],
                axis=0,
            )
            scores = lax.dot_general(queries, band_keys, BY_COLUMNS, preferred_element_type=jnp.float32)
            probs = []
            for head in range(groups):
                mine = scores[head * WINDOW : (head + 1) * WINDOW]
                if first:
                    weight = jnp.where(present, jnp.exp(mine * HD ** (-0.5) - biases[head]), 0.0)
                else:
                    score = jnp.where(present, mine[:, WINDOW:], mine[:, :WINDOW])
                    weight = jnp.exp(score * HD ** (-0.5) - biases[head])
                total = jnp.sum(weight, axis=-1, keepdims=True) + sink_ref[owner, head]
                share = weight / total
                if first:
                    probs.append(share.astype(jnp.bfloat16))
                else:
                    probs.append(
                        jnp.concatenate(
                            [
                                jnp.where(present, 0.0, share).astype(jnp.bfloat16),
                                jnp.where(present, share, 0.0).astype(jnp.bfloat16),
                            ],
                            axis=1,
                        )
                    )
            outs = jnp.dot(jnp.concatenate(probs, axis=0), band_values, preferred_element_type=jnp.float32)
            joined = jnp.concatenate(
                [outs[head * WINDOW : (head + 1) * WINDOW] for head in range(groups)], axis=1
            ).astype(out_ref.dtype)
            for piece, a in enumerate(at):
                out_ref[a, base : base + groups * HD] = joined[piece * unit : (piece + 1) * unit]


def window_heads(place, group, half, slopes, sinks, key_value, query):
    return _call(
        functools.partial(window_kernel, group, half),
        jax.ShapeDtypeStruct(query.shape, jnp.bfloat16),
        2 * 10**9,
        2**21,
        in_specs=[SMEM, SMEM, SMEM, VMEM, VMEM],
        out_specs=VMEM,
    )(place, slopes, sinks, key_value, query)


def output_kernel(sources, place_ref, *refs):
    count = 1 + max(max(row) for row in sources)
    pieces = len(sources)
    passed = refs[:count]
    own_ref, other_ref = refs[count : count + 2]
    held, arrival = refs[-2:]
    rest = refs[count + 2 : -2]
    split = rest[-1].shape[0] != held.shape[1]
    outs = rest[-2:] if split else rest[-1:]
    before = rest[: len(rest) - len(outs)]
    depth = place_ref[2]
    for at in range(len(sources[0])):

        @pl.when(depth == at)
        def _():
            for piece in range(pieces):
                pltpu.make_async_copy(passed[sources[piece][at]], held.at[piece], arrival.at[piece]).start()

    for piece in range(pieces):
        pltpu.make_async_copy(passed[0], held.at[piece], arrival.at[piece]).wait()
    width = held.shape[2] // 2
    rows = outs[0].shape[0]
    columns = outs[0].shape[1]
    block = columns // 2
    for top, out_ref in enumerate(outs):
        at = slice(top * rows, (top + 1) * rows)
        for part in range(2):
            span = slice(part * block, (part + 1) * block)
            total = before[0][at, span] if before else jnp.zeros((rows, block), jnp.float32)
            for piece in range(pieces):
                lines = slice(piece * width, (piece + 1) * width)
                total = total + jnp.dot(
                    held[piece, at, :width], own_ref[lines, span], preferred_element_type=jnp.float32
                )
                total = total + jnp.dot(
                    held[piece, at, width:], other_ref[lines, span], preferred_element_type=jnp.float32
                )
            out_ref[:, span] = total.astype(out_ref.dtype)


def output_sum(place, passed, sources, own, other, before, split):
    rows, width = passed[0].shape
    pieces = len(sources)
    lines, columns = other.shape
    kind, parts = (jnp.bfloat16, 2) if split else (jnp.float32, 1)
    whole = pl.BlockSpec((rows, columns), lambda i, place: (0, 0))
    out = pl.BlockSpec((rows // parts, columns), lambda i, place: (0, 0))
    return _call(
        functools.partial(output_kernel, sources),
        [jax.ShapeDtypeStruct((rows // parts, columns), kind)] * parts,
        4 * rows * columns * lines,
        8 * rows * columns,
        grid_spec=_prefetch(
            1,
            (1,),
            [ANY] * len(passed)
            + [
                pl.BlockSpec((lines, columns), lambda i, place: (place[1], 0)),
                pl.BlockSpec((lines, columns), lambda i, place: (0, 0)),
            ]
            + ([] if before is None else [whole]),
            [out] * parts,
            [pltpu.VMEM((pieces, rows, width), jnp.bfloat16), pltpu.SemaphoreType.DMA((pieces,))],
        ),
    )(place, *passed, own, other, *([] if before is None else [before]))


def resident(
    activations,
    input_norm_gain,
    window_query_weight,
    window_key_weight,
    window_value_weight,
    linear_query_weight,
    linear_key_weight,
    linear_value_weight,
    decay_down_factor,
    decay_up_factor,
    decay_offset_bias,
    extra_fading_exponent,
    starting_state,
    head_sink_logit,
    linear_head_gain,
    window_output_weight,
    linear_output_weight,
):
    peers = lax.axis_size("sp")
    hops = peers - 1
    line, me = lax.axis_index("sp"), lax.axis_index("tp")
    depth = jnp.where(me == 0, line, hops - line)
    far, near = 1 - me, me
    place = jnp.stack([me, far, hops - depth, line]).astype(jnp.int32)
    rows, half_model = activations.shape
    half = rows // 2
    bf16, f32 = jnp.bfloat16, jnp.float32
    lin = extra_fading_exponent.shape[1] // 2
    key_heads = window_key_weight.shape[1] // HD // 2
    query_heads = window_query_weight.shape[1] // HD // 2
    groups = query_heads // key_heads
    rank = decay_down_factor.shape[1]

    def swap(value):
        return lax.ppermute(value, "tp", SWAP)


    message = _call(
        message_kernel,
        jax.ShapeDtypeStruct((half, half_model + LOOKUP_FEATURES), bf16),
        10**11,
        2**20,
        in_specs=[SMEM, VMEM, VMEM],
        out_specs=VMEM,
    )(place, activations, extra_fading_exponent)
    mate = swap(message)
    wide = 2 * half_model // peers + LOOKUP_FEATURES
    outgoing = _call(
        norm_kernel,
        [jax.ShapeDtypeStruct((half, wide), bf16)] * peers,
        10**11,
        2**21,
        in_specs=[SMEM] + [VMEM] * 5,
        out_specs=[VMEM] * peers,
    )(place, activations, extra_fading_exponent, mate, input_norm_gain.reshape(1, -1), decay_down_factor.T)

    (
        outgoing,
        matrices,
        window_output_weight,
        linear_output_weight,
        starting_state,
        decay_up_factor,
        decay_offset_bias,
        head_sink_logit,
    ) = lax.optimization_barrier(
        (
            outgoing,
            (
                window_query_weight,
                window_key_weight,
                window_value_weight,
                linear_query_weight,
                linear_key_weight,
                linear_value_weight,
            ),
            window_output_weight,
            linear_output_weight,
            starting_state,
            decay_up_factor,
            decay_offset_bias,
            head_sink_logit,
        )
    )
    incoming = to_offsets(outgoing)
    packed = pack_items(near.reshape(1), lin, key_heads, matrices)
    other_in = swap(packed)
    own_in = pack_items(far.reshape(1), lin, key_heads, matrices)
    features = decay_up_factor.shape[1]
    own_small = jnp.concatenate(
        [
            decay_up_factor.astype(f32),
            decay_offset_bias.reshape(1, features),
            jnp.pad(head_sink_logit, (0, features - head_sink_logit.shape[0])).reshape(1, features),
            jnp.zeros((6, features), f32),
        ],
        axis=0,
    )
    other_small = swap(own_small)
    other_state = swap(starting_state)
    lines = linear_output_weight.shape[0] // 2
    other_linear = lax.dynamic_slice_in_dim(linear_output_weight, near * lines, lines, axis=0)
    other_linear = swap(other_linear)
    lines = window_output_weight.shape[0] // 2
    other_window = lax.dynamic_slice_in_dim(window_output_weight, near * lines, lines, axis=0)
    other_window = swap(other_window)

    incoming = collect(place, incoming)
    mine = incoming.reshape(peers * half, wide)
    theirs = swap(incoming).reshape(peers * half, wide)

    count = 1 + key_heads + 2 * lin
    arrived, finals = {}, []
    for step in range(count + 2 * hops):
        index = jnp.clip(step - 2 * depth, 0, count - 1).astype(jnp.int32).reshape(1)
        value = partial_sum(index, mine, theirs, own_in, other_in, arrived.get(step - 2))
        depths = [d for d in range(hops) if 0 <= step - 2 * d < count]
        if depths:
            arrived[step] = lax.ppermute(value, ("sp", "tp"), _pairs(peers, depths, 0))
        if step >= 2 * hops:
            finals.append(value)

    running = decay_sums(place, lin, rank, mine, theirs, own_small, other_small)
    sinks = jnp.stack(
        [
            lax.dynamic_slice_in_dim(small[rank + 1], far * query_heads, query_heads).reshape(key_heads, groups)
            for small in (own_small, other_small)
        ]
    )
    sinks = jnp.exp(sinks)
    attended = []
    for group in range(key_heads):
        number = jnp.stack([me, 1 - me])[:, None] * (2 * query_heads) + (
            far * query_heads + group * groups + jnp.arange(groups, dtype=jnp.int32)
        )
        slopes = jnp.exp2(-8.0 * (number + 1).astype(f32) / QH)
        attended.append(
            window_heads(place, group, half, slopes, sinks[:, group], finals[0], finals[1 + group])
        )
    for head in range(lin):
        attended.append(
            linear_heads(
                place,
                lin,
                head,
                half,
                finals[1 + key_heads + 2 * head],
                finals[2 + key_heads + 2 * head],
                running[head],
                starting_state,
                other_state,
                linear_head_gain.reshape(1, DV),
            )
        )

    pieces = len(attended)
    held = []
    for piece in range(pieces):
        seen = [attended[piece]]
        for hop in range(hops):
            if piece < pieces - 1:
                seen.append(lax.ppermute(seen[-1], ("sp", "tp"), _pairs(peers, [hop], 1)))
            else:
                last = hops - hop
                pairs = [(hops * 2, (hops - last) * 2), (1, last * 2 + 1)]
                seen.insert(1, lax.ppermute(seen[0], ("sp", "tp"), pairs))
        held.append(seen)
    table = lambda count: tuple(tuple(range(k * peers, (k + 1) * peers)) for k in range(count))
    flat = lambda lists: [value for seen in lists for value in seen]
    (terms,) = output_sum(
        place, flat(held[:key_heads]), table(key_heads), window_output_weight, other_window, None, False
    )
    kept, given = output_sum(
        place, flat(held[key_heads:]), table(lin), linear_output_weight, other_linear, terms, True
    )

    return spread(place, to_offsets(join(place, kept, swap(given), peers)))


def fits(mesh):
    return mesh.shape["tp"] == 2 and mesh.shape["sp"] > 1


def solution(mesh):
    placed = (
        P(("fs", "sp"), "tp"),
        P(),
        P("sp", "tp"),
        P("sp", "tp"),
        P("sp", "tp"),
        P("sp", "tp"),
        P("sp", "tp"),
        P("sp", "tp"),
        P(),
        P(None, "tp"),
        P("tp"),
        P(("fs", "sp"), "tp"),
        P("tp", None, None),
        P("tp"),
        P(),
        P("tp", "sp"),
        P("tp", "sp"),
    )
    if not fits(mesh):
        return jax.shard_map(
            local, mesh=mesh, in_specs=placed, out_specs=P(("fs", "sp", "tp"), None), check_vma=False
        )

    return jax.shard_map(resident, mesh=mesh, in_specs=placed, out_specs=P(("fs", "sp", "tp"), None), check_vma=False)
```

```python
import functools

import jax
import jax.numpy as jnp
from jax import lax
from jax.experimental import pallas as pl
from jax.experimental.pallas import tpu as pltpu
from jax.sharding import PartitionSpec as P


QH = 32
HD = 64
WINDOW = 128
LOOKUP_FEATURES = 128
DV = 256
SPAN = 64


EPS = 1e-05
FADING_SOFTNESS = 16.0
HIGH_PRECISION = lax.Precision.HIGHEST


def passed_along(value, axis, steps):
    count = lax.axis_size(axis)
    leading, last = (max(0, -steps), min(count, count - steps))
    return lax.ppermute(value, axis, [(source, source + steps) for source in range(leading, last)])


def prefix(x, axis, combine, identity):
    peers, place = (lax.axis_size(axis), lax.axis_index(axis))
    everything = jax.tree.map(
        lambda part, kind: lax.all_gather(part.astype(kind), axis), x, (jnp.bfloat16, jnp.bfloat16)
    )
    start = jax.tree.map(
        lambda part, zero: jnp.broadcast_to(jnp.asarray(zero, part.dtype), part.shape), x, identity
    )

    def hop(k, before):
        reached = k < place
        new = combine(
            before, jax.tree.map(lambda part, own: part[k].astype(own.dtype), everything, x)
        )
        return jax.tree.map(lambda a, b: jnp.where(reached, a, b), new, before)

    return lax.fori_loop(0, peers, hop, start)


def window_attention(near_query, near_keys, near_values, head_sink_logit):
    stream_extent = near_query.shape[0]
    key_heads = near_keys.shape[1] // HD
    heads_here = near_query.shape[1] // HD
    groups = heads_here // key_heads
    blocks = stream_extent // WINDOW
    tail_rows = jnp.stack([near_keys, near_values])
    before = passed_along(tail_rows, "sp", 1)

    def banded(previous, current):
        extended = jnp.concatenate([previous, current], axis=0)
        earlier = extended[:stream_extent].reshape(blocks, WINDOW, key_heads, HD)
        present = extended[WINDOW:].reshape(blocks, WINDOW, key_heads, HD)
        return jnp.concatenate([earlier, present], axis=1)

    key_band = banded(before[0], near_keys)
    value_band = banded(before[1], near_values)
    queries = near_query.reshape(blocks, WINDOW, key_heads, groups, HD)
    scores = jnp.einsum(
        "nqhgd,nkhd->hgnqk", queries, key_band, preferred_element_type=jnp.float32
    ) * HD ** (-0.5)
    head_ids = lax.axis_index("tp") * heads_here + jnp.arange(heads_here, dtype=jnp.int32)
    slopes = jnp.exp2(-8.0 * (head_ids + 1).astype(jnp.float32) / QH).reshape(key_heads, groups)
    query_pos = jnp.arange(WINDOW, dtype=jnp.int32)
    key_pos = jnp.arange(2 * WINDOW, dtype=jnp.int32)
    distance = query_pos[:, None] - key_pos[None, :] + WINDOW
    start_pos = (
        lax.axis_index("sp") * stream_extent + (jnp.arange(blocks, dtype=jnp.int32) - 1) * WINDOW
    )
    absolute = start_pos[:, None] + key_pos[None, :]
    allowed = ((distance >= 0) & (distance < WINDOW))[None] & (absolute >= 0)[:, None, :]
    biased = scores - slopes[:, :, None, None, None] * distance.astype(jnp.float32)
    weights = jnp.where(allowed, jnp.exp(biased), 0.0)
    denominator = (
        jnp.sum(weights, axis=-1, keepdims=True)
        + jnp.exp(head_sink_logit.reshape(key_heads, groups))[:, :, None, None, None]
    )
    attention = (weights / denominator).astype(jnp.bfloat16)
    attended = jnp.einsum(
        "hgnqk,nkhd->nqhgd", attention, value_band, preferred_element_type=jnp.float32
    )
    return attended.reshape(stream_extent, heads_here * HD).astype(jnp.bfloat16)


def linear_attention(
    gated_query, gated_keys, gated_values, fading_exponent, linear_head_gain, starting_state
):
    stream_extent = gated_query.shape[0]
    head_total = gated_query.shape[1] // LOOKUP_FEATURES
    span_count = stream_extent // SPAN
    scaled_query = gated_query.astype(jnp.float32).reshape(
        span_count, SPAN, head_total, LOOKUP_FEATURES
    ) * LOOKUP_FEATURES ** (-0.5)
    keys_wide = gated_keys.astype(jnp.float32).reshape(
        span_count, SPAN, head_total, LOOKUP_FEATURES
    )
    values_wide = gated_values.astype(jnp.float32).reshape(span_count, SPAN, head_total, DV)
    running = jnp.cumsum(
        fading_exponent.reshape(span_count, SPAN, head_total, LOOKUP_FEATURES), axis=1
    )
    span_end = running[:, -1]
    query_with_decay = scaled_query * jnp.exp(running)
    inverse_keys = keys_wide * jnp.exp(-running)
    ending_keys = keys_wide * jnp.exp(span_end[:, None] - running)
    inner = jnp.einsum("nchk,nshk->nhcs", query_with_decay, inverse_keys, precision=HIGH_PRECISION)
    lower = jnp.tril(jnp.ones((SPAN, SPAN), dtype=bool))
    inner = jnp.where(lower, inner, 0.0)
    within = jnp.einsum("nhcs,nshv->nchv", inner, values_wide, precision=HIGH_PRECISION)

    def advance(running_state, inputs):
        query_portion, key_portion, value_portion, scale_factor = inputs
        layer_output = jnp.einsum(
            "fmy,mys->fms", query_portion, running_state, precision=HIGH_PRECISION
        )
        running_state = running_state * scale_factor[..., None] + jnp.einsum(
            "gxp,gxz->xpz", key_portion, value_portion, precision=HIGH_PRECISION
        )
        return (running_state, layer_output)

    start_state = jnp.zeros((head_total, LOOKUP_FEATURES, DV), jnp.float32)
    state_end, carried = lax.scan(
        advance, start_state, (query_with_decay, ending_keys, values_wide, jnp.exp(span_end))
    )
    device_decay = jnp.exp(jnp.sum(span_end, axis=0))
    prefix_sums = jnp.cumsum(span_end, axis=0) - span_end

    def combine(earlier, later):
        return (earlier[0] * later[0], later[0][..., None] * earlier[1] + later[1])

    decay_before, state_before = prefix(
        (device_decay, state_end),
        "sp",
        combine,
        (jnp.ones_like(device_decay), jnp.zeros_like(state_end)),
    )
    incoming_rows = state_before + decay_before[..., None] * starting_state
    crossing = jnp.einsum(
        "qwso,soz->qwsz",
        query_with_decay * jnp.exp(prefix_sums)[:, None],
        incoming_rows,
        precision=HIGH_PRECISION,
    )
    flat = (within + carried + crossing).reshape(stream_extent, head_total, DV)
    normal = (
        flat * lax.rsqrt(jnp.mean(flat * flat, axis=-1, keepdims=True) + EPS) * linear_head_gain
    )
    return normal.reshape(stream_extent, head_total * DV).astype(jnp.bfloat16)


def local(
    activations,
    input_norm_gain,
    window_query_weight,
    window_key_weight,
    window_value_weight,
    linear_query_weight,
    linear_key_weight,
    linear_value_weight,
    decay_down_factor,
    decay_up_factor,
    decay_offset_bias,
    extra_fading_exponent,
    starting_state,
    head_sink_logit,
    linear_head_gain,
    window_output_weight,
    linear_output_weight,
):
    gathered = lax.all_gather(activations, "tp", axis=1, tiled=True)
    widened = gathered.astype(jnp.float32)
    normed = (
        widened
        * lax.rsqrt(jnp.mean(widened * widened, axis=1, keepdims=True) + EPS)
        * input_norm_gain
    ).astype(jnp.bfloat16)
    row_total = normed.shape[0]
    matrices = (
        window_query_weight,
        window_key_weight,
        window_value_weight,
        linear_query_weight,
        linear_key_weight,
        linear_value_weight,
    )
    segments = (
        lax.all_gather(matrices[0], "sp", axis=0, tiled=True),
        lax.all_gather(matrices[1], "sp", axis=0, tiled=True),
        lax.all_gather(matrices[2], "sp", axis=0, tiled=True),
        lax.all_gather(matrices[3], "sp", axis=0, tiled=True),
        lax.all_gather(matrices[4], "sp", axis=0, tiled=True),
        lax.all_gather(matrices[5], "sp", axis=0, tiled=True),
    )
    projected = tuple(
        (jnp.dot(normed, segment, preferred_element_type=jnp.float32) for segment in segments)
    )
    near_query, near_keys, near_values, gated_query, gated_keys, gated_values = [
        product.astype(jnp.bfloat16) for product in projected
    ]
    low_rank = jnp.dot(normed, decay_down_factor, preferred_element_type=jnp.float32).astype(
        jnp.bfloat16
    )
    attention_energies = (
        jnp.dot(low_rank, decay_up_factor, preferred_element_type=jnp.float32) + decay_offset_bias
    )
    head_total = extra_fading_exponent.shape[1]
    fading_exponent = (jax.nn.log_sigmoid(attention_energies) / FADING_SOFTNESS).reshape(
        row_total, head_total, LOOKUP_FEATURES
    ) + extra_fading_exponent[:, :, None]
    near_out = window_attention(near_query, near_keys, near_values, head_sink_logit)
    gated_out = linear_attention(
        gated_query, gated_keys, gated_values, fading_exponent, linear_head_gain, starting_state
    )
    window_full, linear_full = (
        lax.all_gather(window_output_weight, "sp", axis=1, tiled=True),
        lax.all_gather(linear_output_weight, "sp", axis=1, tiled=True),
    )
    return lax.psum_scatter(
        (
            jnp.dot(near_out, window_full, preferred_element_type=jnp.float32)
            + jnp.dot(gated_out, linear_full, preferred_element_type=jnp.float32)
        ).astype(jnp.bfloat16),
        "tp",
        scatter_dimension=0,
        tiled=True,
    )


def _pairs(peers, depths, core):
    out = []
    for d in depths:
        out.append((d * 2 + core, (d + 1) * 2 + core))
        out.append(((peers - 1 - d) * 2 + 1 - core, (peers - 2 - d) * 2 + 1 - core))
    return out


SWAP = [(0, 1), (1, 0)]
VMEM = pl.BlockSpec(memory_space=pltpu.VMEM)
SMEM = pl.BlockSpec(memory_space=pltpu.SMEM)
ANY = pl.BlockSpec(memory_space=pl.ANY)
BY_COLUMNS = (((1,), (1,)), ((), ()))
BY_ROWS = (((0,), (0,)), ((), ()))


def _call(kernel, out_shape, flops, moved, grant=24, **kw):
    return pl.pallas_call(
        kernel,
        out_shape=out_shape,
        compiler_params=pltpu.CompilerParams(vmem_limit_bytes=grant * 1024 * 1024),
        cost_estimate=pl.CostEstimate(flops=flops, bytes_accessed=moved, transcendentals=0),
        **kw,
    )


def _prefetch(scalars, grid, in_specs, out_specs, scratch=()):
    return pltpu.PrefetchScalarGridSpec(
        num_scalar_prefetch=scalars, grid=grid, in_specs=in_specs, out_specs=out_specs, scratch_shapes=scratch
    )


def message_kernel(place_ref, x_ref, fade_ref, out_ref):
    rows, wide = out_ref.shape
    half_model = x_ref.shape[1]
    at = pl.ds(pl.multiple_of(place_ref[1] * rows, rows), rows)
    out_ref[:, :half_model] = x_ref[at, :]
    out_ref[:, half_model:] = jnp.concatenate(
        [_parts(fade_ref[at, :]), jnp.zeros((rows, wide - half_model - 3 * fade_ref.shape[1]), jnp.float32)], axis=1
    ).astype(out_ref.dtype)


def _parts(value):
    high = value.astype(jnp.bfloat16).astype(jnp.float32)
    rest = value - high
    middle = rest.astype(jnp.bfloat16).astype(jnp.float32)
    return jnp.concatenate([high, middle, rest - middle], axis=1)


def norm_kernel(place_ref, x_ref, fade_ref, mate_ref, gain_ref, down_ref, *out_refs):
    me, line = place_ref[0], place_ref[3]
    pieces = len(out_refs)
    rows, wide = out_refs[0].shape
    half_model = x_ref.shape[1]
    cut = 2 * half_model // pieces
    fades = 3 * fade_ref.shape[1]
    own = x_ref[pl.ds(pl.multiple_of(me * rows, rows), rows), :].astype(jnp.float32)
    mate = mate_ref[:, :half_model].astype(jnp.float32)
    square = jnp.sum(own * own, axis=1, keepdims=True) + jnp.sum(mate * mate, axis=1, keepdims=True)
    scale = lax.rsqrt(square / (2 * half_model) + EPS)
    low_rank = None
    for side, value in ((me, own), (1 - me, mate)):
        start = pl.multiple_of(side * half_model, half_model)
        normed = (value * scale * gain_ref[:, pl.ds(start, half_model)]).astype(jnp.bfloat16)
        part = lax.dot_general(
            normed, down_ref[:, pl.ds(start, half_model)], BY_COLUMNS, preferred_element_type=jnp.float32
        )
        low_rank = part if low_rank is None else low_rank + part
        for k in range(pieces // 2):
            away = lax.rem(side * (pieces // 2) + k - line + pieces, pieces)
            for offset, out_ref in enumerate(out_refs):

                @pl.when(away == offset)
                def _():
                    out_ref[:, :cut] = normed[:, k * cut : (k + 1) * cut]

    mine = _parts(fade_ref[pl.ds(pl.multiple_of(me * rows, rows), rows), :])
    theirs = mate_ref[:, half_model : half_model + fades].astype(jnp.float32)
    tail = jnp.concatenate(
        [
            low_rank.astype(jnp.bfloat16).astype(jnp.float32),
            jnp.where(me == 0, mine, theirs),
            jnp.where(me == 0, theirs, mine),
            jnp.zeros((rows, wide - cut - low_rank.shape[1] - 2 * fades), jnp.float32),
        ],
        axis=1,
    ).astype(jnp.bfloat16)
    for out_ref in out_refs:
        out_ref[:, cut:] = tail


def collect_kernel(place_ref, *refs):
    pieces = len(refs) - 1
    for offset in range(pieces):
        refs[-1][lax.rem(place_ref[3] - offset + pieces, pieces)] = refs[offset][...]


def collect(place, parts):
    rows, wide = parts[0].shape
    return _call(
        collect_kernel,
        jax.ShapeDtypeStruct((len(parts), rows, wide), parts[0].dtype),
        10**8,
        2**21,
        in_specs=[SMEM] + [VMEM] * len(parts),
        out_specs=VMEM,
    )(place, *parts)


def join_kernel(place_ref, kept_ref, given_ref, *out_refs):
    pieces = len(out_refs)
    rows = out_refs[0].shape[0]
    for offset, out_ref in enumerate(out_refs):
        at = pl.ds(pl.multiple_of(lax.rem(place_ref[3] + offset, pieces) * rows, rows), rows)
        out_ref[...] = (kept_ref[at].astype(jnp.float32) + given_ref[at].astype(jnp.float32)).astype(out_ref.dtype)


def join(place, kept, given, pieces):
    rows, columns = kept.shape
    return _call(
        join_kernel,
        [jax.ShapeDtypeStruct((rows // pieces, columns), kept.dtype)] * pieces,
        10**8,
        2**21,
        in_specs=[SMEM, VMEM, VMEM],
        out_specs=[VMEM] * pieces,
    )(place, kept, given)


def spread_kernel(place_ref, *refs):
    pieces = len(refs) - 1
    columns = refs[0].shape[1]
    for offset in range(pieces):
        start = lax.rem(place_ref[3] - offset + pieces, pieces) * columns
        refs[-1][:, pl.ds(pl.multiple_of(start, columns), columns)] = refs[offset][...]


def spread(place, parts):
    rows, columns = parts[0].shape
    return _call(
        spread_kernel,
        jax.ShapeDtypeStruct((rows, len(parts) * columns), parts[0].dtype),
        10**8,
        2**21,
        in_specs=[SMEM] + [VMEM] * len(parts),
        out_specs=VMEM,
    )(place, *parts)


def to_offsets(parts):
    peers = len(parts)
    out = [parts[0]]
    for k in range(1, peers):
        out.append(lax.ppermute(parts[k], "sp", [(i, (i + k) % peers) for i in range(peers)]))
    return out


def pack_kernel(key_heads, side_ref, wq, wk, wv, lq, lk, lv, out_ref):
    step = pl.program_id(0)
    half = out_ref.shape[2] // 2
    keys_and_values = step == 0
    queries = (step > 0) & (step <= key_heads)
    head_items = (step > key_heads) & ((step - key_heads) % 2 == 1)
    head_values = (step > key_heads) & ((step - key_heads) % 2 == 0)

    @pl.when(keys_and_values)
    def _():
        out_ref[0, :, :half] = wk[...]
        out_ref[0, :, half:] = wv[...]

    @pl.when(queries)
    def _():
        out_ref[0] = wq[...]

    @pl.when(head_items)
    def _():
        out_ref[0, :, :half] = lq[...]
        out_ref[0, :, half:] = lk[...]

    @pl.when(head_values)
    def _():
        out_ref[0] = lv[...]


def pack_items(side, lin, key_heads, matrices):
    depth = matrices[0].shape[0]
    width = 2 * LOOKUP_FEATURES
    count = 1 + key_heads + 2 * lin
    fixed = pl.BlockSpec((depth, width // 2), lambda i, side: (0, side[0]))
    query = pl.BlockSpec(
        (depth, width), lambda i, side: (0, side[0] * key_heads + jnp.clip(i - 1, 0, key_heads - 1))
    )
    head = lambda i, side: (0, side[0] * lin + jnp.clip((i - 1 - key_heads) // 2, 0, lin - 1))
    narrow, full = pl.BlockSpec((depth, width // 2), head), pl.BlockSpec((depth, width), head)
    return _call(
        functools.partial(pack_kernel, key_heads),
        jax.ShapeDtypeStruct((count, depth, width), jnp.bfloat16),
        10**11,
        4 * count * depth * width,
        grid_spec=_prefetch(
            1,
            (count,),
            [query, fixed, fixed, narrow, narrow, full],
            pl.BlockSpec((1, depth, width), lambda i, side: (i, 0, 0)),
        ),
    )(side, *matrices)


def partial_kernel(index_ref, mine_ref, theirs_ref, own_ref, other_ref, *rest):
    out_ref, weight, arrival = rest[-3:]
    rows = mine_ref.shape[0]
    depth, width = weight.shape
    copy = pltpu.make_async_copy(other_ref.at[index_ref[0]], weight, arrival)
    copy.start()
    for half in range(2):
        if half == 1:
            copy.wait()
        for top, x_ref in enumerate((mine_ref, theirs_ref)):
            at = slice(top * rows, (top + 1) * rows)
            span = slice(half * width, (half + 1) * width)
            matrix = own_ref[index_ref[0]] if half == 0 else weight[...]
            total = jnp.dot(x_ref[:, :depth], matrix, preferred_element_type=jnp.float32)
            if len(rest) == 4:
                total = total + rest[0][at, span].astype(jnp.float32)
            out_ref[at, span] = total.astype(out_ref.dtype)


def partial_sum(index, mine, theirs, own, other, arrived):
    rows = mine.shape[0]
    _, depth, width = own.shape
    operands = [mine, theirs, own, other] + ([] if arrived is None else [arrived])
    return _call(
        partial_kernel,
        jax.ShapeDtypeStruct((2 * rows, 2 * width), jnp.bfloat16),
        160 * rows * depth * width,
        4 * depth * (rows + width),
        in_specs=[SMEM, VMEM, VMEM, VMEM, ANY] + [VMEM] * (len(operands) - 4),
        out_specs=VMEM,
        scratch_shapes=[pltpu.VMEM((depth, width), jnp.bfloat16), pltpu.SemaphoreType.DMA],
    )(index, *operands)


def decay_kernel(lin, rank, place_ref, mine_ref, theirs_ref, own_ref, other_ref, *out_refs):
    me, side = place_ref[0], place_ref[1]
    rows = mine_ref.shape[0]
    features = LOOKUP_FEATURES
    lower = (
        lax.broadcasted_iota(jnp.int32, (SPAN, SPAN), 0) >= lax.broadcasted_iota(jnp.int32, (SPAN, SPAN), 1)
    ).astype(jnp.bfloat16)
    for top, tail_ref in enumerate((mine_ref, theirs_ref)):
        tail = tail_ref[:, tail_ref.shape[1] - features :]
        low_rank = tail[:, :rank]
        parts = [
            tail[:, rank + k * 2 * lin : rank + (k + 1) * 2 * lin].astype(jnp.float32) for k in range(6)
        ]
        by_core = [parts[0] + parts[1] + parts[2], parts[3] + parts[4] + parts[5]]
        fades = [jnp.where(me == 0, by_core[0], by_core[1]), jnp.where(me == 0, by_core[1], by_core[0])]
        for head in range(lin):
            for owner, small_ref in enumerate((own_ref, other_ref)):
                at = pl.ds(pl.multiple_of((side * lin + head) * features, features), features)
                up = small_ref[:rank, at].astype(jnp.bfloat16)
                energy = jnp.dot(low_rank, up, preferred_element_type=jnp.float32) + small_ref[rank : rank + 1, at]
                soft = jnp.minimum(energy, 0.0) - jnp.log1p(jnp.exp(-jnp.abs(energy)))
                both = fades[owner]
                fade = jnp.where(side == 0, both[:, head : head + 1], both[:, lin + head : lin + head + 1])
                step = soft * (1.0 / FADING_SOFTNESS) + fade
                high = step.astype(jnp.bfloat16)
                rest = step - high.astype(jnp.float32)
                middle = rest.astype(jnp.bfloat16)
                low = (rest - middle.astype(jnp.float32)).astype(jnp.bfloat16)
                column = owner * features
                out_ref = out_refs[head]
                for span in range(rows // SPAN):
                    cut = slice(span * SPAN, (span + 1) * SPAN)
                    out_ref[top * rows + span * SPAN : top * rows + (span + 1) * SPAN, column : column + features] = (
                        jnp.dot(lower, high[cut], preferred_element_type=jnp.float32)
                        + jnp.dot(lower, middle[cut], preferred_element_type=jnp.float32)
                        + jnp.dot(lower, low[cut], preferred_element_type=jnp.float32)
                    )


def decay_sums(place, lin, rank, mine, theirs, own, other):
    return _call(
        functools.partial(decay_kernel, lin, rank),
        [jax.ShapeDtypeStruct((2 * mine.shape[0], 2 * LOOKUP_FEATURES), jnp.float32)] * lin,
        10**9,
        2**20,
        in_specs=[SMEM] + [VMEM] * 4,
        out_specs=[VMEM] * lin,
    )(place, mine, theirs, own, other)


def linear_kernel(lin, head, half, place_ref, query_key_ref, value_ref, running_ref, own_ref, other_ref, gain_ref, out_ref):
    me, side = place_ref[0], place_ref[1]
    rows, width = query_key_ref.shape
    features = LOOKUP_FEATURES
    values = width // 2
    lower = lax.broadcasted_iota(jnp.int32, (SPAN, SPAN), 0) >= lax.broadcasted_iota(
        jnp.int32, (SPAN, SPAN), 1
    )
    states = [state_ref[side * lin + head].T for state_ref in (own_ref, other_ref)]
    for span in range(rows // SPAN):
        per = half // SPAN
        device, inside = span // (2 * per), span % (2 * per)
        apart = jnp.where(me == inside // per, 0, rows // 2)
        at = pl.ds(pl.multiple_of(apart + device * half + (inside % per) * SPAN, SPAN), SPAN)
        for owner in range(2):
            base = owner * values
            running = running_ref[at, owner * features : (owner + 1) * features]
            query = query_key_ref[at, base : base + features].astype(jnp.float32)
            key = query_key_ref[at, base + features : base + 2 * features].astype(jnp.float32)
            value = value_ref[at, base : base + values]
            end = running[SPAN - 1 : SPAN]
            scaled = (query * features ** (-0.5) * jnp.exp(running)).astype(jnp.bfloat16)
            inverse = (key * jnp.exp(-running)).astype(jnp.bfloat16)
            ending = (key * jnp.exp(end - running)).astype(jnp.bfloat16)
            inner = lax.dot_general(scaled, inverse, BY_COLUMNS, preferred_element_type=jnp.float32)
            inner = jnp.where(lower, inner, 0.0).astype(jnp.bfloat16)
            state = states[owner]
            raw = jnp.dot(inner, value, preferred_element_type=jnp.float32) + lax.dot_general(
                scaled, state.astype(jnp.bfloat16), BY_COLUMNS, preferred_element_type=jnp.float32
            )
            states[owner] = state * jnp.exp(end) + lax.dot_general(
                value, ending, BY_ROWS, preferred_element_type=jnp.float32
            )
            scale = lax.rsqrt(jnp.mean(raw * raw, axis=-1, keepdims=True) + EPS)
            out_ref[at, base : base + values] = (raw * scale * gain_ref[...]).astype(out_ref.dtype)


def linear_heads(place, lin, head, half, query_key, value, running, own, other, gain):
    return _call(
        functools.partial(linear_kernel, lin, head, half),
        jax.ShapeDtypeStruct(query_key.shape, jnp.bfloat16),
        2 * 10**9,
        2**21,
        in_specs=[SMEM] + [VMEM] * 6,
        out_specs=VMEM,
    )(place, query_key, value, running, own, other, gain)


def window_kernel(group, half, place_ref, slope_ref, sink_ref, key_value_ref, query_ref, out_ref):
    me = place_ref[0]
    rows = query_ref.shape[0]
    owners, groups = slope_ref.shape
    pair = key_value_ref.shape[1] // (2 * owners)
    from_query = lax.broadcasted_iota(jnp.int32, (WINDOW, WINDOW), 0)
    from_key = lax.broadcasted_iota(jnp.int32, (WINDOW, WINDOW), 1)
    present = from_key <= from_query
    distance = jnp.where(present, from_query - from_key, from_query - from_key + WINDOW).astype(jnp.float32)
    unit = min(half, WINDOW)

    def places(block):
        out = []
        for piece in range(WINDOW // unit):
            start = block * WINDOW + piece * unit
            device, inside = start // (2 * half), start % (2 * half)
            apart = jnp.where(me == inside // half, 0, rows // 2)
            out.append(pl.ds(pl.multiple_of(apart + device * half + inside % half, unit), unit))
        return out

    for owner in range(owners):
        key_at = owner * 2 * pair + group * HD
        value_at = key_at + pair
        base = owner * groups * HD
        biases = [slope_ref[owner, head] * distance for head in range(groups)]
        past_keys, past_values = None, None
        for block in range(rows // WINDOW):
            first = block == 0
            at = places(block)
            keys = jnp.concatenate([key_value_ref[a, key_at : key_at + HD] for a in at], axis=0)
            values = jnp.concatenate([key_value_ref[a, value_at : value_at + HD] for a in at], axis=0)
            band_keys = keys if first else jnp.concatenate([past_keys, keys], axis=0)
            band_values = values if first else jnp.concatenate([past_values, values], axis=0)
            past_keys, past_values = keys, values
            queries = jnp.concatenate(
                [query_ref[a, base + head * HD : base + (head + 1) * HD] for head in range(groups) for a in at],
                axis=0,
            )
            scores = lax.dot_general(queries, band_keys, BY_COLUMNS, preferred_element_type=jnp.float32)
            probs = []
            for head in range(groups):
                mine = scores[head * WINDOW : (head + 1) * WINDOW]
                if first:
                    weight = jnp.where(present, jnp.exp(mine * HD ** (-0.5) - biases[head]), 0.0)
                else:
                    score = jnp.where(present, mine[:, WINDOW:], mine[:, :WINDOW])
                    weight = jnp.exp(score * HD ** (-0.5) - biases[head])
                total = jnp.sum(weight, axis=-1, keepdims=True) + sink_ref[owner, head]
                share = weight / total
                if first:
                    probs.append(share.astype(jnp.bfloat16))
                else:
                    probs.append(
                        jnp.concatenate(
                            [
                                jnp.where(present, 0.0, share).astype(jnp.bfloat16),
                                jnp.where(present, share, 0.0).astype(jnp.bfloat16),
                            ],
                            axis=1,
                        )
                    )
            outs = jnp.dot(jnp.concatenate(probs, axis=0), band_values, preferred_element_type=jnp.float32)
            joined = jnp.concatenate(
                [outs[head * WINDOW : (head + 1) * WINDOW] for head in range(groups)], axis=1
            ).astype(out_ref.dtype)
            for piece, a in enumerate(at):
                out_ref[a, base : base + groups * HD] = joined[piece * unit : (piece + 1) * unit]


def window_heads(place, group, half, slopes, sinks, key_value, query):
    return _call(
        functools.partial(window_kernel, group, half),
        jax.ShapeDtypeStruct(query.shape, jnp.bfloat16),
        2 * 10**9,
        2**21,
        in_specs=[SMEM, SMEM, SMEM, VMEM, VMEM],
        out_specs=VMEM,
    )(place, slopes, sinks, key_value, query)


def output_kernel(sources, place_ref, *refs):
    count = 1 + max(max(row) for row in sources)
    pieces = len(sources)
    passed = refs[:count]
    own_ref, other_ref = refs[count : count + 2]
    held, arrival = refs[-2:]
    rest = refs[count + 2 : -2]
    split = rest[-1].shape[0] != held.shape[1]
    outs = rest[-2:] if split else rest[-1:]
    before = rest[: len(rest) - len(outs)]
    depth = place_ref[2]
    for at in range(len(sources[0])):

        @pl.when(depth == at)
        def _():
            for piece in range(pieces):
                pltpu.make_async_copy(passed[sources[piece][at]], held.at[piece], arrival.at[piece]).start()

    for piece in range(pieces):
        pltpu.make_async_copy(passed[0], held.at[piece], arrival.at[piece]).wait()
    width = held.shape[2] // 2
    rows = outs[0].shape[0]
    columns = outs[0].shape[1]
    block = columns // 2
    for top, out_ref in enumerate(outs):
        at = slice(top * rows, (top + 1) * rows)
        for part in range(2):
            span = slice(part * block, (part + 1) * block)
            total = before[0][at, span] if before else jnp.zeros((rows, block), jnp.float32)
            for piece in range(pieces):
                lines = slice(piece * width, (piece + 1) * width)
                total = total + jnp.dot(
                    held[piece, at, :width], own_ref[lines, span], preferred_element_type=jnp.float32
                )
                total = total + jnp.dot(
                    held[piece, at, width:], other_ref[lines, span], preferred_element_type=jnp.float32
                )
            out_ref[:, span] = total.astype(out_ref.dtype)


def output_sum(place, passed, sources, own, other, before, split):
    rows, width = passed[0].shape
    pieces = len(sources)
    lines, columns = other.shape
    kind, parts = (jnp.bfloat16, 2) if split else (jnp.float32, 1)
    whole = pl.BlockSpec((rows, columns), lambda i, place: (0, 0))
    out = pl.BlockSpec((rows // parts, columns), lambda i, place: (0, 0))
    return _call(
        functools.partial(output_kernel, sources),
        [jax.ShapeDtypeStruct((rows // parts, columns), kind)] * parts,
        4 * rows * columns * lines,
        8 * rows * columns,
        grid_spec=_prefetch(
            1,
            (1,),
            [ANY] * len(passed)
            + [
                pl.BlockSpec((lines, columns), lambda i, place: (place[1], 0)),
                pl.BlockSpec((lines, columns), lambda i, place: (0, 0)),
            ]
            + ([] if before is None else [whole]),
            [out] * parts,
            [pltpu.VMEM((pieces, rows, width), jnp.bfloat16), pltpu.SemaphoreType.DMA((pieces,))],
        ),
    )(place, *passed, own, other, *([] if before is None else [before]))


def resident(
    activations,
    input_norm_gain,
    window_query_weight,
    window_key_weight,
    window_value_weight,
    linear_query_weight,
    linear_key_weight,
    linear_value_weight,
    decay_down_factor,
    decay_up_factor,
    decay_offset_bias,
    extra_fading_exponent,
    starting_state,
    head_sink_logit,
    linear_head_gain,
    window_output_weight,
    linear_output_weight,
):
    peers = lax.axis_size("sp")
    hops = peers - 1
    line, me = lax.axis_index("sp"), lax.axis_index("tp")
    depth = jnp.where(me == 0, line, hops - line)
    far, near = 1 - me, me
    place = jnp.stack([me, far, hops - depth, line]).astype(jnp.int32)
    rows, half_model = activations.shape
    half = rows // 2
    bf16, f32 = jnp.bfloat16, jnp.float32
    lin = extra_fading_exponent.shape[1] // 2
    key_heads = window_key_weight.shape[1] // HD // 2
    query_heads = window_query_weight.shape[1] // HD // 2
    groups = query_heads // key_heads
    rank = decay_down_factor.shape[1]

    def swap(value):
        return lax.ppermute(value, "tp", SWAP)


    message = _call(
        message_kernel,
        jax.ShapeDtypeStruct((half, half_model + LOOKUP_FEATURES), bf16),
        10**11,
        2**20,
        in_specs=[SMEM, VMEM, VMEM],
        out_specs=VMEM,
    )(place, activations, extra_fading_exponent)
    mate = swap(message)
    wide = 2 * half_model // peers + LOOKUP_FEATURES
    outgoing = _call(
        norm_kernel,
        [jax.ShapeDtypeStruct((half, wide), bf16)] * peers,
        10**11,
        2**21,
        in_specs=[SMEM] + [VMEM] * 5,
        out_specs=[VMEM] * peers,
    )(place, activations, extra_fading_exponent, mate, input_norm_gain.reshape(1, -1), decay_down_factor.T)

    (
        outgoing,
        matrices,
        window_output_weight,
        linear_output_weight,
        starting_state,
        decay_up_factor,
        decay_offset_bias,
        head_sink_logit,
    ) = lax.optimization_barrier(
        (
            outgoing,
            (
                window_query_weight,
                window_key_weight,
                window_value_weight,
                linear_query_weight,
                linear_key_weight,
                linear_value_weight,
            ),
            window_output_weight,
            linear_output_weight,
            starting_state,
            decay_up_factor,
            decay_offset_bias,
            head_sink_logit,
        )
    )
    incoming = to_offsets(outgoing)
    packed = pack_items(near.reshape(1), lin, key_heads, matrices)
    other_in = swap(packed)
    own_in = pack_items(far.reshape(1), lin, key_heads, matrices)
    features = decay_up_factor.shape[1]
    own_small = jnp.concatenate(
        [
            decay_up_factor.astype(f32),
            decay_offset_bias.reshape(1, features),
            jnp.pad(head_sink_logit, (0, features - head_sink_logit.shape[0])).reshape(1, features),
            jnp.zeros((6, features), f32),
        ],
        axis=0,
    )
    other_small = swap(own_small)
    other_state = swap(starting_state)
    lines = linear_output_weight.shape[0] // 2
    other_linear = lax.dynamic_slice_in_dim(linear_output_weight, near * lines, lines, axis=0)
    other_linear = swap(other_linear)
    lines = window_output_weight.shape[0] // 2
    other_window = lax.dynamic_slice_in_dim(window_output_weight, near * lines, lines, axis=0)
    other_window = swap(other_window)

    incoming = collect(place, incoming)
    mine = incoming.reshape(peers * half, wide)
    theirs = swap(incoming).reshape(peers * half, wide)

    count = 1 + key_heads + 2 * lin
    arrived, finals = {}, []
    for step in range(count + 2 * hops):
        index = jnp.clip(step - 2 * depth, 0, count - 1).astype(jnp.int32).reshape(1)
        value = partial_sum(index, mine, theirs, own_in, other_in, arrived.get(step - 2))
        depths = [d for d in range(hops) if 0 <= step - 2 * d < count]
        if depths:
            arrived[step] = lax.ppermute(value, ("sp", "tp"), _pairs(peers, depths, 0))
        if step >= 2 * hops:
            finals.append(value)

    running = decay_sums(place, lin, rank, mine, theirs, own_small, other_small)
    sinks = jnp.stack(
        [
            lax.dynamic_slice_in_dim(small[rank + 1], far * query_heads, query_heads).reshape(key_heads, groups)
            for small in (own_small, other_small)
        ]
    )
    sinks = jnp.exp(sinks)
    attended = []
    for group in range(key_heads):
        number = jnp.stack([me, 1 - me])[:, None] * (2 * query_heads) + (
            far * query_heads + group * groups + jnp.arange(groups, dtype=jnp.int32)
        )
        slopes = jnp.exp2(-8.0 * (number + 1).astype(f32) / QH)
        attended.append(
            window_heads(place, group, half, slopes, sinks[:, group], finals[0], finals[1 + group])
        )
    for head in range(lin):
        attended.append(
            linear_heads(
                place,
                lin,
                head,
                half,
                finals[1 + key_heads + 2 * head],
                finals[2 + key_heads + 2 * head],
                running[head],
                starting_state,
                other_state,
                linear_head_gain.reshape(1, DV),
            )
        )

    pieces = len(attended)
    held = []
    for piece in range(pieces):
        seen = [attended[piece]]
        for hop in range(hops):
            if piece == pieces - 1 and 0 < hop == hops - 1:
                seen.append(lax.ppermute(seen[0], ("sp", "tp"), [(hops * 2, 0), (1, hops * 2 + 1)]))
            else:
                seen.append(lax.ppermute(seen[-1], ("sp", "tp"), _pairs(peers, [hop], 1)))
        held.append(seen)
    table = lambda count: tuple(tuple(range(k * peers, (k + 1) * peers)) for k in range(count))
    flat = lambda lists: [value for seen in lists for value in seen]
    (terms,) = output_sum(
        place, flat(held[:key_heads]), table(key_heads), window_output_weight, other_window, None, False
    )
    kept, given = output_sum(
        place, flat(held[key_heads:]), table(lin), linear_output_weight, other_linear, terms, True
    )

    return spread(place, to_offsets(join(place, kept, swap(given), peers)))


def fits(mesh):
    return mesh.shape["tp"] == 2 and mesh.shape["sp"] > 1


def solution(mesh):
    placed = (
        P(("fs", "sp"), "tp"),
        P(),
        P("sp", "tp"),
        P("sp", "tp"),
        P("sp", "tp"),
        P("sp", "tp"),
        P("sp", "tp"),
        P("sp", "tp"),
        P(),
        P(None, "tp"),
        P("tp"),
        P(("fs", "sp"), "tp"),
        P("tp", None, None),
        P("tp"),
        P(),
        P("tp", "sp"),
        P("tp", "sp"),
    )
    if not fits(mesh):
        return jax.shard_map(
            local, mesh=mesh, in_specs=placed, out_specs=P(("fs", "sp", "tp"), None), check_vma=False
        )

    return jax.shard_map(resident, mesh=mesh, in_specs=placed, out_specs=P(("fs", "sp", "tp"), None), check_vma=False)
```

```python
import functools

import jax
import jax.numpy as jnp
from jax import lax
from jax.experimental import pallas as pl
from jax.experimental.pallas import tpu as pltpu
from jax.sharding import PartitionSpec as P


QH = 32
HD = 64
WINDOW = 128
LOOKUP_FEATURES = 128
DV = 256
SPAN = 64


EPS = 1e-05
FADING_SOFTNESS = 16.0
HIGH_PRECISION = lax.Precision.HIGHEST


def passed_along(value, axis, steps):
    count = lax.axis_size(axis)
    leading, last = (max(0, -steps), min(count, count - steps))
    return lax.ppermute(value, axis, [(source, source + steps) for source in range(leading, last)])


def prefix(x, axis, combine, identity):
    peers, place = (lax.axis_size(axis), lax.axis_index(axis))
    everything = jax.tree.map(
        lambda part, kind: lax.all_gather(part.astype(kind), axis), x, (jnp.bfloat16, jnp.bfloat16)
    )
    start = jax.tree.map(
        lambda part, zero: jnp.broadcast_to(jnp.asarray(zero, part.dtype), part.shape), x, identity
    )

    def hop(k, before):
        reached = k < place
        new = combine(
            before, jax.tree.map(lambda part, own: part[k].astype(own.dtype), everything, x)
        )
        return jax.tree.map(lambda a, b: jnp.where(reached, a, b), new, before)

    return lax.fori_loop(0, peers, hop, start)


def window_attention(near_query, near_keys, near_values, head_sink_logit):
    stream_extent = near_query.shape[0]
    key_heads = near_keys.shape[1] // HD
    heads_here = near_query.shape[1] // HD
    groups = heads_here // key_heads
    blocks = stream_extent // WINDOW
    tail_rows = jnp.stack([near_keys, near_values])
    before = passed_along(tail_rows, "sp", 1)

    def banded(previous, current):
        extended = jnp.concatenate([previous, current], axis=0)
        earlier = extended[:stream_extent].reshape(blocks, WINDOW, key_heads, HD)
        present = extended[WINDOW:].reshape(blocks, WINDOW, key_heads, HD)
        return jnp.concatenate([earlier, present], axis=1)

    key_band = banded(before[0], near_keys)
    value_band = banded(before[1], near_values)
    queries = near_query.reshape(blocks, WINDOW, key_heads, groups, HD)
    scores = jnp.einsum(
        "nqhgd,nkhd->hgnqk", queries, key_band, preferred_element_type=jnp.float32
    ) * HD ** (-0.5)
    head_ids = lax.axis_index("tp") * heads_here + jnp.arange(heads_here, dtype=jnp.int32)
    slopes = jnp.exp2(-8.0 * (head_ids + 1).astype(jnp.float32) / QH).reshape(key_heads, groups)
    query_pos = jnp.arange(WINDOW, dtype=jnp.int32)
    key_pos = jnp.arange(2 * WINDOW, dtype=jnp.int32)
    distance = query_pos[:, None] - key_pos[None, :] + WINDOW
    start_pos = (
        lax.axis_index("sp") * stream_extent + (jnp.arange(blocks, dtype=jnp.int32) - 1) * WINDOW
    )
    absolute = start_pos[:, None] + key_pos[None, :]
    allowed = ((distance >= 0) & (distance < WINDOW))[None] & (absolute >= 0)[:, None, :]
    biased = scores - slopes[:, :, None, None, None] * distance.astype(jnp.float32)
    weights = jnp.where(allowed, jnp.exp(biased), 0.0)
    denominator = (
        jnp.sum(weights, axis=-1, keepdims=True)
        + jnp.exp(head_sink_logit.reshape(key_heads, groups))[:, :, None, None, None]
    )
    attention = (weights / denominator).astype(jnp.bfloat16)
    attended = jnp.einsum(
        "hgnqk,nkhd->nqhgd", attention, value_band, preferred_element_type=jnp.float32
    )
    return attended.reshape(stream_extent, heads_here * HD).astype(jnp.bfloat16)


def linear_attention(
    gated_query, gated_keys, gated_values, fading_exponent, linear_head_gain, starting_state
):
    stream_extent = gated_query.shape[0]
    head_total = gated_query.shape[1] // LOOKUP_FEATURES
    span_count = stream_extent // SPAN
    scaled_query = gated_query.astype(jnp.float32).reshape(
        span_count, SPAN, head_total, LOOKUP_FEATURES
    ) * LOOKUP_FEATURES ** (-0.5)
    keys_wide = gated_keys.astype(jnp.float32).reshape(
        span_count, SPAN, head_total, LOOKUP_FEATURES
    )
    values_wide = gated_values.astype(jnp.float32).reshape(span_count, SPAN, head_total, DV)
    running = jnp.cumsum(
        fading_exponent.reshape(span_count, SPAN, head_total, LOOKUP_FEATURES), axis=1
    )
    span_end = running[:, -1]
    query_with_decay = scaled_query * jnp.exp(running)
    inverse_keys = keys_wide * jnp.exp(-running)
    ending_keys = keys_wide * jnp.exp(span_end[:, None] - running)
    inner = jnp.einsum("nchk,nshk->nhcs", query_with_decay, inverse_keys, precision=HIGH_PRECISION)
    lower = jnp.tril(jnp.ones((SPAN, SPAN), dtype=bool))
    inner = jnp.where(lower, inner, 0.0)
    within = jnp.einsum("nhcs,nshv->nchv", inner, values_wide, precision=HIGH_PRECISION)

    def advance(running_state, inputs):
        query_portion, key_portion, value_portion, scale_factor = inputs
        layer_output = jnp.einsum(
            "fmy,mys->fms", query_portion, running_state, precision=HIGH_PRECISION
        )
        running_state = running_state * scale_factor[..., None] + jnp.einsum(
            "gxp,gxz->xpz", key_portion, value_portion, precision=HIGH_PRECISION
        )
        return (running_state, layer_output)

    start_state = jnp.zeros((head_total, LOOKUP_FEATURES, DV), jnp.float32)
    state_end, carried = lax.scan(
        advance, start_state, (query_with_decay, ending_keys, values_wide, jnp.exp(span_end))
    )
    device_decay = jnp.exp(jnp.sum(span_end, axis=0))
    prefix_sums = jnp.cumsum(span_end, axis=0) - span_end

    def combine(earlier, later):
        return (earlier[0] * later[0], later[0][..., None] * earlier[1] + later[1])

    decay_before, state_before = prefix(
        (device_decay, state_end),
        "sp",
        combine,
        (jnp.ones_like(device_decay), jnp.zeros_like(state_end)),
    )
    incoming_rows = state_before + decay_before[..., None] * starting_state
    crossing = jnp.einsum(
        "qwso,soz->qwsz",
        query_with_decay * jnp.exp(prefix_sums)[:, None],
        incoming_rows,
        precision=HIGH_PRECISION,
    )
    flat = (within + carried + crossing).reshape(stream_extent, head_total, DV)
    normal = (
        flat * lax.rsqrt(jnp.mean(flat * flat, axis=-1, keepdims=True) + EPS) * linear_head_gain
    )
    return normal.reshape(stream_extent, head_total * DV).astype(jnp.bfloat16)


def local(
    activations,
    input_norm_gain,
    window_query_weight,
    window_key_weight,
    window_value_weight,
    linear_query_weight,
    linear_key_weight,
    linear_value_weight,
    decay_down_factor,
    decay_up_factor,
    decay_offset_bias,
    extra_fading_exponent,
    starting_state,
    head_sink_logit,
    linear_head_gain,
    window_output_weight,
    linear_output_weight,
):
    gathered = lax.all_gather(activations, "tp", axis=1, tiled=True)
    widened = gathered.astype(jnp.float32)
    normed = (
        widened
        * lax.rsqrt(jnp.mean(widened * widened, axis=1, keepdims=True) + EPS)
        * input_norm_gain
    ).astype(jnp.bfloat16)
    row_total = normed.shape[0]
    matrices = (
        window_query_weight,
        window_key_weight,
        window_value_weight,
        linear_query_weight,
        linear_key_weight,
        linear_value_weight,
    )
    segments = (
        lax.all_gather(matrices[0], "sp", axis=0, tiled=True),
        lax.all_gather(matrices[1], "sp", axis=0, tiled=True),
        lax.all_gather(matrices[2], "sp", axis=0, tiled=True),
        lax.all_gather(matrices[3], "sp", axis=0, tiled=True),
        lax.all_gather(matrices[4], "sp", axis=0, tiled=True),
        lax.all_gather(matrices[5], "sp", axis=0, tiled=True),
    )
    projected = tuple(
        (jnp.dot(normed, segment, preferred_element_type=jnp.float32) for segment in segments)
    )
    near_query, near_keys, near_values, gated_query, gated_keys, gated_values = [
        product.astype(jnp.bfloat16) for product in projected
    ]
    low_rank = jnp.dot(normed, decay_down_factor, preferred_element_type=jnp.float32).astype(
        jnp.bfloat16
    )
    attention_energies = (
        jnp.dot(low_rank, decay_up_factor, preferred_element_type=jnp.float32) + decay_offset_bias
    )
    head_total = extra_fading_exponent.shape[1]
    fading_exponent = (jax.nn.log_sigmoid(attention_energies) / FADING_SOFTNESS).reshape(
        row_total, head_total, LOOKUP_FEATURES
    ) + extra_fading_exponent[:, :, None]
    near_out = window_attention(near_query, near_keys, near_values, head_sink_logit)
    gated_out = linear_attention(
        gated_query, gated_keys, gated_values, fading_exponent, linear_head_gain, starting_state
    )
    window_full, linear_full = (
        lax.all_gather(window_output_weight, "sp", axis=1, tiled=True),
        lax.all_gather(linear_output_weight, "sp", axis=1, tiled=True),
    )
    return lax.psum_scatter(
        (
            jnp.dot(near_out, window_full, preferred_element_type=jnp.float32)
            + jnp.dot(gated_out, linear_full, preferred_element_type=jnp.float32)
        ).astype(jnp.bfloat16),
        "tp",
        scatter_dimension=0,
        tiled=True,
    )


def _pairs(peers, depths, core):
    out = []
    for d in depths:
        out.append((d * 2 + core, (d + 1) * 2 + core))
        out.append(((peers - 1 - d) * 2 + 1 - core, (peers - 2 - d) * 2 + 1 - core))
    return out


SWAP = [(0, 1), (1, 0)]
VMEM = pl.BlockSpec(memory_space=pltpu.VMEM)
SMEM = pl.BlockSpec(memory_space=pltpu.SMEM)
ANY = pl.BlockSpec(memory_space=pl.ANY)
BY_COLUMNS = (((1,), (1,)), ((), ()))
BY_ROWS = (((0,), (0,)), ((), ()))


def _call(kernel, out_shape, flops, moved, grant=24, **kw):
    return pl.pallas_call(
        kernel,
        out_shape=out_shape,
        compiler_params=pltpu.CompilerParams(vmem_limit_bytes=grant * 1024 * 1024),
        cost_estimate=pl.CostEstimate(flops=flops, bytes_accessed=moved, transcendentals=0),
        **kw,
    )


def _prefetch(scalars, grid, in_specs, out_specs, scratch=()):
    return pltpu.PrefetchScalarGridSpec(
        num_scalar_prefetch=scalars, grid=grid, in_specs=in_specs, out_specs=out_specs, scratch_shapes=scratch
    )


def message_kernel(place_ref, x_ref, fade_ref, out_ref):
    rows, wide = out_ref.shape
    half_model = x_ref.shape[1]
    at = pl.ds(pl.multiple_of(place_ref[1] * rows, rows), rows)
    out_ref[:, :half_model] = x_ref[at, :]
    out_ref[:, half_model:] = jnp.concatenate(
        [_parts(_half(fade_ref, place_ref[1])), jnp.zeros((rows, wide - half_model - 3 * fade_ref.shape[0]), jnp.float32)], axis=1
    ).astype(out_ref.dtype)


def _half(turned_ref, which):
    value = turned_ref[...].T
    rows = value.shape[0] // 2
    return jnp.where(which == 0, value[:rows], value[rows:])


def _parts(value):
    high = value.astype(jnp.bfloat16).astype(jnp.float32)
    rest = value - high
    middle = rest.astype(jnp.bfloat16).astype(jnp.float32)
    return jnp.concatenate([high, middle, rest - middle], axis=1)


def norm_kernel(place_ref, x_ref, fade_ref, mate_ref, gain_ref, down_ref, *out_refs):
    me, line = place_ref[0], place_ref[3]
    pieces = len(out_refs)
    rows, wide = out_refs[0].shape
    half_model = x_ref.shape[1]
    cut = 2 * half_model // pieces
    fades = 3 * fade_ref.shape[0]
    own = x_ref[pl.ds(pl.multiple_of(me * rows, rows), rows), :].astype(jnp.float32)
    mate = mate_ref[:, :half_model].astype(jnp.float32)
    square = jnp.sum(own * own, axis=1, keepdims=True) + jnp.sum(mate * mate, axis=1, keepdims=True)
    scale = lax.rsqrt(square / (2 * half_model) + EPS)
    low_rank = None
    for side, value in ((me, own), (1 - me, mate)):
        start = pl.multiple_of(side * half_model, half_model)
        normed = (value * scale * gain_ref[:, pl.ds(start, half_model)]).astype(jnp.bfloat16)
        part = lax.dot_general(
            normed, down_ref[:, pl.ds(start, half_model)], BY_COLUMNS, preferred_element_type=jnp.float32
        )
        low_rank = part if low_rank is None else low_rank + part
        for k in range(pieces // 2):
            away = lax.rem(side * (pieces // 2) + k - line + pieces, pieces)
            for offset, out_ref in enumerate(out_refs):

                @pl.when(away == offset)
                def _():
                    out_ref[:, :cut] = normed[:, k * cut : (k + 1) * cut]

    mine = _parts(_half(fade_ref, me))
    theirs = mate_ref[:, half_model : half_model + fades].astype(jnp.float32)
    tail = jnp.concatenate(
        [
            low_rank.astype(jnp.bfloat16).astype(jnp.float32),
            jnp.where(me == 0, mine, theirs),
            jnp.where(me == 0, theirs, mine),
            jnp.zeros((rows, wide - cut - low_rank.shape[1] - 2 * fades), jnp.float32),
        ],
        axis=1,
    ).astype(jnp.bfloat16)
    for out_ref in out_refs:
        out_ref[:, cut:] = tail


def collect_kernel(place_ref, *refs):
    pieces = len(refs) - 1
    for offset in range(pieces):
        refs[-1][lax.rem(place_ref[3] - offset + pieces, pieces)] = refs[offset][...]


def collect(place, parts):
    rows, wide = parts[0].shape
    return _call(
        collect_kernel,
        jax.ShapeDtypeStruct((len(parts), rows, wide), parts[0].dtype),
        10**8,
        2**21,
        in_specs=[SMEM] + [VMEM] * len(parts),
        out_specs=VMEM,
    )(place, *parts)


def join_kernel(place_ref, kept_ref, given_ref, *out_refs):
    pieces = len(out_refs)
    rows = out_refs[0].shape[0]
    for offset, out_ref in enumerate(out_refs):
        at = pl.ds(pl.multiple_of(lax.rem(place_ref[3] + offset, pieces) * rows, rows), rows)
        out_ref[...] = (kept_ref[at].astype(jnp.float32) + given_ref[at].astype(jnp.float32)).astype(out_ref.dtype)


def join(place, kept, given, pieces):
    rows, columns = kept.shape
    return _call(
        join_kernel,
        [jax.ShapeDtypeStruct((rows // pieces, columns), kept.dtype)] * pieces,
        10**8,
        2**21,
        in_specs=[SMEM, VMEM, VMEM],
        out_specs=[VMEM] * pieces,
    )(place, kept, given)


def spread_kernel(place_ref, *refs):
    pieces = len(refs) - 1
    columns = refs[0].shape[1]
    for offset in range(pieces):
        start = lax.rem(place_ref[3] - offset + pieces, pieces) * columns
        refs[-1][:, pl.ds(pl.multiple_of(start, columns), columns)] = refs[offset][...]


def spread(place, parts):
    rows, columns = parts[0].shape
    return _call(
        spread_kernel,
        jax.ShapeDtypeStruct((rows, len(parts) * columns), parts[0].dtype),
        10**8,
        2**21,
        in_specs=[SMEM] + [VMEM] * len(parts),
        out_specs=VMEM,
    )(place, *parts)


def to_offsets(parts):
    peers = len(parts)
    out = [parts[0]]
    for k in range(1, peers):
        out.append(lax.ppermute(parts[k], "sp", [(i, (i + k) % peers) for i in range(peers)]))
    return out


def pack_kernel(key_heads, side_ref, wq, wk, wv, lq, lk, lv, out_ref):
    step = pl.program_id(0)
    half = out_ref.shape[2] // 2
    keys_and_values = step == 0
    queries = (step > 0) & (step <= key_heads)
    head_items = (step > key_heads) & ((step - key_heads) % 2 == 1)
    head_values = (step > key_heads) & ((step - key_heads) % 2 == 0)

    @pl.when(keys_and_values)
    def _():
        out_ref[0, :, :half] = wk[...]
        out_ref[0, :, half:] = wv[...]

    @pl.when(queries)
    def _():
        out_ref[0] = wq[...]

    @pl.when(head_items)
    def _():
        out_ref[0, :, :half] = lq[...]
        out_ref[0, :, half:] = lk[...]

    @pl.when(head_values)
    def _():
        out_ref[0] = lv[...]


def pack_items(side, lin, key_heads, matrices):
    depth = matrices[0].shape[0]
    width = 2 * LOOKUP_FEATURES
    count = 1 + key_heads + 2 * lin
    fixed = pl.BlockSpec((depth, width // 2), lambda i, side: (0, side[0]))
    query = pl.BlockSpec(
        (depth, width), lambda i, side: (0, side[0] * key_heads + jnp.clip(i - 1, 0, key_heads - 1))
    )
    head = lambda i, side: (0, side[0] * lin + jnp.clip((i - 1 - key_heads) // 2, 0, lin - 1))
    narrow, full = pl.BlockSpec((depth, width // 2), head), pl.BlockSpec((depth, width), head)
    return _call(
        functools.partial(pack_kernel, key_heads),
        jax.ShapeDtypeStruct((count, depth, width), jnp.bfloat16),
        10**11,
        4 * count * depth * width,
        grid_spec=_prefetch(
            1,
            (count,),
            [query, fixed, fixed, narrow, narrow, full],
            pl.BlockSpec((1, depth, width), lambda i, side: (i, 0, 0)),
        ),
    )(side, *matrices)


def partial_kernel(index_ref, mine_ref, theirs_ref, own_ref, other_ref, *rest):
    out_ref, weight, arrival = rest[-3:]
    rows = mine_ref.shape[0]
    depth, width = weight.shape
    copy = pltpu.make_async_copy(other_ref.at[index_ref[0]], weight, arrival)
    copy.start()
    for half in range(2):
        if half == 1:
            copy.wait()
        for top, x_ref in enumerate((mine_ref, theirs_ref)):
            at = slice(top * rows, (top + 1) * rows)
            span = slice(half * width, (half + 1) * width)
            matrix = own_ref[index_ref[0]] if half == 0 else weight[...]
            total = jnp.dot(x_ref[:, :depth], matrix, preferred_element_type=jnp.float32)
            if len(rest) == 4:
                total = total + rest[0][at, span].astype(jnp.float32)
            out_ref[at, span] = total.astype(out_ref.dtype)


def partial_sum(index, mine, theirs, own, other, arrived):
    rows = mine.shape[0]
    _, depth, width = own.shape
    operands = [mine, theirs, own, other] + ([] if arrived is None else [arrived])
    return _call(
        partial_kernel,
        jax.ShapeDtypeStruct((2 * rows, 2 * width), jnp.bfloat16),
        160 * rows * depth * width,
        4 * depth * (rows + width),
        in_specs=[SMEM, VMEM, VMEM, VMEM, ANY] + [VMEM] * (len(operands) - 4),
        out_specs=VMEM,
        scratch_shapes=[pltpu.VMEM((depth, width), jnp.bfloat16), pltpu.SemaphoreType.DMA],
    )(index, *operands)


def decay_kernel(lin, rank, place_ref, mine_ref, theirs_ref, own_ref, other_ref, *out_refs):
    me, side = place_ref[0], place_ref[1]
    rows = mine_ref.shape[0]
    features = LOOKUP_FEATURES
    lower = (
        lax.broadcasted_iota(jnp.int32, (SPAN, SPAN), 0) >= lax.broadcasted_iota(jnp.int32, (SPAN, SPAN), 1)
    ).astype(jnp.bfloat16)
    for top, tail_ref in enumerate((mine_ref, theirs_ref)):
        tail = tail_ref[:, tail_ref.shape[1] - features :]
        low_rank = tail[:, :rank]
        parts = [
            tail[:, rank + k * 2 * lin : rank + (k + 1) * 2 * lin].astype(jnp.float32) for k in range(6)
        ]
        by_core = [parts[0] + parts[1] + parts[2], parts[3] + parts[4] + parts[5]]
        fades = [jnp.where(me == 0, by_core[0], by_core[1]), jnp.where(me == 0, by_core[1], by_core[0])]
        for head in range(lin):
            for owner, small_ref in enumerate((own_ref, other_ref)):
                at = pl.ds(pl.multiple_of((side * lin + head) * features, features), features)
                up = small_ref[:rank, at].astype(jnp.bfloat16)
                energy = jnp.dot(low_rank, up, preferred_element_type=jnp.float32) + small_ref[rank : rank + 1, at]
                soft = jnp.minimum(energy, 0.0) - jnp.log1p(jnp.exp(-jnp.abs(energy)))
                both = fades[owner]
                fade = jnp.where(side == 0, both[:, head : head + 1], both[:, lin + head : lin + head + 1])
                step = soft * (1.0 / FADING_SOFTNESS) + fade
                high = step.astype(jnp.bfloat16)
                rest = step - high.astype(jnp.float32)
                middle = rest.astype(jnp.bfloat16)
                low = (rest - middle.astype(jnp.float32)).astype(jnp.bfloat16)
                column = owner * features
                out_ref = out_refs[head]
                for span in range(rows // SPAN):
                    cut = slice(span * SPAN, (span + 1) * SPAN)
                    out_ref[top * rows + span * SPAN : top * rows + (span + 1) * SPAN, column : column + features] = (
                        jnp.dot(lower, high[cut], preferred_element_type=jnp.float32)
                        + jnp.dot(lower, middle[cut], preferred_element_type=jnp.float32)
                        + jnp.dot(lower, low[cut], preferred_element_type=jnp.float32)
                    )


def decay_sums(place, lin, rank, mine, theirs, own, other):
    return _call(
        functools.partial(decay_kernel, lin, rank),
        [jax.ShapeDtypeStruct((2 * mine.shape[0], 2 * LOOKUP_FEATURES), jnp.float32)] * lin,
        10**9,
        2**20,
        in_specs=[SMEM] + [VMEM] * 4,
        out_specs=[VMEM] * lin,
    )(place, mine, theirs, own, other)


def linear_kernel(lin, head, half, place_ref, query_key_ref, value_ref, running_ref, own_ref, other_ref, gain_ref, *rest):
    me, side = place_ref[0], place_ref[1]
    out_ref = rest[-1]
    rows, width = query_key_ref.shape
    features = LOOKUP_FEATURES
    values = width // 2
    lower = lax.broadcasted_iota(jnp.int32, (SPAN, SPAN), 0) >= lax.broadcasted_iota(
        jnp.int32, (SPAN, SPAN), 1
    )
    states = [state_ref[side * lin + head].T for state_ref in (own_ref, other_ref)]
    for span in range(rows // SPAN):
        per = half // SPAN
        device, inside = span // (2 * per), span % (2 * per)
        apart = jnp.where(me == inside // per, 0, rows // 2)
        at = pl.ds(pl.multiple_of(apart + device * half + (inside % per) * SPAN, SPAN), SPAN)
        for owner in range(2):
            base = owner * values
            running = running_ref[at, owner * features : (owner + 1) * features]
            query = query_key_ref[at, base : base + features].astype(jnp.float32)
            key = query_key_ref[at, base + features : base + 2 * features].astype(jnp.float32)
            value = value_ref[at, base : base + values]
            if len(rest) == 2:
                more = rest[0][at, base : base + values].astype(jnp.float32)
                value = (value.astype(jnp.float32) + more).astype(jnp.bfloat16)
            end = running[SPAN - 1 : SPAN]
            scaled = (query * features ** (-0.5) * jnp.exp(running)).astype(jnp.bfloat16)
            inverse = (key * jnp.exp(-running)).astype(jnp.bfloat16)
            ending = (key * jnp.exp(end - running)).astype(jnp.bfloat16)
            inner = lax.dot_general(scaled, inverse, BY_COLUMNS, preferred_element_type=jnp.float32)
            inner = jnp.where(lower, inner, 0.0).astype(jnp.bfloat16)
            state = states[owner]
            raw = jnp.dot(inner, value, preferred_element_type=jnp.float32) + lax.dot_general(
                scaled, state.astype(jnp.bfloat16), BY_COLUMNS, preferred_element_type=jnp.float32
            )
            states[owner] = state * jnp.exp(end) + lax.dot_general(
                value, ending, BY_ROWS, preferred_element_type=jnp.float32
            )
            scale = lax.rsqrt(jnp.mean(raw * raw, axis=-1, keepdims=True) + EPS)
            out_ref[at, base : base + values] = (raw * scale * gain_ref[...]).astype(out_ref.dtype)


def linear_heads(place, lin, head, half, query_key, value, running, own, other, gain, *more):
    return _call(
        functools.partial(linear_kernel, lin, head, half),
        jax.ShapeDtypeStruct(query_key.shape, jnp.bfloat16),
        2 * 10**9,
        2**21,
        in_specs=[SMEM] + [VMEM] * (6 + len(more)),
        out_specs=VMEM,
    )(place, query_key, value, running, own, other, gain, *more)


def window_kernel(group, half, place_ref, slope_ref, sink_ref, key_value_ref, query_ref, out_ref):
    me = place_ref[0]
    rows = query_ref.shape[0]
    owners, groups = slope_ref.shape
    pair = key_value_ref.shape[1] // (2 * owners)
    from_query = lax.broadcasted_iota(jnp.int32, (WINDOW, WINDOW), 0)
    from_key = lax.broadcasted_iota(jnp.int32, (WINDOW, WINDOW), 1)
    present = from_key <= from_query
    distance = jnp.where(present, from_query - from_key, from_query - from_key + WINDOW).astype(jnp.float32)
    unit = min(half, WINDOW)

    def places(block):
        out = []
        for piece in range(WINDOW // unit):
            start = block * WINDOW + piece * unit
            device, inside = start // (2 * half), start % (2 * half)
            apart = jnp.where(me == inside // half, 0, rows // 2)
            out.append(pl.ds(pl.multiple_of(apart + device * half + inside % half, unit), unit))
        return out

    lanes = lax.broadcasted_iota(jnp.int32, (WINDOW, pair), 1)
    of_group = lanes // HD == group
    first_half = lanes < HD
    keep_present = present.astype(jnp.float32).astype(jnp.bfloat16)
    keep_past = (1.0 - present.astype(jnp.float32)).astype(jnp.bfloat16)
    turned = lambda value: jnp.concatenate([value[:, HD:], value[:, :HD]], axis=1)

    for owner in range(owners):
        key_at = owner * 2 * pair
        base = owner * groups * HD
        biases = [slope_ref[owner, head] * distance for head in range(groups)]
        past_keys, past_values = None, None
        for block in range(rows // WINDOW):
            first = block == 0
            at = places(block)
            load = lambda ref, start: jnp.concatenate([ref[a, start : start + pair] for a in at], axis=0)
            keys, values = load(key_value_ref, key_at), load(key_value_ref, key_at + pair)
            band_keys = keys if first else jnp.concatenate([past_keys, keys], axis=0)
            band_values = values if first else jnp.concatenate([past_values, values], axis=0)
            past_keys, past_values = keys, values
            queries = []
            for couple in range(groups // 2):
                both = load(query_ref, base + couple * pair).astype(jnp.float32) * HD ** (-0.5)
                swapped = turned(both)
                ordered = (both, swapped) if group == 0 else (swapped, both)
                queries += [jnp.where(of_group, value, 0.0).astype(jnp.bfloat16) for value in ordered]
            scores = lax.dot_general(
                jnp.concatenate(queries, axis=0), band_keys, BY_COLUMNS, preferred_element_type=jnp.float32
            )
            probs = []
            for head in range(groups):
                mine = scores[head * WINDOW : (head + 1) * WINDOW]
                if first:
                    weight = jnp.where(present, jnp.exp(mine - biases[head]), 0.0)
                else:
                    weight = jnp.exp(jnp.where(present, mine[:, WINDOW:], mine[:, :WINDOW]) - biases[head])
                total = jnp.sum(weight, axis=-1, keepdims=True) + sink_ref[owner, head]
                share = (weight / total).astype(jnp.bfloat16)
                if first:
                    probs.append(share)
                else:
                    probs.append(jnp.concatenate([share * keep_past, share * keep_present], axis=1))
            outs = jnp.dot(jnp.concatenate(probs, axis=0), band_values, preferred_element_type=jnp.float32)
            for couple in range(groups // 2):
                even = outs[2 * couple * WINDOW : (2 * couple + 1) * WINDOW]
                odd = outs[(2 * couple + 1) * WINDOW : (2 * couple + 2) * WINDOW]
                if group == 0:
                    odd = turned(odd)
                else:
                    even = turned(even)
                joined = jnp.where(first_half, even, odd).astype(out_ref.dtype)
                start = base + couple * pair
                for piece, a in enumerate(at):
                    out_ref[a, start : start + pair] = joined[piece * unit : (piece + 1) * unit]


def window_heads(place, group, half, slopes, sinks, key_value, query):
    return _call(
        functools.partial(window_kernel, group, half),
        jax.ShapeDtypeStruct(query.shape, jnp.bfloat16),
        2 * 10**9,
        2**21,
        in_specs=[SMEM, SMEM, SMEM, VMEM, VMEM],
        out_specs=VMEM,
    )(place, slopes, sinks, key_value, query)


def output_kernel(sources, place_ref, *refs):
    count = 1 + max(max(row) for row in sources)
    pieces = len(sources)
    passed = refs[:count]
    own_ref, other_ref = refs[count : count + 2]
    held, arrival = refs[-2:]
    rest = refs[count + 2 : -2]
    split = rest[-1].shape[0] != held.shape[1]
    outs = rest[-2:] if split else rest[-1:]
    before = rest[: len(rest) - len(outs)]
    depth = place_ref[2]
    for at in range(len(sources[0])):

        @pl.when(depth == at)
        def _():
            for piece in range(pieces):
                pltpu.make_async_copy(passed[sources[piece][at]], held.at[piece], arrival.at[piece]).start()

    for piece in range(pieces):
        pltpu.make_async_copy(passed[0], held.at[piece], arrival.at[piece]).wait()
    width = held.shape[2] // 2
    rows = outs[0].shape[0]
    columns = outs[0].shape[1]
    block = columns // 2
    for top, out_ref in enumerate(outs):
        at = slice(top * rows, (top + 1) * rows)
        for part in range(2):
            span = slice(part * block, (part + 1) * block)
            total = before[0][at, span] if before else jnp.zeros((rows, block), jnp.float32)
            for piece in range(pieces):
                lines = slice(piece * width, (piece + 1) * width)
                total = total + jnp.dot(
                    held[piece, at, :width], own_ref[lines, span], preferred_element_type=jnp.float32
                )
                total = total + jnp.dot(
                    held[piece, at, width:], other_ref[lines, span], preferred_element_type=jnp.float32
                )
            out_ref[:, span] = total.astype(out_ref.dtype)


def output_sum(place, passed, sources, own, other, before, split):
    rows, width = passed[0].shape
    pieces = len(sources)
    lines, columns = other.shape
    kind, parts = (jnp.bfloat16, 2) if split else (jnp.float32, 1)
    whole = pl.BlockSpec((rows, columns), lambda i, place: (0, 0))
    out = pl.BlockSpec((rows // parts, columns), lambda i, place: (0, 0))
    return _call(
        functools.partial(output_kernel, sources),
        [jax.ShapeDtypeStruct((rows // parts, columns), kind)] * parts,
        4 * rows * columns * lines,
        8 * rows * columns,
        grid_spec=_prefetch(
            1,
            (1,),
            [ANY] * len(passed)
            + [
                pl.BlockSpec((lines, columns), lambda i, place: (place[1], 0)),
                pl.BlockSpec((lines, columns), lambda i, place: (0, 0)),
            ]
            + ([] if before is None else [whole]),
            [out] * parts,
            [pltpu.VMEM((pieces, rows, width), jnp.bfloat16), pltpu.SemaphoreType.DMA((pieces,))],
        ),
    )(place, *passed, own, other, *([] if before is None else [before]))


def resident(
    activations,
    input_norm_gain,
    window_query_weight,
    window_key_weight,
    window_value_weight,
    linear_query_weight,
    linear_key_weight,
    linear_value_weight,
    decay_down_factor,
    decay_up_factor,
    decay_offset_bias,
    extra_fading_exponent,
    starting_state,
    head_sink_logit,
    linear_head_gain,
    window_output_weight,
    linear_output_weight,
):
    peers = lax.axis_size("sp")
    hops = peers - 1
    line, me = lax.axis_index("sp"), lax.axis_index("tp")
    depth = jnp.where(me == 0, line, hops - line)
    far, near = 1 - me, me
    place = jnp.stack([me, far, hops - depth, line]).astype(jnp.int32)
    rows, half_model = activations.shape
    half = rows // 2
    bf16, f32 = jnp.bfloat16, jnp.float32
    lin = extra_fading_exponent.shape[1] // 2
    key_heads = window_key_weight.shape[1] // HD // 2
    query_heads = window_query_weight.shape[1] // HD // 2
    groups = query_heads // key_heads
    rank = decay_down_factor.shape[1]

    def swap(value):
        return lax.ppermute(value, "tp", SWAP)


    message = _call(
        message_kernel,
        jax.ShapeDtypeStruct((half, half_model + LOOKUP_FEATURES), bf16),
        10**11,
        2**20,
        in_specs=[SMEM, VMEM, VMEM],
        out_specs=VMEM,
    )(place, activations, extra_fading_exponent.T)
    mate = swap(message)
    wide = 2 * half_model // peers + LOOKUP_FEATURES
    outgoing = _call(
        norm_kernel,
        [jax.ShapeDtypeStruct((half, wide), bf16)] * peers,
        10**11,
        2**21,
        in_specs=[SMEM] + [VMEM] * 5,
        out_specs=[VMEM] * peers,
    )(place, activations, extra_fading_exponent.T, mate, input_norm_gain.reshape(1, -1), decay_down_factor.T)

    (
        outgoing,
        matrices,
        window_output_weight,
        linear_output_weight,
        starting_state,
        decay_up_factor,
        decay_offset_bias,
        head_sink_logit,
    ) = lax.optimization_barrier(
        (
            outgoing,
            (
                window_query_weight,
                window_key_weight,
                window_value_weight,
                linear_query_weight,
                linear_key_weight,
                linear_value_weight,
            ),
            window_output_weight,
            linear_output_weight,
            starting_state,
            decay_up_factor,
            decay_offset_bias,
            head_sink_logit,
        )
    )
    incoming = to_offsets(outgoing)
    packed = pack_items(near.reshape(1), lin, key_heads, matrices)
    other_in = swap(packed)
    own_in = pack_items(far.reshape(1), lin, key_heads, matrices)
    features = decay_up_factor.shape[1]
    own_small = jnp.concatenate(
        [
            decay_up_factor.astype(f32),
            decay_offset_bias.reshape(1, features),
            jnp.pad(head_sink_logit, (0, features - head_sink_logit.shape[0])).reshape(1, features),
            jnp.zeros((6, features), f32),
        ],
        axis=0,
    )
    other_small = swap(own_small)
    other_state = swap(starting_state)
    lines = linear_output_weight.shape[0] // 2
    other_linear = lax.dynamic_slice_in_dim(linear_output_weight, near * lines, lines, axis=0)
    other_linear = swap(other_linear)
    lines = window_output_weight.shape[0] // 2
    other_window = lax.dynamic_slice_in_dim(window_output_weight, near * lines, lines, axis=0)
    other_window = swap(other_window)

    incoming = collect(place, incoming)
    mine = incoming.reshape(peers * half, wide)
    theirs = swap(incoming).reshape(peers * half, wide)

    count = 1 + key_heads + 2 * lin
    chained = count - 1 if hops > 1 else count
    arrived, sums, straight = {}, [], []
    for step in range(chained + 2 * hops):
        turn = step - 2 * depth
        index = jnp.clip(jnp.where(turn >= 0, turn, count - 1), 0, count - 1).astype(jnp.int32).reshape(1)
        value = partial_sum(index, mine, theirs, own_in, other_in, arrived.get(step - 2))
        sums.append(value)
        if step == chained and hops > 1:
            straight.append(lax.ppermute(value, ("sp", "tp"), [(0, hops * 2), (hops * 2 + 1, 1)]))
        depths = [
            d for d in range(hops) if 0 <= step - 2 * d < chained or (chained < count and d and step - 2 * d == -2)
        ]
        if depths:
            arrived[step] = lax.ppermute(value, ("sp", "tp"), _pairs(peers, depths, 0))
    finals = sums[2 * hops :]
    if straight:
        finals.append(sums[2 * (hops - 1)])

    running = decay_sums(place, lin, rank, mine, theirs, own_small, other_small)
    sinks = jnp.stack(
        [
            lax.dynamic_slice_in_dim(small[rank + 1], far * query_heads, query_heads).reshape(key_heads, groups)
            for small in (own_small, other_small)
        ]
    )
    sinks = jnp.exp(sinks)
    attended = []
    for group in range(key_heads):
        number = jnp.stack([me, 1 - me])[:, None] * (2 * query_heads) + (
            far * query_heads + group * groups + jnp.arange(groups, dtype=jnp.int32)
        )
        slopes = jnp.exp2(-8.0 * (number + 1).astype(f32) / QH)
        attended.append(
            window_heads(place, group, half, slopes, sinks[:, group], finals[0], finals[1 + group])
        )
    for head in range(lin):
        attended.append(
            linear_heads(
                place,
                lin,
                head,
                half,
                finals[1 + key_heads + 2 * head],
                finals[2 + key_heads + 2 * head],
                running[head],
                starting_state,
                other_state,
                linear_head_gain.reshape(1, DV),
                *(straight if head == lin - 1 else []),
            )
        )

    pieces = len(attended)
    held = []
    for piece in range(pieces):
        seen = [attended[piece]]
        for hop in range(hops):
            if piece == pieces - 1 and 0 < hop == hops - 1:
                seen.append(lax.ppermute(seen[0], ("sp", "tp"), [(hops * 2, 0), (1, hops * 2 + 1)]))
            else:
                seen.append(lax.ppermute(seen[-1], ("sp", "tp"), _pairs(peers, [hop], 1)))
        held.append(seen)
    table = lambda count: tuple(tuple(range(k * peers, (k + 1) * peers)) for k in range(count))
    flat = lambda lists: [value for seen in lists for value in seen]
    (terms,) = output_sum(
        place, flat(held[:key_heads]), table(key_heads), window_output_weight, other_window, None, False
    )
    kept, given = output_sum(
        place, flat(held[key_heads:]), table(lin), linear_output_weight, other_linear, terms, True
    )

    return spread(place, to_offsets(join(place, kept, swap(given), peers)))


def fits(mesh):
    return mesh.shape["tp"] == 2 and mesh.shape["sp"] > 1


def solution(mesh):
    placed = (
        P(("fs", "sp"), "tp"),
        P(),
        P("sp", "tp"),
        P("sp", "tp"),
        P("sp", "tp"),
        P("sp", "tp"),
        P("sp", "tp"),
        P("sp", "tp"),
        P(),
        P(None, "tp"),
        P("tp"),
        P(("fs", "sp"), "tp"),
        P("tp", None, None),
        P("tp"),
        P(),
        P("tp", "sp"),
        P("tp", "sp"),
    )
    if not fits(mesh):
        return jax.shard_map(
            local, mesh=mesh, in_specs=placed, out_specs=P(("fs", "sp", "tp"), None), check_vma=False
        )

    return jax.shard_map(resident, mesh=mesh, in_specs=placed, out_specs=P(("fs", "sp", "tp"), None), check_vma=False)
```

```python
import functools

import jax
import jax.numpy as jnp
from jax import lax
from jax.experimental import pallas as pl
from jax.experimental.pallas import tpu as pltpu
from jax.sharding import PartitionSpec as P


QH = 32
HD = 64
WINDOW = 128
LOOKUP_FEATURES = 128
DV = 256
SPAN = 64


EPS = 1e-05
FADING_SOFTNESS = 16.0
HIGH_PRECISION = lax.Precision.HIGHEST


def passed_along(value, axis, steps):
    count = lax.axis_size(axis)
    leading, last = (max(0, -steps), min(count, count - steps))
    return lax.ppermute(value, axis, [(source, source + steps) for source in range(leading, last)])


def prefix(x, axis, combine, identity):
    peers, place = (lax.axis_size(axis), lax.axis_index(axis))
    everything = jax.tree.map(
        lambda part, kind: lax.all_gather(part.astype(kind), axis), x, (jnp.bfloat16, jnp.bfloat16)
    )
    start = jax.tree.map(
        lambda part, zero: jnp.broadcast_to(jnp.asarray(zero, part.dtype), part.shape), x, identity
    )

    def hop(k, before):
        reached = k < place
        new = combine(
            before, jax.tree.map(lambda part, own: part[k].astype(own.dtype), everything, x)
        )
        return jax.tree.map(lambda a, b: jnp.where(reached, a, b), new, before)

    return lax.fori_loop(0, peers, hop, start)


def window_attention(near_query, near_keys, near_values, head_sink_logit):
    stream_extent = near_query.shape[0]
    key_heads = near_keys.shape[1] // HD
    heads_here = near_query.shape[1] // HD
    groups = heads_here // key_heads
    blocks = stream_extent // WINDOW
    tail_rows = jnp.stack([near_keys, near_values])
    before = passed_along(tail_rows, "sp", 1)

    def banded(previous, current):
        extended = jnp.concatenate([previous, current], axis=0)
        earlier = extended[:stream_extent].reshape(blocks, WINDOW, key_heads, HD)
        present = extended[WINDOW:].reshape(blocks, WINDOW, key_heads, HD)
        return jnp.concatenate([earlier, present], axis=1)

    key_band = banded(before[0], near_keys)
    value_band = banded(before[1], near_values)
    queries = near_query.reshape(blocks, WINDOW, key_heads, groups, HD)
    scores = jnp.einsum(
        "nqhgd,nkhd->hgnqk", queries, key_band, preferred_element_type=jnp.float32
    ) * HD ** (-0.5)
    head_ids = lax.axis_index("tp") * heads_here + jnp.arange(heads_here, dtype=jnp.int32)
    slopes = jnp.exp2(-8.0 * (head_ids + 1).astype(jnp.float32) / QH).reshape(key_heads, groups)
    query_pos = jnp.arange(WINDOW, dtype=jnp.int32)
    key_pos = jnp.arange(2 * WINDOW, dtype=jnp.int32)
    distance = query_pos[:, None] - key_pos[None, :] + WINDOW
    start_pos = (
        lax.axis_index("sp") * stream_extent + (jnp.arange(blocks, dtype=jnp.int32) - 1) * WINDOW
    )
    absolute = start_pos[:, None] + key_pos[None, :]
    allowed = ((distance >= 0) & (distance < WINDOW))[None] & (absolute >= 0)[:, None, :]
    biased = scores - slopes[:, :, None, None, None] * distance.astype(jnp.float32)
    weights = jnp.where(allowed, jnp.exp(biased), 0.0)
    denominator = (
        jnp.sum(weights, axis=-1, keepdims=True)
        + jnp.exp(head_sink_logit.reshape(key_heads, groups))[:, :, None, None, None]
    )
    attention = (weights / denominator).astype(jnp.bfloat16)
    attended = jnp.einsum(
        "hgnqk,nkhd->nqhgd", attention, value_band, preferred_element_type=jnp.float32
    )
    return attended.reshape(stream_extent, heads_here * HD).astype(jnp.bfloat16)


def linear_attention(
    gated_query, gated_keys, gated_values, fading_exponent, linear_head_gain, starting_state
):
    stream_extent = gated_query.shape[0]
    head_total = gated_query.shape[1] // LOOKUP_FEATURES
    span_count = stream_extent // SPAN
    scaled_query = gated_query.astype(jnp.float32).reshape(
        span_count, SPAN, head_total, LOOKUP_FEATURES
    ) * LOOKUP_FEATURES ** (-0.5)
    keys_wide = gated_keys.astype(jnp.float32).reshape(
        span_count, SPAN, head_total, LOOKUP_FEATURES
    )
    values_wide = gated_values.astype(jnp.float32).reshape(span_count, SPAN, head_total, DV)
    running = jnp.cumsum(
        fading_exponent.reshape(span_count, SPAN, head_total, LOOKUP_FEATURES), axis=1
    )
    span_end = running[:, -1]
    query_with_decay = scaled_query * jnp.exp(running)
    inverse_keys = keys_wide * jnp.exp(-running)
    ending_keys = keys_wide * jnp.exp(span_end[:, None] - running)
    inner = jnp.einsum("nchk,nshk->nhcs", query_with_decay, inverse_keys, precision=HIGH_PRECISION)
    lower = jnp.tril(jnp.ones((SPAN, SPAN), dtype=bool))
    inner = jnp.where(lower, inner, 0.0)
    within = jnp.einsum("nhcs,nshv->nchv", inner, values_wide, precision=HIGH_PRECISION)

    def advance(running_state, inputs):
        query_portion, key_portion, value_portion, scale_factor = inputs
        layer_output = jnp.einsum(
            "fmy,mys->fms", query_portion, running_state, precision=HIGH_PRECISION
        )
        running_state = running_state * scale_factor[..., None] + jnp.einsum(
            "gxp,gxz->xpz", key_portion, value_portion, precision=HIGH_PRECISION
        )
        return (running_state, layer_output)

    start_state = jnp.zeros((head_total, LOOKUP_FEATURES, DV), jnp.float32)
    state_end, carried = lax.scan(
        advance, start_state, (query_with_decay, ending_keys, values_wide, jnp.exp(span_end))
    )
    device_decay = jnp.exp(jnp.sum(span_end, axis=0))
    prefix_sums = jnp.cumsum(span_end, axis=0) - span_end

    def combine(earlier, later):
        return (earlier[0] * later[0], later[0][..., None] * earlier[1] + later[1])

    decay_before, state_before = prefix(
        (device_decay, state_end),
        "sp",
        combine,
        (jnp.ones_like(device_decay), jnp.zeros_like(state_end)),
    )
    incoming_rows = state_before + decay_before[..., None] * starting_state
    crossing = jnp.einsum(
        "qwso,soz->qwsz",
        query_with_decay * jnp.exp(prefix_sums)[:, None],
        incoming_rows,
        precision=HIGH_PRECISION,
    )
    flat = (within + carried + crossing).reshape(stream_extent, head_total, DV)
    normal = (
        flat * lax.rsqrt(jnp.mean(flat * flat, axis=-1, keepdims=True) + EPS) * linear_head_gain
    )
    return normal.reshape(stream_extent, head_total * DV).astype(jnp.bfloat16)


def local(
    activations,
    input_norm_gain,
    window_query_weight,
    window_key_weight,
    window_value_weight,
    linear_query_weight,
    linear_key_weight,
    linear_value_weight,
    decay_down_factor,
    decay_up_factor,
    decay_offset_bias,
    extra_fading_exponent,
    starting_state,
    head_sink_logit,
    linear_head_gain,
    window_output_weight,
    linear_output_weight,
):
    gathered = lax.all_gather(activations, "tp", axis=1, tiled=True)
    widened = gathered.astype(jnp.float32)
    normed = (
        widened
        * lax.rsqrt(jnp.mean(widened * widened, axis=1, keepdims=True) + EPS)
        * input_norm_gain
    ).astype(jnp.bfloat16)
    row_total = normed.shape[0]
    matrices = (
        window_query_weight,
        window_key_weight,
        window_value_weight,
        linear_query_weight,
        linear_key_weight,
        linear_value_weight,
    )
    segments = (
        lax.all_gather(matrices[0], "sp", axis=0, tiled=True),
        lax.all_gather(matrices[1], "sp", axis=0, tiled=True),
        lax.all_gather(matrices[2], "sp", axis=0, tiled=True),
        lax.all_gather(matrices[3], "sp", axis=0, tiled=True),
        lax.all_gather(matrices[4], "sp", axis=0, tiled=True),
        lax.all_gather(matrices[5], "sp", axis=0, tiled=True),
    )
    projected = tuple(
        (jnp.dot(normed, segment, preferred_element_type=jnp.float32) for segment in segments)
    )
    near_query, near_keys, near_values, gated_query, gated_keys, gated_values = [
        product.astype(jnp.bfloat16) for product in projected
    ]
    low_rank = jnp.dot(normed, decay_down_factor, preferred_element_type=jnp.float32).astype(
        jnp.bfloat16
    )
    attention_energies = (
        jnp.dot(low_rank, decay_up_factor, preferred_element_type=jnp.float32) + decay_offset_bias
    )
    head_total = extra_fading_exponent.shape[1]
    fading_exponent = (jax.nn.log_sigmoid(attention_energies) / FADING_SOFTNESS).reshape(
        row_total, head_total, LOOKUP_FEATURES
    ) + extra_fading_exponent[:, :, None]
    near_out = window_attention(near_query, near_keys, near_values, head_sink_logit)
    gated_out = linear_attention(
        gated_query, gated_keys, gated_values, fading_exponent, linear_head_gain, starting_state
    )
    window_full, linear_full = (
        lax.all_gather(window_output_weight, "sp", axis=1, tiled=True),
        lax.all_gather(linear_output_weight, "sp", axis=1, tiled=True),
    )
    return lax.psum_scatter(
        (
            jnp.dot(near_out, window_full, preferred_element_type=jnp.float32)
            + jnp.dot(gated_out, linear_full, preferred_element_type=jnp.float32)
        ).astype(jnp.bfloat16),
        "tp",
        scatter_dimension=0,
        tiled=True,
    )


def _pairs(peers, depths, core):
    out = []
    for d in depths:
        out.append((d * 2 + core, (d + 1) * 2 + core))
        out.append(((peers - 1 - d) * 2 + 1 - core, (peers - 2 - d) * 2 + 1 - core))
    return out


SWAP = [(0, 1), (1, 0)]
VMEM = pl.BlockSpec(memory_space=pltpu.VMEM)
SMEM = pl.BlockSpec(memory_space=pltpu.SMEM)
ANY = pl.BlockSpec(memory_space=pl.ANY)
BY_COLUMNS = (((1,), (1,)), ((), ()))
BY_ROWS = (((0,), (0,)), ((), ()))


def _call(kernel, out_shape, flops, moved, grant=24, **kw):
    return pl.pallas_call(
        kernel,
        out_shape=out_shape,
        compiler_params=pltpu.CompilerParams(vmem_limit_bytes=grant * 1024 * 1024),
        cost_estimate=pl.CostEstimate(flops=flops, bytes_accessed=moved, transcendentals=0),
        **kw,
    )


def _prefetch(scalars, grid, in_specs, out_specs, scratch=()):
    return pltpu.PrefetchScalarGridSpec(
        num_scalar_prefetch=scalars, grid=grid, in_specs=in_specs, out_specs=out_specs, scratch_shapes=scratch
    )


def message_kernel(place_ref, x_ref, fade_ref, out_ref):
    rows, wide = out_ref.shape
    half_model = x_ref.shape[1]
    at = pl.ds(pl.multiple_of(place_ref[1] * rows, rows), rows)
    out_ref[:, :half_model] = x_ref[at, :]
    out_ref[:, half_model:] = jnp.concatenate(
        [_parts(_half(fade_ref, place_ref[1])), jnp.zeros((rows, wide - half_model - 3 * fade_ref.shape[0]), jnp.float32)], axis=1
    ).astype(out_ref.dtype)


def _half(turned_ref, which):
    value = turned_ref[...].T
    rows = value.shape[0] // 2
    return jnp.where(which == 0, value[:rows], value[rows:])


def _parts(value):
    high = value.astype(jnp.bfloat16).astype(jnp.float32)
    rest = value - high
    middle = rest.astype(jnp.bfloat16).astype(jnp.float32)
    return jnp.concatenate([high, middle, rest - middle], axis=1)


def norm_kernel(place_ref, x_ref, fade_ref, mate_ref, gain_ref, down_ref, *out_refs):
    me, line = place_ref[0], place_ref[3]
    pieces = len(out_refs)
    rows, wide = out_refs[0].shape
    half_model = x_ref.shape[1]
    cut = 2 * half_model // pieces
    fades = 3 * fade_ref.shape[0]
    own = x_ref[pl.ds(pl.multiple_of(me * rows, rows), rows), :].astype(jnp.float32)
    mate = mate_ref[:, :half_model].astype(jnp.float32)
    square = jnp.sum(own * own, axis=1, keepdims=True) + jnp.sum(mate * mate, axis=1, keepdims=True)
    scale = lax.rsqrt(square / (2 * half_model) + EPS)
    low_rank = None
    for side, value in ((me, own), (1 - me, mate)):
        start = pl.multiple_of(side * half_model, half_model)
        normed = (value * scale * gain_ref[:, pl.ds(start, half_model)]).astype(jnp.bfloat16)
        part = lax.dot_general(
            normed, down_ref[:, pl.ds(start, half_model)], BY_COLUMNS, preferred_element_type=jnp.float32
        )
        low_rank = part if low_rank is None else low_rank + part
        for k in range(pieces // 2):
            away = lax.rem(side * (pieces // 2) + k - line + pieces, pieces)
            for offset, out_ref in enumerate(out_refs):

                @pl.when(away == offset)
                def _():
                    out_ref[:, :cut] = normed[:, k * cut : (k + 1) * cut]

    mine = _parts(_half(fade_ref, me))
    theirs = mate_ref[:, half_model : half_model + fades].astype(jnp.float32)
    tail = jnp.concatenate(
        [
            low_rank.astype(jnp.bfloat16).astype(jnp.float32),
            jnp.where(me == 0, mine, theirs),
            jnp.where(me == 0, theirs, mine),
            jnp.zeros((rows, wide - cut - low_rank.shape[1] - 2 * fades), jnp.float32),
        ],
        axis=1,
    ).astype(jnp.bfloat16)
    for out_ref in out_refs:
        out_ref[:, cut:] = tail


def collect_kernel(place_ref, *refs):
    pieces = len(refs) - 1
    for offset in range(pieces):
        refs[-1][lax.rem(place_ref[3] - offset + pieces, pieces)] = refs[offset][...]


def collect(place, parts):
    rows, wide = parts[0].shape
    return _call(
        collect_kernel,
        jax.ShapeDtypeStruct((len(parts), rows, wide), parts[0].dtype),
        10**8,
        2**21,
        in_specs=[SMEM] + [VMEM] * len(parts),
        out_specs=VMEM,
    )(place, *parts)


def join_kernel(place_ref, kept_ref, given_ref, *out_refs):
    pieces = len(out_refs)
    rows = out_refs[0].shape[0]
    for offset, out_ref in enumerate(out_refs):
        at = pl.ds(pl.multiple_of(lax.rem(place_ref[3] + offset, pieces) * rows, rows), rows)
        out_ref[...] = (kept_ref[at].astype(jnp.float32) + given_ref[at].astype(jnp.float32)).astype(out_ref.dtype)


def join(place, kept, given, pieces):
    rows, columns = kept.shape
    return _call(
        join_kernel,
        [jax.ShapeDtypeStruct((rows // pieces, columns), kept.dtype)] * pieces,
        10**8,
        2**21,
        in_specs=[SMEM, VMEM, VMEM],
        out_specs=[VMEM] * pieces,
    )(place, kept, given)


def spread_kernel(place_ref, *refs):
    pieces = len(refs) - 1
    columns = refs[0].shape[1]
    for offset in range(pieces):
        start = lax.rem(place_ref[3] - offset + pieces, pieces) * columns
        refs[-1][:, pl.ds(pl.multiple_of(start, columns), columns)] = refs[offset][...]


def spread(place, parts):
    rows, columns = parts[0].shape
    return _call(
        spread_kernel,
        jax.ShapeDtypeStruct((rows, len(parts) * columns), parts[0].dtype),
        10**8,
        2**21,
        in_specs=[SMEM] + [VMEM] * len(parts),
        out_specs=VMEM,
    )(place, *parts)


def to_offsets(parts):
    peers = len(parts)
    out = [parts[0]]
    for k in range(1, peers):
        out.append(lax.ppermute(parts[k], "sp", [(i, (i + k) % peers) for i in range(peers)]))
    return out


def pack_kernel(key_heads, side_ref, wq, wk, wv, lq, lk, lv, out_ref):
    step = pl.program_id(0)
    half = out_ref.shape[2] // 2
    keys_and_values = step == 0
    queries = (step > 0) & (step <= key_heads)
    head_items = (step > key_heads) & ((step - key_heads) % 2 == 1)
    head_values = (step > key_heads) & ((step - key_heads) % 2 == 0)

    @pl.when(keys_and_values)
    def _():
        out_ref[0, :, :half] = wk[...]
        out_ref[0, :, half:] = wv[...]

    @pl.when(queries)
    def _():
        out_ref[0] = wq[...]

    @pl.when(head_items)
    def _():
        out_ref[0, :, :half] = lq[...]
        out_ref[0, :, half:] = lk[...]

    @pl.when(head_values)
    def _():
        out_ref[0] = lv[...]


def pack_items(side, lin, key_heads, matrices):
    depth = matrices[0].shape[0]
    width = 2 * LOOKUP_FEATURES
    count = 1 + key_heads + 2 * lin
    fixed = pl.BlockSpec((depth, width // 2), lambda i, side: (0, side[0]))
    query = pl.BlockSpec(
        (depth, width), lambda i, side: (0, side[0] * key_heads + jnp.clip(i - 1, 0, key_heads - 1))
    )
    head = lambda i, side: (0, side[0] * lin + jnp.clip((i - 1 - key_heads) // 2, 0, lin - 1))
    narrow, full = pl.BlockSpec((depth, width // 2), head), pl.BlockSpec((depth, width), head)
    return _call(
        functools.partial(pack_kernel, key_heads),
        jax.ShapeDtypeStruct((count, depth, width), jnp.bfloat16),
        10**11,
        4 * count * depth * width,
        grid_spec=_prefetch(
            1,
            (count,),
            [query, fixed, fixed, narrow, narrow, full],
            pl.BlockSpec((1, depth, width), lambda i, side: (i, 0, 0)),
        ),
    )(side, *matrices)


def partial_kernel(index_ref, mine_ref, theirs_ref, own_ref, other_ref, *rest):
    out_ref, weight, arrival = rest[-3:]
    rows = mine_ref.shape[0]
    depth, width = weight.shape
    copy = pltpu.make_async_copy(other_ref.at[index_ref[0]], weight, arrival)
    copy.start()
    for half in range(2):
        if half == 1:
            copy.wait()
        for top, x_ref in enumerate((mine_ref, theirs_ref)):
            at = slice(top * rows, (top + 1) * rows)
            span = slice(half * width, (half + 1) * width)
            matrix = own_ref[index_ref[0]] if half == 0 else weight[...]
            total = jnp.dot(x_ref[:, :depth], matrix, preferred_element_type=jnp.float32)
            if len(rest) == 4:
                total = total + rest[0][at, span].astype(jnp.float32)
            out_ref[at, span] = total.astype(out_ref.dtype)


def partial_sum(index, mine, theirs, own, other, arrived):
    rows = mine.shape[0]
    _, depth, width = own.shape
    operands = [mine, theirs, own, other] + ([] if arrived is None else [arrived])
    return _call(
        partial_kernel,
        jax.ShapeDtypeStruct((2 * rows, 2 * width), jnp.bfloat16),
        160 * rows * depth * width,
        4 * depth * (rows + width),
        in_specs=[SMEM, VMEM, VMEM, VMEM, ANY] + [VMEM] * (len(operands) - 4),
        out_specs=VMEM,
        scratch_shapes=[pltpu.VMEM((depth, width), jnp.bfloat16), pltpu.SemaphoreType.DMA],
    )(index, *operands)


def decay_kernel(lin, rank, place_ref, mine_ref, theirs_ref, own_ref, other_ref, *out_refs):
    me, side = place_ref[0], place_ref[1]
    rows = mine_ref.shape[0]
    features = LOOKUP_FEATURES
    lower = (
        lax.broadcasted_iota(jnp.int32, (SPAN, SPAN), 0) >= lax.broadcasted_iota(jnp.int32, (SPAN, SPAN), 1)
    ).astype(jnp.bfloat16)
    for top, tail_ref in enumerate((mine_ref, theirs_ref)):
        tail = tail_ref[:, tail_ref.shape[1] - features :]
        low_rank = tail[:, :rank]
        parts = [
            tail[:, rank + k * 2 * lin : rank + (k + 1) * 2 * lin].astype(jnp.float32) for k in range(6)
        ]
        by_core = [parts[0] + parts[1] + parts[2], parts[3] + parts[4] + parts[5]]
        fades = [jnp.where(me == 0, by_core[0], by_core[1]), jnp.where(me == 0, by_core[1], by_core[0])]
        for head in range(lin):
            for owner, small_ref in enumerate((own_ref, other_ref)):
                at = pl.ds(pl.multiple_of((side * lin + head) * features, features), features)
                up = small_ref[:rank, at].astype(jnp.bfloat16)
                energy = jnp.dot(low_rank, up, preferred_element_type=jnp.float32) + small_ref[rank : rank + 1, at]
                soft = jnp.minimum(energy, 0.0) - jnp.log1p(jnp.exp(-jnp.abs(energy)))
                both = fades[owner]
                fade = jnp.where(side == 0, both[:, head : head + 1], both[:, lin + head : lin + head + 1])
                step = soft * (1.0 / FADING_SOFTNESS) + fade
                high = step.astype(jnp.bfloat16)
                rest = step - high.astype(jnp.float32)
                middle = rest.astype(jnp.bfloat16)
                low = (rest - middle.astype(jnp.float32)).astype(jnp.bfloat16)
                column = owner * features
                out_ref = out_refs[head]
                for span in range(rows // SPAN):
                    cut = slice(span * SPAN, (span + 1) * SPAN)
                    out_ref[top * rows + span * SPAN : top * rows + (span + 1) * SPAN, column : column + features] = (
                        jnp.dot(lower, high[cut], preferred_element_type=jnp.float32)
                        + jnp.dot(lower, middle[cut], preferred_element_type=jnp.float32)
                        + jnp.dot(lower, low[cut], preferred_element_type=jnp.float32)
                    )


def decay_sums(place, lin, rank, mine, theirs, own, other):
    return _call(
        functools.partial(decay_kernel, lin, rank),
        [jax.ShapeDtypeStruct((2 * mine.shape[0], 2 * LOOKUP_FEATURES), jnp.float32)] * lin,
        10**9,
        2**20,
        in_specs=[SMEM] + [VMEM] * 4,
        out_specs=[VMEM] * lin,
    )(place, mine, theirs, own, other)


def linear_kernel(lin, head, half, place_ref, query_key_ref, value_ref, running_ref, own_ref, other_ref, gain_ref, out_ref):
    me, side = place_ref[0], place_ref[1]
    rows, width = query_key_ref.shape
    features = LOOKUP_FEATURES
    values = width // 2
    lower = lax.broadcasted_iota(jnp.int32, (SPAN, SPAN), 0) >= lax.broadcasted_iota(
        jnp.int32, (SPAN, SPAN), 1
    )
    states = [state_ref[side * lin + head].T for state_ref in (own_ref, other_ref)]
    for span in range(rows // SPAN):
        per = half // SPAN
        device, inside = span // (2 * per), span % (2 * per)
        apart = jnp.where(me == inside // per, 0, rows // 2)
        at = pl.ds(pl.multiple_of(apart + device * half + (inside % per) * SPAN, SPAN), SPAN)
        for owner in range(2):
            base = owner * values
            running = running_ref[at, owner * features : (owner + 1) * features]
            query = query_key_ref[at, base : base + features].astype(jnp.float32)
            key = query_key_ref[at, base + features : base + 2 * features].astype(jnp.float32)
            value = value_ref[at, base : base + values]
            end = running[SPAN - 1 : SPAN]
            scaled = (query * features ** (-0.5) * jnp.exp(running)).astype(jnp.bfloat16)
            inverse = (key * jnp.exp(-running)).astype(jnp.bfloat16)
            ending = (key * jnp.exp(end - running)).astype(jnp.bfloat16)
            inner = lax.dot_general(scaled, inverse, BY_COLUMNS, preferred_element_type=jnp.float32)
            inner = jnp.where(lower, inner, 0.0).astype(jnp.bfloat16)
            state = states[owner]
            raw = jnp.dot(inner, value, preferred_element_type=jnp.float32) + lax.dot_general(
                scaled, state.astype(jnp.bfloat16), BY_COLUMNS, preferred_element_type=jnp.float32
            )
            states[owner] = state * jnp.exp(end) + lax.dot_general(
                value, ending, BY_ROWS, preferred_element_type=jnp.float32
            )
            scale = lax.rsqrt(jnp.mean(raw * raw, axis=-1, keepdims=True) + EPS)
            out_ref[at, base : base + values] = (raw * scale * gain_ref[...]).astype(out_ref.dtype)


def linear_heads(place, lin, head, half, query_key, value, running, own, other, gain):
    return _call(
        functools.partial(linear_kernel, lin, head, half),
        jax.ShapeDtypeStruct(query_key.shape, jnp.bfloat16),
        2 * 10**9,
        2**21,
        in_specs=[SMEM] + [VMEM] * 6,
        out_specs=VMEM,
    )(place, query_key, value, running, own, other, gain)


def window_kernel(group, half, place_ref, slope_ref, sink_ref, key_value_ref, query_ref, out_ref):
    me = place_ref[0]
    rows = query_ref.shape[0]
    owners, groups = slope_ref.shape
    pair = key_value_ref.shape[1] // (2 * owners)
    from_query = lax.broadcasted_iota(jnp.int32, (WINDOW, WINDOW), 0)
    from_key = lax.broadcasted_iota(jnp.int32, (WINDOW, WINDOW), 1)
    present = from_key <= from_query
    distance = jnp.where(present, from_query - from_key, from_query - from_key + WINDOW).astype(jnp.float32)
    unit = min(half, WINDOW)

    def places(block):
        out = []
        for piece in range(WINDOW // unit):
            start = block * WINDOW + piece * unit
            device, inside = start // (2 * half), start % (2 * half)
            apart = jnp.where(me == inside // half, 0, rows // 2)
            out.append(pl.ds(pl.multiple_of(apart + device * half + inside % half, unit), unit))
        return out

    lanes = lax.broadcasted_iota(jnp.int32, (WINDOW, pair), 1)
    of_group = lanes // HD == group
    first_half = lanes < HD
    keep_present = present.astype(jnp.float32).astype(jnp.bfloat16)
    keep_past = (1.0 - present.astype(jnp.float32)).astype(jnp.bfloat16)
    turned = lambda value: jnp.concatenate([value[:, HD:], value[:, :HD]], axis=1)

    for owner in range(owners):
        key_at = owner * 2 * pair
        base = owner * groups * HD
        biases = [slope_ref[owner, head] * distance for head in range(groups)]
        past_keys, past_values = None, None
        for block in range(rows // WINDOW):
            first = block == 0
            at = places(block)
            load = lambda ref, start: jnp.concatenate([ref[a, start : start + pair] for a in at], axis=0)
            keys, values = load(key_value_ref, key_at), load(key_value_ref, key_at + pair)
            band_keys = keys if first else jnp.concatenate([past_keys, keys], axis=0)
            band_values = values if first else jnp.concatenate([past_values, values], axis=0)
            past_keys, past_values = keys, values
            queries = []
            for couple in range(groups // 2):
                both = load(query_ref, base + couple * pair).astype(jnp.float32) * HD ** (-0.5)
                swapped = turned(both)
                ordered = (both, swapped) if group == 0 else (swapped, both)
                queries += [jnp.where(of_group, value, 0.0).astype(jnp.bfloat16) for value in ordered]
            scores = lax.dot_general(
                jnp.concatenate(queries, axis=0), band_keys, BY_COLUMNS, preferred_element_type=jnp.float32
            )
            probs = []
            for head in range(groups):
                mine = scores[head * WINDOW : (head + 1) * WINDOW]
                if first:
                    weight = jnp.where(present, jnp.exp(mine - biases[head]), 0.0)
                else:
                    weight = jnp.exp(jnp.where(present, mine[:, WINDOW:], mine[:, :WINDOW]) - biases[head])
                total = jnp.sum(weight, axis=-1, keepdims=True) + sink_ref[owner, head]
                share = (weight / total).astype(jnp.bfloat16)
                if first:
                    probs.append(share)
                else:
                    probs.append(jnp.concatenate([share * keep_past, share * keep_present], axis=1))
            outs = jnp.dot(jnp.concatenate(probs, axis=0), band_values, preferred_element_type=jnp.float32)
            for couple in range(groups // 2):
                even = outs[2 * couple * WINDOW : (2 * couple + 1) * WINDOW]
                odd = outs[(2 * couple + 1) * WINDOW : (2 * couple + 2) * WINDOW]
                if group == 0:
                    odd = turned(odd)
                else:
                    even = turned(even)
                joined = jnp.where(first_half, even, odd).astype(out_ref.dtype)
                start = base + couple * pair
                for piece, a in enumerate(at):
                    out_ref[a, start : start + pair] = joined[piece * unit : (piece + 1) * unit]


def window_heads(place, group, half, slopes, sinks, key_value, query):
    return _call(
        functools.partial(window_kernel, group, half),
        jax.ShapeDtypeStruct(query.shape, jnp.bfloat16),
        2 * 10**9,
        2**21,
        in_specs=[SMEM, SMEM, SMEM, VMEM, VMEM],
        out_specs=VMEM,
    )(place, slopes, sinks, key_value, query)


def output_kernel(sources, place_ref, *refs):
    count = 1 + max(max(row) for row in sources)
    pieces = len(sources)
    passed = refs[:count]
    own_ref, other_ref = refs[count : count + 2]
    held, arrival = refs[-2:]
    rest = refs[count + 2 : -2]
    split = rest[-1].shape[0] != held.shape[1]
    outs = rest[-2:] if split else rest[-1:]
    before = rest[: len(rest) - len(outs)]
    depth = place_ref[2]
    for at in range(len(sources[0])):

        @pl.when(depth == at)
        def _():
            for piece in range(pieces):
                pltpu.make_async_copy(passed[sources[piece][at]], held.at[piece], arrival.at[piece]).start()

    for piece in range(pieces):
        pltpu.make_async_copy(passed[0], held.at[piece], arrival.at[piece]).wait()
    width = held.shape[2] // 2
    rows = outs[0].shape[0]
    columns = outs[0].shape[1]
    block = columns // 2
    for top, out_ref in enumerate(outs):
        at = slice(top * rows, (top + 1) * rows)
        for part in range(2):
            span = slice(part * block, (part + 1) * block)
            total = before[0][at, span] if before else jnp.zeros((rows, block), jnp.float32)
            for piece in range(pieces):
                lines = slice(piece * width, (piece + 1) * width)
                total = total + jnp.dot(
                    held[piece, at, :width], own_ref[lines, span], preferred_element_type=jnp.float32
                )
                total = total + jnp.dot(
                    held[piece, at, width:], other_ref[lines, span], preferred_element_type=jnp.float32
                )
            out_ref[:, span] = total.astype(out_ref.dtype)


def output_sum(place, passed, sources, own, other, before, split):
    rows, width = passed[0].shape
    pieces = len(sources)
    lines, columns = other.shape
    kind, parts = (jnp.bfloat16, 2) if split else (jnp.float32, 1)
    whole = pl.BlockSpec((rows, columns), lambda i, place: (0, 0))
    out = pl.BlockSpec((rows // parts, columns), lambda i, place: (0, 0))
    return _call(
        functools.partial(output_kernel, sources),
        [jax.ShapeDtypeStruct((rows // parts, columns), kind)] * parts,
        4 * rows * columns * lines,
        8 * rows * columns,
        grid_spec=_prefetch(
            1,
            (1,),
            [ANY] * len(passed)
            + [
                pl.BlockSpec((lines, columns), lambda i, place: (place[1], 0)),
                pl.BlockSpec((lines, columns), lambda i, place: (0, 0)),
            ]
            + ([] if before is None else [whole]),
            [out] * parts,
            [pltpu.VMEM((pieces, rows, width), jnp.bfloat16), pltpu.SemaphoreType.DMA((pieces,))],
        ),
    )(place, *passed, own, other, *([] if before is None else [before]))


def resident(
    activations,
    input_norm_gain,
    window_query_weight,
    window_key_weight,
    window_value_weight,
    linear_query_weight,
    linear_key_weight,
    linear_value_weight,
    decay_down_factor,
    decay_up_factor,
    decay_offset_bias,
    extra_fading_exponent,
    starting_state,
    head_sink_logit,
    linear_head_gain,
    window_output_weight,
    linear_output_weight,
):
    peers = lax.axis_size("sp")
    hops = peers - 1
    line, me = lax.axis_index("sp"), lax.axis_index("tp")
    depth = jnp.where(me == 0, line, hops - line)
    far, near = 1 - me, me
    place = jnp.stack([me, far, hops - depth, line]).astype(jnp.int32)
    rows, half_model = activations.shape
    half = rows // 2
    bf16, f32 = jnp.bfloat16, jnp.float32
    lin = extra_fading_exponent.shape[1] // 2
    key_heads = window_key_weight.shape[1] // HD // 2
    query_heads = window_query_weight.shape[1] // HD // 2
    groups = query_heads // key_heads
    rank = decay_down_factor.shape[1]

    def swap(value):
        return lax.ppermute(value, "tp", SWAP)


    message = _call(
        message_kernel,
        jax.ShapeDtypeStruct((half, half_model + LOOKUP_FEATURES), bf16),
        10**11,
        2**20,
        in_specs=[SMEM, VMEM, VMEM],
        out_specs=VMEM,
    )(place, activations, extra_fading_exponent.T)
    mate = swap(message)
    wide = 2 * half_model // peers + LOOKUP_FEATURES
    outgoing = _call(
        norm_kernel,
        [jax.ShapeDtypeStruct((half, wide), bf16)] * peers,
        10**11,
        2**21,
        in_specs=[SMEM] + [VMEM] * 5,
        out_specs=[VMEM] * peers,
    )(place, activations, extra_fading_exponent.T, mate, input_norm_gain.reshape(1, -1), decay_down_factor.T)

    (
        outgoing,
        matrices,
        window_output_weight,
        linear_output_weight,
        starting_state,
        decay_up_factor,
        decay_offset_bias,
        head_sink_logit,
    ) = lax.optimization_barrier(
        (
            outgoing,
            (
                window_query_weight,
                window_key_weight,
                window_value_weight,
                linear_query_weight,
                linear_key_weight,
                linear_value_weight,
            ),
            window_output_weight,
            linear_output_weight,
            starting_state,
            decay_up_factor,
            decay_offset_bias,
            head_sink_logit,
        )
    )
    incoming = to_offsets(outgoing)
    packed = pack_items(near.reshape(1), lin, key_heads, matrices)
    other_in = swap(packed)
    own_in = pack_items(far.reshape(1), lin, key_heads, matrices)
    features = decay_up_factor.shape[1]
    own_small = jnp.concatenate(
        [
            decay_up_factor.astype(f32),
            decay_offset_bias.reshape(1, features),
            jnp.pad(head_sink_logit, (0, features - head_sink_logit.shape[0])).reshape(1, features),
            jnp.zeros((6, features), f32),
        ],
        axis=0,
    )
    other_small = swap(own_small)
    other_state = swap(starting_state)
    lines = linear_output_weight.shape[0] // 2
    other_linear = lax.dynamic_slice_in_dim(linear_output_weight, near * lines, lines, axis=0)
    other_linear = swap(other_linear)
    lines = window_output_weight.shape[0] // 2
    other_window = lax.dynamic_slice_in_dim(window_output_weight, near * lines, lines, axis=0)
    other_window = swap(other_window)

    incoming = collect(place, incoming)
    mine = incoming.reshape(peers * half, wide)
    theirs = swap(incoming).reshape(peers * half, wide)

    count = 1 + key_heads + 2 * lin
    arrived, finals = {}, []
    for step in range(count + 2 * hops):
        index = jnp.clip(step - 2 * depth, 0, count - 1).astype(jnp.int32).reshape(1)
        value = partial_sum(index, mine, theirs, own_in, other_in, arrived.get(step - 2))
        depths = [d for d in range(hops) if 0 <= step - 2 * d < count]
        if depths:
            arrived[step] = lax.ppermute(value, ("sp", "tp"), _pairs(peers, depths, 0))
        if step >= 2 * hops:
            finals.append(value)

    running = decay_sums(place, lin, rank, mine, theirs, own_small, other_small)
    sinks = jnp.stack(
        [
            lax.dynamic_slice_in_dim(small[rank + 1], far * query_heads, query_heads).reshape(key_heads, groups)
            for small in (own_small, other_small)
        ]
    )
    sinks = jnp.exp(sinks)
    attended = []
    for group in range(key_heads):
        number = jnp.stack([me, 1 - me])[:, None] * (2 * query_heads) + (
            far * query_heads + group * groups + jnp.arange(groups, dtype=jnp.int32)
        )
        slopes = jnp.exp2(-8.0 * (number + 1).astype(f32) / QH)
        attended.append(
            window_heads(place, group, half, slopes, sinks[:, group], finals[0], finals[1 + group])
        )
    for head in range(lin):
        attended.append(
            linear_heads(
                place,
                lin,
                head,
                half,
                finals[1 + key_heads + 2 * head],
                finals[2 + key_heads + 2 * head],
                running[head],
                starting_state,
                other_state,
                linear_head_gain.reshape(1, DV),
            )
        )

    pieces = len(attended)
    held = []
    for piece in range(pieces):
        seen = [attended[piece]]
        for hop in range(hops):
            if piece == pieces - 1 and 0 < hop == hops - 1:
                seen.append(lax.ppermute(seen[0], ("sp", "tp"), [(hops * 2, 0), (1, hops * 2 + 1)]))
            else:
                seen.append(lax.ppermute(seen[-1], ("sp", "tp"), _pairs(peers, [hop], 1)))
        held.append(seen)
    table = lambda count: tuple(tuple(range(k * peers, (k + 1) * peers)) for k in range(count))
    flat = lambda lists: [value for seen in lists for value in seen]
    (terms,) = output_sum(
        place, flat(held[:key_heads]), table(key_heads), window_output_weight, other_window, None, False
    )
    kept, given = output_sum(
        place, flat(held[key_heads:]), table(lin), linear_output_weight, other_linear, terms, True
    )

    return spread(place, to_offsets(join(place, kept, swap(given), peers)))


def fits(mesh):
    return mesh.shape["tp"] == 2 and mesh.shape["sp"] > 1


def solution(mesh):
    placed = (
        P(("fs", "sp"), "tp"),
        P(),
        P("sp", "tp"),
        P("sp", "tp"),
        P("sp", "tp"),
        P("sp", "tp"),
        P("sp", "tp"),
        P("sp", "tp"),
        P(),
        P(None, "tp"),
        P("tp"),
        P(("fs", "sp"), "tp"),
        P("tp", None, None),
        P("tp"),
        P(),
        P("tp", "sp"),
        P("tp", "sp"),
    )
    if not fits(mesh):
        return jax.shard_map(
            local, mesh=mesh, in_specs=placed, out_specs=P(("fs", "sp", "tp"), None), check_vma=False
        )

    return jax.shard_map(resident, mesh=mesh, in_specs=placed, out_specs=P(("fs", "sp", "tp"), None), check_vma=False)
```
